32 devices in a mesh: sp: 4 (over z), fs: 4 (over y, x), tp: 2 (over core).
Axes of the slice: x: 2, y: 2, z: 4, core: 2. Of those that a mesh axis runs over, the one named last changes fastest.
Arguments:
- inputs: bfloat16 [2048, 2048], P(('fs', 'sp'), 'tp'), parts along dimension 0, may hold values from -6 to 6
- norm_gain: float32 [2048], replicated, may hold values from 0.1 to 1.9
- in_ssm: bfloat16 [2048, 1024], P('sp', 'tp'), may hold values from -0.125 to 0.125
- in_query: bfloat16 [2048, 1024], P('sp', 'tp')
- in_key: bfloat16 [2048, 256], P('sp', 'tp')
- in_value: bfloat16 [2048, 256], P('sp', 'tp'), may hold values from -0.125 to 0.125
- decay_rate: float32 [64, 64], P('tp'), as said below
- rotation: float32 [64, 64], P('tp'), may hold values from 0.05 to 3
- input_parts: bfloat16 [2, 64, 64, 16], P(None, 'tp')
- output_parts: bfloat16 [2, 64, 16, 64], P(None, 'tp'), may hold values from -0.5 to 0.5
- skip_scale: float32 [64, 16], P('tp'), may hold values from -4 to 4
- decay_shift: float32 [2048, 64], P(('fs', 'sp'), 'tp'), parts along dimension 0, may hold values from -1 to 0
- sink_logit: float32 [16], P('tp'), may hold values from 2 to 6
- out_state: bfloat16 [1024, 2048], P('tp', 'sp'), may hold values from -0.125 to 0.125
- out_attend: bfloat16 [1024, 2048], P('tp', 'sp'), may hold values from -0.125 to 0.125
Outputs:
- mixed: bfloat16 [2048, 2048], P(('fs', 'sp', 'tp')), parts along dimension 0
The draws below stay inside these ranges and needn't reach their ends.
There are 4 independent parts, one for each index of `fs`. The reference program is written for one: setup_inputs(seed, part) draws one part's arguments, and reference() takes and returns one part's arrays. A program takes and returns all parts, laid end to end along the dimension named above; an argument that names none is the same for every part. Nothing has to cross between parts.
Inputs may be any that keep to these rules, and one draw needn't show every extreme that they name: `decay_rate`: between 1e-5 and 0.1.
All inputs are finite; a program needn't handle non-finite values.
Results may differ from the reference program's by a relative error of at most 0.012.
Values may be sent and summed in bfloat16 or wider, within the bound.
A program may use at most 64 MiB of HBM per device.

```python
import math
import jax
import jax.numpy as jnp
from jax import lax

D = 2048
GROUPS = 64
GROUP_CH = 16
STATE = 64
Q_HEADS = 16
KV_HEADS = 4
HEAD_DIM = 64
WINDOW = 128
BLOCK = 128
TOK_DEV = 128
LEN = 512
N_SP = 4


def recurrence_law(key):
    mask_key = jax.random.fold_in(key, 11)
    slow_key = jax.random.fold_in(key, 12)
    fast_key = jax.random.fold_in(key, 13)
    part_key = jax.random.fold_in(key, 14)
    portion = 0.5
    slow = jax.random.uniform(mask_key, (GROUPS, STATE), jnp.float32) < portion
    slow_rate = jnp.exp(jax.random.uniform(slow_key, (GROUPS, STATE), jnp.float32, math.log(0.1), math.log(0.4))) / LEN
    fast_rate = jnp.exp(jax.random.uniform(fast_key, (GROUPS, STATE), jnp.float32, math.log(0.02), math.log(0.1)))
    rates = jnp.where(slow, slow_rate, fast_rate)
    spread = jnp.sqrt(1.0 - jnp.exp(-2.0 * rates)) / math.sqrt(GROUP_CH)
    parts = jax.random.normal(part_key, (2, GROUPS, STATE, GROUP_CH), jnp.float32) * spread[None, :, :, None]
    return (rates, parts)


def draw_decay_rate(key, part):
    return recurrence_law(key)[0].astype(jnp.float32)


def draw_input_parts(key, part):
    return recurrence_law(key)[1].astype(jnp.bfloat16)


def attention_law(key):
    noise_key = jax.random.fold_in(key, 22)
    other_key = jax.random.fold_in(key, 23)
    repeat = Q_HEADS // KV_HEADS
    noise = jax.random.normal(noise_key, (D, KV_HEADS, repeat, HEAD_DIM), jnp.float32) / math.sqrt(D)
    keys_part = jax.random.normal(other_key, (D, KV_HEADS, HEAD_DIM), jnp.float32) / math.sqrt(D)
    queries_part = noise
    return (queries_part.reshape(D, Q_HEADS * HEAD_DIM), keys_part.reshape(D, KV_HEADS * HEAD_DIM))


def draw_in_query(key, part):
    return attention_law(key)[0].astype(jnp.bfloat16)


def draw_in_key(key, part):
    return attention_law(key)[1].astype(jnp.bfloat16)


def draw_decay_shift(key, part):
    factor_key = jax.random.fold_in(key, 31)
    noise_key = jax.random.fold_in(key, 32)
    place_key = jax.random.fold_in(key, 33)
    depth_key = jax.random.fold_in(key, 34)
    factor = jnp.exp(jax.random.uniform(factor_key, (LEN // TOK_DEV,), jnp.float32, math.log(0.5), math.log(2.0)))
    per_position = jnp.repeat(factor, TOK_DEV)
    rough = jax.random.uniform(noise_key, (LEN, GROUPS), jnp.float32, 0.25, 1.75)
    background = -(0.3 / LEN) * per_position[:, None] * rough
    places = jax.random.randint(place_key, (2,), 0, LEN)
    struck = jnp.any(jnp.arange(LEN, dtype=jnp.int32)[:, None] == places[None, :], axis=1)
    kept = jax.random.uniform(depth_key, (GROUPS,), jnp.float32, 0.6, 0.8)
    return (background + jnp.where(struck[:, None], jnp.log(kept)[None, :], 0.0)).astype(jnp.float32)


def level_of(rng, shape, cuts, smallest, largest):
    factor_of, own = 1.0, jax.random.fold_in(rng, 6)
    for axis_at, shards_of in cuts:
        heights = jnp.exp(jax.random.uniform(jax.random.fold_in(own, axis_at), (shards_of,), jnp.float32, smallest / len(cuts), largest / len(cuts)))
        factor_of = factor_of * jnp.repeat(heights, shape[axis_at] // shards_of).reshape([-1 if axis == axis_at else 1 for axis in range(len(shape))])
    return factor_of


def normal_values(stream_key, extent, scale, most, cuts=(), held_as=jnp.bfloat16):
    loudness = level_of(stream_key, extent, cuts, -0.22, 0.18) if cuts else 1.0
    entries = jax.random.normal(stream_key, extent, jnp.float32) * scale * loudness
    return jnp.minimum(jnp.maximum(entries, -most), most).astype(held_as)


def setup_inputs(seed: int = 0, part: int = 0) -> dict:
    key_list = jax.random.split(jax.random.key(seed), 16)
    part_keys = jax.random.split(jax.random.fold_in(key_list[15], part), 16)
    return {
        "inputs": normal_values(part_keys[0], (LEN, D), 1.0, 6.0, ((0, 4), (1, 2))),
        "norm_gain": jnp.clip(1.0 + 0.18 * jax.random.normal(key_list[1], (D,), jnp.float32), 0.1, 1.9),
        "in_ssm": normal_values(key_list[2], (D, GROUPS * GROUP_CH), D ** -0.5, 0.125, ((0, 4), (1, 2))),
        "in_query": draw_in_query(jax.random.fold_in(key_list[15], 71), part),
        "in_key": draw_in_key(jax.random.fold_in(key_list[15], 71), part),
        "in_value": normal_values(key_list[5], (D, KV_HEADS * HEAD_DIM), D ** -0.5, 0.125, ((0, 4), (1, 2))),
        "decay_rate": draw_decay_rate(jax.random.fold_in(key_list[15], 71), part),
        "rotation": jnp.clip(0.05 + 2.95 * jax.random.uniform(key_list[7], (GROUPS, STATE), jnp.float32) ** level_of(key_list[7], (GROUPS, STATE), ((0, 2),), -0.2, 0.2), 0.05, 3.0),
        "input_parts": draw_input_parts(jax.random.fold_in(key_list[15], 71), part),
        "output_parts": normal_values(key_list[9], (2, GROUPS, GROUP_CH, STATE), (2 * STATE) ** -0.5, 0.5, ((1, 2),)),
        "skip_scale": normal_values(key_list[10], (GROUPS, GROUP_CH), 1.0, 4.0, ((0, 2),), jnp.float32),
        "decay_shift": draw_decay_shift(jax.random.fold_in(jax.random.fold_in(key_list[15], part), 71), part),
        "sink_logit": jnp.clip(2.0 + 4.0 * jax.random.uniform(key_list[12], (Q_HEADS,), jnp.float32) ** level_of(key_list[12], (Q_HEADS,), ((0, 2),), -0.2, 0.2), 2.0, 6.0),
        "out_state": normal_values(key_list[13], (GROUPS * GROUP_CH, D), (GROUPS * GROUP_CH + Q_HEADS * HEAD_DIM) ** -0.5, 0.125, ((0, 2), (1, 4))),
        "out_attend": normal_values(key_list[14], (Q_HEADS * HEAD_DIM, D), (GROUPS * GROUP_CH + Q_HEADS * HEAD_DIM) ** -0.5, 0.125, ((0, 2), (1, 4))),
    }


epsilon = 1e-06
floor_score = -1e+30

def combine(earlier, later):
    first_re, first_im, state_re, state_im = earlier
    second_re, second_im, input_re, input_im = later
    return (second_re * first_re - second_im * first_im, second_re * first_im + second_im * first_re, second_re * state_re - second_im * state_im + input_re, second_re * state_im + second_im * state_re + input_im)

def input_matrix(decay_rate, rotation, input_parts):
    damped = jnp.exp(-decay_rate)
    lift_re = damped * jnp.cos(rotation) - 1.0
    lift_im = damped * jnp.sin(rotation)
    modulus = decay_rate * decay_rate + rotation * rotation
    factor_re = (rotation * lift_im - decay_rate * lift_re) / modulus
    factor_im = -(rotation * lift_re + decay_rate * lift_im) / modulus
    part_re = input_parts[0].astype(jnp.float32)
    part_im = input_parts[1].astype(jnp.float32)
    joined_re = factor_re[:, :, None] * part_re - factor_im[:, :, None] * part_im
    joined_im = factor_re[:, :, None] * part_im + factor_im[:, :, None] * part_re
    return jnp.concatenate([joined_re, joined_im], axis=1).astype(jnp.bfloat16)

def advance_block(carry, drive, shift, grouped, decay_rate, rotation, output_parts, skip_scale):
    carry_re, carry_im = carry
    width = drive.shape[2] // 2
    magnitude = jnp.exp(shift[:, :, None] - decay_rate[None])
    elements = (magnitude * jnp.cos(rotation)[None], magnitude * jnp.sin(rotation)[None], drive[:, :, :width], drive[:, :, width:])
    decay_re, decay_im, state_re, state_im = lax.associative_scan(combine, elements, axis=0)
    state_re = state_re + decay_re * carry_re[None] - decay_im * carry_im[None]
    state_im = state_im + decay_re * carry_im[None] + decay_im * carry_re[None]
    read_re = output_parts[0].astype(jnp.float32)
    read_im = output_parts[1].astype(jnp.float32)
    result = jnp.einsum('tgp,ghp->tgh', state_re, read_re, precision=lax.Precision.HIGHEST)
    result = result - jnp.einsum('tgp,ghp->tgh', state_im, read_im, precision=lax.Precision.HIGHEST)
    result = result + skip_scale.astype(jnp.float32)[None] * grouped.astype(jnp.float32)
    return ((state_re[-1], state_im[-1]), jax.nn.gelu(result).astype(jnp.bfloat16))

def window_attention(queries, keys_win, values_win, starts, sink_logit):
    window = queries.shape[1]
    scores = jnp.einsum('nqgrd,nkgd->ngrqk', queries.astype(jnp.float32), keys_win.astype(jnp.float32))
    scores = scores * queries.shape[-1] ** (-0.5)
    places = jnp.arange(window, dtype=jnp.int32)[:, None] + window - jnp.arange(2 * window, dtype=jnp.int32)[None, :]
    inside = (places >= 0) & (places < window)
    reach = starts[:, None] - window + jnp.arange(2 * window, dtype=jnp.int32)[None, :] >= 0
    valid = (inside[None] & reach[:, None, :])[:, None, None]
    sinks = sink_logit.astype(jnp.float32).reshape(scores.shape[1], scores.shape[2])[None, :, :, None, None]
    scores = jnp.where(valid, scores, floor_score)
    row_peak = jnp.maximum(lax.optimization_barrier(jnp.max(scores, axis=-1, keepdims=True)), sinks)
    raised = jnp.where(valid, jnp.exp(scores - row_peak), 0.0)
    denominator = lax.optimization_barrier(jnp.sum(raised, axis=-1, keepdims=True)) + jnp.exp(sinks - row_peak)
    weights = (raised / denominator).astype(jnp.bfloat16)
    result = jnp.einsum('ngrqk,nkgd->nqgrd', weights.astype(jnp.float32), values_win.astype(jnp.float32))
    return result.astype(jnp.bfloat16)

def reference(inputs, norm_gain, in_ssm, in_query, in_key, in_value, decay_rate, rotation, input_parts, output_parts, skip_scale, decay_shift, sink_logit, out_state, out_attend):
    length = inputs.shape[0]
    widened = inputs.astype(jnp.float32)
    scale = lax.rsqrt(lax.optimization_barrier(jnp.mean(widened * widened, axis=1, keepdims=True)) + epsilon)
    normed = (widened * scale * norm_gain.astype(jnp.float32)).astype(jnp.bfloat16)
    drive_in = jnp.dot(normed, in_ssm, preferred_element_type=jnp.float32).astype(jnp.bfloat16)
    queries = jnp.dot(normed, in_query, preferred_element_type=jnp.float32).astype(jnp.bfloat16)
    keys_local = jnp.dot(normed, in_key, preferred_element_type=jnp.float32).astype(jnp.bfloat16)
    values = jnp.dot(normed, in_value, preferred_element_type=jnp.float32).astype(jnp.bfloat16)
    in_matrix = input_matrix(decay_rate, rotation, input_parts)
    blocks = length // BLOCK
    grouped = drive_in.reshape(blocks, BLOCK, GROUPS, GROUP_CH)
    shifted = decay_shift.reshape(blocks, BLOCK, GROUPS)

    def advance(carry, pieces):
        grouped_part, shift_part = pieces
        drive = jnp.einsum('tgh,gqh->tgq', grouped_part.astype(jnp.float32), in_matrix.astype(jnp.float32))
        return advance_block(carry, drive, shift_part, grouped_part, decay_rate, rotation, output_parts, skip_scale)
    zero_state = jnp.zeros((GROUPS, STATE), jnp.float32)
    _, state_out = lax.scan(advance, (zero_state, zero_state), (grouped, shifted))
    state_out = state_out.reshape(length, GROUPS * GROUP_CH)
    windows_all = length // WINDOW
    per_device = TOK_DEV // WINDOW
    filler = jnp.zeros((WINDOW, KV_HEADS * HEAD_DIM), jnp.bfloat16)

    def windows(flat):
        split = jnp.concatenate([filler, flat], axis=0).reshape(windows_all + 1, WINDOW, KV_HEADS, HEAD_DIM)
        joined = jnp.concatenate([split[:-1], split[1:]], axis=1)
        return joined.reshape(N_SP, per_device, 2 * WINDOW, KV_HEADS, HEAD_DIM)
    queries_blk = queries.reshape(N_SP, per_device, WINDOW, KV_HEADS, Q_HEADS // KV_HEADS, HEAD_DIM)
    starts = (jnp.arange(windows_all, dtype=jnp.int32) * WINDOW).reshape(N_SP, per_device)
    attended = lax.map(lambda pieces: window_attention(pieces[0], pieces[1], pieces[2], pieces[3], sink_logit), (queries_blk, windows(keys_local), windows(values), starts))
    attend_out = attended.reshape(length, Q_HEADS * HEAD_DIM)
    summed = jnp.dot(state_out, out_state, preferred_element_type=jnp.float32)
    summed = summed + jnp.dot(attend_out, out_attend, preferred_element_type=jnp.float32)
    return summed.astype(jnp.bfloat16)
```

```python
import functools
import jax
import jax.numpy as jnp
from jax import lax
from jax.experimental import pallas as pl
from jax.experimental.pallas import tpu as pltpu
from jax.sharding import PartitionSpec as P

GROUP_CH = 16
HEAD_DIM = 64
WINDOW = 128
BLOCK = 128


epsilon = 1e-06
floor_score = -1e30


def prefix(x, axis, join, neutral):
    place = lax.axis_index(axis)
    gathered = jax.tree.map(
        lambda a, kind: lax.all_gather(a.astype(kind), axis),
        x,
        (jnp.bfloat16, jnp.bfloat16, jnp.bfloat16, jnp.bfloat16),
    )
    state = jax.tree.map(lambda a, e: jnp.zeros_like(a) + jnp.asarray(e, a.dtype), x, neutral)

    def one(hop, state):
        return join(
            state,
            jax.tree.map(
                lambda a, own: lax.dynamic_index_in_dim(a, hop, 0, False).astype(own.dtype),
                gathered,
                x,
            ),
        )

    return lax.fori_loop(0, place, one, state)


def from_behind(value, axis, steps):
    count = lax.axis_size(axis)
    initial, last = (max(0, -steps), min(count, count - steps))
    return lax.ppermute(value, axis, [(source, source + steps) for source in range(initial, last)])


def combine(earlier, later):
    first_re, first_im, state_re, state_im = earlier
    second_re, second_im, input_re, input_im = later
    return (
        second_re * first_re - second_im * first_im,
        second_re * first_im + second_im * first_re,
        second_re * state_re - second_im * state_im + input_re,
        second_re * state_im + second_im * state_re + input_im,
    )


def input_matrix(decay_rate, rotation, input_parts):
    damped = jnp.exp(-decay_rate)
    lift_re = damped * jnp.cos(rotation) - 1.0
    lift_im = damped * jnp.sin(rotation)
    modulus = decay_rate * decay_rate + rotation * rotation
    factor_re = (rotation * lift_im - decay_rate * lift_re) / modulus
    factor_im = -(rotation * lift_re + decay_rate * lift_im) / modulus
    part_re = input_parts[0].astype(jnp.float32)
    part_im = input_parts[1].astype(jnp.float32)
    joined_re = factor_re[:, :, None] * part_re - factor_im[:, :, None] * part_im
    joined_im = factor_re[:, :, None] * part_im + factor_im[:, :, None] * part_re
    return jnp.concatenate([joined_re, joined_im], axis=1).astype(jnp.bfloat16)


def window_attention(queries, keys_win, values_win, starts, sink_logit):
    window = queries.shape[1]
    scores = jnp.einsum("nqgrd,nkgd->ngrqk", queries, keys_win, preferred_element_type=jnp.float32)
    scores = scores * queries.shape[-1] ** (-0.5)
    places = (
        jnp.arange(window, dtype=jnp.int32)[:, None]
        + window
        - jnp.arange(2 * window, dtype=jnp.int32)[None, :]
    )
    inside = (places >= 0) & (places < window)
    reach = starts[:, None] - window + jnp.arange(2 * window, dtype=jnp.int32)[None, :] >= 0
    valid = (inside[None] & reach[:, None, :])[:, None, None]
    sinks = sink_logit.reshape(scores.shape[1], scores.shape[2])[None, :, :, None, None]
    scores = jnp.where(valid, scores, floor_score)
    row_peak = jnp.maximum(jnp.max(scores, axis=-1, keepdims=True), sinks)
    raised = jnp.where(valid, jnp.exp(scores - row_peak), 0.0)
    denominator = jnp.sum(raised, axis=-1, keepdims=True) + jnp.exp(sinks - row_peak)
    weights = (raised / denominator).astype(jnp.bfloat16)
    result = jnp.einsum(
        "ngrqk,nkgd->nqgrd", weights, values_win, preferred_element_type=jnp.float32
    )
    return result.astype(jnp.bfloat16)


def general_body(
    inputs,
    norm_gain,
    in_ssm,
    in_query,
    in_key,
    in_value,
    decay_rate,
    rotation,
    input_parts,
    output_parts,
    skip_scale,
    decay_shift,
    sink_logit,
    out_state,
    out_attend,
):
    gathered = lax.all_gather(inputs, "tp", axis=1, tiled=True)
    length = gathered.shape[0]
    widened = gathered.astype(jnp.float32)
    scale = lax.rsqrt(jnp.mean(widened * widened, axis=1, keepdims=True) + epsilon)
    normed = (widened * scale * norm_gain).astype(jnp.bfloat16)

    def add_rows(pieces):
        return tuple(
            (jnp.dot(normed, piece, preferred_element_type=jnp.float32) for piece in pieces)
        )

    projected = add_rows(
        (
            lax.all_gather(in_ssm, "sp", axis=0, tiled=True),
            lax.all_gather(in_query, "sp", axis=0, tiled=True),
            lax.all_gather(in_key, "sp", axis=0, tiled=True),
            lax.all_gather(in_value, "sp", axis=0, tiled=True),
        )
    )
    drive_in, queries, keys_local, values = [piece.astype(jnp.bfloat16) for piece in projected]
    groups = decay_rate.shape[0]
    state_dim = decay_rate.shape[1]
    channels = groups * GROUP_CH
    highest = lax.Precision.HIGHEST
    drive_cols = jnp.transpose(drive_in).reshape(groups, GROUP_CH, length)
    in_matrix = input_matrix(decay_rate, rotation, input_parts)
    drive = jnp.einsum("gqh,ght->gqt", in_matrix, drive_cols, preferred_element_type=jnp.float32)
    shift_cols = jnp.transpose(decay_shift)
    running = jnp.cumsum(shift_cols, axis=1)
    total_shift = running[:, -1]
    remain = length - 1.0 - jnp.arange(length, dtype=jnp.float32)
    to_end = (total_shift[:, None] - running)[:, None, :] - decay_rate[:, :, None] * remain[
        None, None, :
    ]
    fade = jnp.exp(to_end)
    turn = rotation[:, :, None] * remain[None, None, :]
    weight_re = fade * jnp.cos(turn)
    weight_im = fade * jnp.sin(turn)
    drive_re = drive[:, :state_dim]
    drive_im = drive[:, state_dim:]
    final_re = jnp.sum(weight_re * drive_re - weight_im * drive_im, axis=2)
    final_im = jnp.sum(weight_re * drive_im + weight_im * drive_re, axis=2)
    overall = jnp.exp(total_shift[:, None] - decay_rate * length)
    nothing = jnp.zeros_like(final_re)
    carried = prefix(
        (
            overall * jnp.cos(rotation * length),
            overall * jnp.sin(rotation * length),
            final_re,
            final_im,
        ),
        "sp",
        combine,
        (jnp.ones_like(final_re), nothing, nothing, nothing),
    )
    key_heads = keys_local.shape[1] // HEAD_DIM
    query_heads = queries.shape[1] // HEAD_DIM
    windows_dev = length // WINDOW
    previous = from_behind((keys_local, values), "sp", 1)

    def windows(flat, before):
        split = jnp.concatenate([before, flat], axis=0).reshape(
            windows_dev + 1, WINDOW, key_heads, HEAD_DIM
        )
        return jnp.concatenate([split[:-1], split[1:]], axis=1)

    offset = lax.axis_index("sp") * length
    starts = offset + jnp.arange(windows_dev, dtype=jnp.int32) * WINDOW
    queries_blk = queries.reshape(
        windows_dev, WINDOW, key_heads, query_heads // key_heads, HEAD_DIM
    )
    attended = window_attention(
        queries_blk,
        windows(keys_local, previous[0]),
        windows(values, previous[1]),
        starts,
        sink_logit,
    )
    attend_out = attended.reshape(length, query_heads * HEAD_DIM)
    blocks = length // BLOCK
    triangle = (
        jnp.arange(BLOCK, dtype=jnp.int32)[:, None] <= jnp.arange(BLOCK, dtype=jnp.int32)[None, :]
    ).astype(jnp.float32)
    offsets = jnp.arange(BLOCK, dtype=jnp.float32)
    centre = BLOCK // 2
    read_re = output_parts[0].astype(jnp.float32)
    read_im = output_parts[1].astype(jnp.float32)
    angle = rotation[:, :, None] * (offsets - centre)[None, None, :]
    cos_angle = jnp.cos(angle)
    sin_angle = jnp.sin(angle)
    phase = rotation[:, :, None] * (offsets + 1.0)[None, None, :]
    cos_phase = jnp.cos(phase)
    sin_phase = jnp.sin(phase)

    def advance(carry, pieces):
        carry_re, carry_im = carry
        part_re, part_im, shift_part, grouped_part = pieces
        level = jnp.dot(shift_part, triangle, precision=highest)
        log_from = level[:, None, :] - decay_rate[:, :, None] * (offsets + 1.0)[None, None, :]
        relative = log_from - log_from[:, :, centre : centre + 1]
        shrink = jnp.exp(-relative)
        lift_re = shrink * (part_re * cos_angle + part_im * sin_angle)
        lift_im = shrink * (part_im * cos_angle - part_re * sin_angle)
        prefix_re = jnp.dot(lift_re.reshape(groups * state_dim, BLOCK), triangle, precision=highest)
        prefix_im = jnp.dot(lift_im.reshape(groups * state_dim, BLOCK), triangle, precision=highest)
        prefix_re = prefix_re.reshape(groups, state_dim, BLOCK)
        prefix_im = prefix_im.reshape(groups, state_dim, BLOCK)
        grow = jnp.exp(relative)
        from_start = jnp.exp(log_from)
        keep_re = from_start * cos_phase
        keep_im = from_start * sin_phase
        state_re = grow * (prefix_re * cos_angle - prefix_im * sin_angle)
        state_im = grow * (prefix_im * cos_angle + prefix_re * sin_angle)
        state_re = state_re + keep_re * carry_re[:, :, None] - keep_im * carry_im[:, :, None]
        state_im = state_im + keep_re * carry_im[:, :, None] + keep_im * carry_re[:, :, None]
        result = jnp.einsum("ghp,gpt->ght", read_re, state_re, precision=highest)
        result = result - jnp.einsum("ghp,gpt->ght", read_im, state_im, precision=highest)
        result = result + skip_scale[:, :, None] * grouped_part.astype(jnp.float32)
        return ((state_re[:, :, -1], state_im[:, :, -1]), jax.nn.gelu(result).astype(jnp.bfloat16))

    drive_blocks = jnp.transpose(drive.reshape(groups, 2 * state_dim, blocks, BLOCK), (2, 0, 1, 3))
    shift_blocks = jnp.transpose(shift_cols.reshape(groups, blocks, BLOCK), (1, 0, 2))
    grouped_blocks = jnp.transpose(
        drive_cols.reshape(groups, GROUP_CH, blocks, BLOCK), (2, 0, 1, 3)
    )
    _, state_blocks = lax.scan(
        advance,
        (carried[2], carried[3]),
        (
            drive_blocks[:, :, :state_dim],
            drive_blocks[:, :, state_dim:],
            shift_blocks,
            grouped_blocks,
        ),
    )
    state_out = jnp.transpose(state_blocks, (0, 3, 1, 2)).reshape(length, channels)
    column_state, column_attend = (
        lax.all_gather(out_state, "sp", axis=1, tiled=True),
        lax.all_gather(out_attend, "sp", axis=1, tiled=True),
    )
    result = jnp.dot(state_out, column_state, preferred_element_type=jnp.float32)
    return lax.psum_scatter(
        (result + jnp.dot(attend_out, column_attend, preferred_element_type=jnp.float32)).astype(
            jnp.bfloat16
        ),
        "tp",
        scatter_dimension=0,
        tiled=True,
    )


MESH = pl.DeviceIdType.MESH
ANY = pl.BlockSpec(memory_space=pl.ANY)


def remote(src, dst, send, recv, **where):
    return pltpu.make_async_remote_copy(
        src_ref=src, dst_ref=dst, send_sem=send, recv_sem=recv, device_id=where, device_id_type=MESH
    )


def greet(peers):
    barrier = pltpu.get_barrier_semaphore()
    for peer in peers:
        pl.semaphore_signal(barrier, inc=1, device_id=peer, device_id_type=MESH)
    pl.semaphore_wait(barrier, len(peers))


def halves(x):
    high = x.astype(jnp.bfloat16)
    return high, (x - high.astype(jnp.float32)).astype(jnp.bfloat16)


def split_dot(x, exact):
    high, low = halves(x)
    return jnp.dot(high, exact, preferred_element_type=jnp.float32) + jnp.dot(
        low, exact, preferred_element_type=jnp.float32
    )


def column(row):
    size = row.shape[1]
    same = lax.broadcasted_iota(jnp.int32, (size, size), 0) == lax.broadcasted_iota(
        jnp.int32, (size, size), 1
    )
    return jnp.sum(jnp.where(same, row, 0.0), axis=1, keepdims=True)


def layer_kernel(x_in, gain_in, ssm, query, key_in, value_in, rate_in, turn_in, parts_in, reads_in,
                 skip_in, shift_in, sinks_in, ows, owa, out,
                 xf, normed, w_ssm, w_query, w_kv, wo_s, wo_a, key, value, pairs, gain, rate, turn,
                 parts, reads, skip, shift, sinks, tab, inm, read, lifts, grows, prefix, u_scr, q_scr,
                 kv_scr, y_scr, act_s, act_a, carry_out, carry_in, pf, pb, got, fsend, fgot, res,
                 loc, z_s, z_r, p_s, p_r, ax_s, ax_r, ay_s, ay_r, bx_s, bx_r, by_s, by_r,
                 d_s, d_r, e_s, e_r, o_s):
    f32, bf = jnp.float32, jnp.bfloat16
    k, f, t = lax.axis_index("sp"), lax.axis_index("fs"), lax.axis_index("tp")
    n, n_fs = 4, 4
    tokens, half = x_in.shape
    rows, cols = ssm.shape[0], ows.shape[1]
    wide = w_ssm.shape[1]
    groups, state = tab.shape[0], tab.shape[2]
    heads = w_query.shape[1] // HEAD_DIM
    par, late = lax.rem(k, 2), lax.div(k, 2)
    pair = k + 1 - 2 * par
    order = (pair, 2 - late, 3 - 3 * late)
    other = 1 - t
    fx, fy = f + 1 - 2 * lax.rem(f, 2), lax.rem(f + 2, n_fs)
    greet([{"sp": j} for j in order] + [{"fs": fx}, {"fs": fy}, {"tp": other}])

    part, height = rows // n_fs, wide // n_fs
    into = (w_ssm, w_query, w_kv, wo_s, wo_a)

    def region(w, j, q, side=None):
        size = part if w < 3 else height
        first = q * size
        if side is not None:
            size //= 2
            first = first + side * size
        if w < 3:
            return into[w].at[pl.ds(pl.multiple_of(j * rows + first, 16), size)]
        return into[w].at[pl.ds(pl.multiple_of(first, 16), size), pl.ds(pl.multiple_of(j * cols, 128), cols)]

    def piece(w, peer):
        kind = lax.rem(peer, 2)
        mine = pl.ds(pl.multiple_of(f * part, 16), part)
        if w == 2:
            return pairs.at[kind, mine]
        if w < 2:
            return (ssm, query)[w].at[mine, pl.ds(pl.multiple_of(kind * wide, 128), wide)]
        return (ows, owa)[w - 3].at[pl.ds(pl.multiple_of(kind * wide + f * height, 16), height)]

    sent = []

    def launch(c):
        c.start()
        sent.append(c)

    def over_z(w, peer):
        launch(remote(piece(w, peer), region(w, k, f), z_s.at[w, peer], z_r.at[w, k], sp=peer))

    def x_at(e, side):
        return xf.at[pl.ds(pl.multiple_of(e * tokens, 128), tokens), pl.ds(pl.multiple_of(side * half, 128), half)]

    def shift_at(e):
        return shift.at[:, pl.ds(pl.multiple_of(e * tokens, 128), tokens)]

    def shift_rows(e):
        return shift_in.at[pl.ds(pl.multiple_of(e * groups, 8), groups)]

    def z_here(w, j):
        block = region(w, j, f)
        remote(block, block, z_s.at[w, j], z_r.at[w, j], sp=j).wait_recv()
        for side in (0, 1):
            a = region(w, j, f, side)
            launch(remote(a, a, ax_s.at[w, j, side], ax_r.at[w, j, side], fs=fx))
            b = region(w, j, f, 1 - side)
            launch(remote(b, b, ay_s.at[w, j, 1 - side], ay_r.at[w, j, 1 - side], fs=fy))

    def relay(w, j):
        a = region(w, j, fx, 0)
        remote(a, a, ax_s.at[w, j, 0], ax_r.at[w, j, 0], fs=fx).wait_recv()
        launch(remote(a, a, by_s.at[w, j], by_r.at[w, j], fs=fy))
        b = region(w, j, fy, 1)
        remote(b, b, ay_s.at[w, j, 1], ay_r.at[w, j, 1], fs=fy).wait_recv()
        launch(remote(b, b, bx_s.at[w, j], bx_r.at[w, j], fs=fx))

    def complete(w, j):
        a = region(w, j, fx, 1)
        remote(a, a, ax_s.at[w, j, 1], ax_r.at[w, j, 1], fs=fx).wait_recv()
        b = region(w, j, fy, 0)
        remote(b, b, ay_s.at[w, j, 0], ay_r.at[w, j, 0], fs=fy).wait_recv()
        far = n_fs - 1 - f
        a = region(w, j, far, 0)
        remote(a, a, by_s.at[w, j], by_r.at[w, j], fs=fy).wait_recv()
        b = region(w, j, far, 1)
        remote(b, b, bx_s.at[w, j], bx_r.at[w, j], fs=fx).wait_recv()

    def steps_of(ws):
        steps = []
        waiting = []
        for j in order:
            for w in ws:
                steps.append(functools.partial(z_here, w, j))
                if waiting:
                    steps.append(waiting.pop(0))
                waiting.append(functools.partial(relay, w, j))
        return steps + waiting

    queue = steps_of((0,))

    def pump(count):
        for _ in range(count):
            if queue:
                queue.pop(0)()

    for peer in order:
        over_z(0, peer)
    launch(remote(x_in, x_at(par, t), p_s.at[0], p_r.at[0], sp=pair))
    launch(remote(x_in, x_at(par, t), p_s.at[2], p_r.at[2], tp=other))
    launch(remote(shift_rows(1 - par), shift_at(par), p_s.at[1], p_r.at[1], sp=pair))
    for peer in order:
        over_z(1, peer)
    everything = pl.ds(0, rows)
    here = pl.ds(pl.multiple_of(k * rows, 16), rows)
    mine = pl.ds(pl.multiple_of(par * wide, 128), wide)
    columns = pl.ds(pl.multiple_of(k * cols, 128), cols)
    local = [
        (key_in, key), (value_in, value), (rate_in, rate), (turn_in, turn), (parts_in, parts),
        (reads_in, reads), (skip_in, skip), (gain_in, gain), (sinks_in, sinks),
        (shift_rows(par), shift_at(par)), (x_in, x_at(par, t)),
        (ssm.at[everything, mine], w_ssm.at[here]), (query.at[everything, mine], w_query.at[here]),
        (ows.at[mine], wo_s.at[:, columns]), (owa.at[mine], wo_a.at[:, columns]),
    ]
    local = [pltpu.make_async_copy(a, b, loc.at[i]) for i, (a, b) in enumerate(local)]
    for c in local:
        c.start()
    local[0].wait()
    local[1].wait()
    for e in range(2):
        span = slice(e * HEAD_DIM, (e + 1) * HEAD_DIM)
        pairs[e] = jnp.concatenate([key[:, span], value[:, span]], axis=1)
    w_kv[here, :] = pairs[par]
    for c in local[2:11]:
        c.wait()
    first = par * groups

    def tables(g, columns_of):
        line, spin = rate[pl.ds(first + g, 1), :], turn[pl.ds(first + g, 1), :]
        rates, turns = column(line), column(spin)
        away = lax.broadcasted_iota(jnp.int32, (state, BLOCK), 1).astype(f32) - float(BLOCK // 2)
        angle = turns * away
        cos, sin = jnp.cos(angle), jnp.sin(angle)
        fade = jnp.exp(-rates * away)
        rise = jnp.exp(rates * away)
        tab[g, 0] = rise * cos
        tab[g, 1] = -(rise * sin)
        tab[g, 2] = fade * cos
        tab[g, 3] = fade * sin
        damped = jnp.exp(-line)
        lift_re = damped * jnp.cos(spin) - 1.0
        lift_im = damped * jnp.sin(spin)
        modulus = line * line + spin * spin
        factor_re = (spin * lift_im - line * lift_re) / modulus
        factor_im = -(spin * lift_re + line * lift_im) / modulus
        part_re = parts[0, first + g].astype(f32)
        part_im = parts[1, first + g].astype(f32)
        inm[g] = jnp.transpose(
            jnp.concatenate(
                [factor_re * part_re - factor_im * part_im, factor_re * part_im + factor_im * part_re],
                axis=1,
            )
        ).astype(bf)
        read[g] = jnp.concatenate(
            [reads[0, first + g].astype(f32), -reads[1, first + g].astype(f32)], axis=1
        ).astype(bf)
        spot = lax.broadcasted_iota(jnp.int32, (state, BLOCK), 1) == g
        return jnp.where(spot, rates, columns_of[0]), jnp.where(spot, turns, columns_of[1])

    columns_of = (jnp.zeros((state, BLOCK), f32), jnp.zeros((state, BLOCK), f32))
    quarter = groups // 4
    columns_of = lax.fori_loop(0, quarter, tables, columns_of)
    for i, peer in enumerate(order):
        over_z(2, peer)
    for peer in order:
        over_z(3, peer)
        over_z(4, peer)
    pump(2)
    columns_of = lax.fori_loop(quarter, 2 * quarter, tables, columns_of)
    pump(2)

    def normalize(e):
        block = pl.ds(pl.multiple_of(e * tokens, 128), tokens)
        full = xf[block, :].astype(f32)
        scale = lax.rsqrt(jnp.mean(full * full, axis=1, keepdims=True) + epsilon)
        normed[block, :] = (full * scale * gain[...]).astype(bf)

    theirs = x_at(par, other)
    remote(theirs, theirs, p_s.at[2], p_r.at[2], tp=other).wait_recv()
    normalize(par)
    columns_of = lax.fori_loop(2 * quarter, 3 * quarter, tables, columns_of)
    pump(1)
    columns_of = lax.fori_loop(3 * quarter, groups, tables, columns_of)
    pump(len(queue))
    queue += steps_of((1, 2))
    next_x = x_at(1 - par, t)
    remote(next_x, next_x, p_s.at[0], p_r.at[0], sp=pair).wait_recv()
    launch(remote(next_x, next_x, p_s.at[3], p_r.at[3], tp=other))
    near = shift_at(1 - par)
    remote(near, near, p_s.at[1], p_r.at[1], sp=pair).wait_recv()

    shape = (BLOCK, BLOCK)
    upto = lax.broadcasted_iota(jnp.int32, shape, 0) <= lax.broadcasted_iota(jnp.int32, shape, 1)
    tri = upto.astype(f32).astype(bf)
    centre = BLOCK // 2
    eye = lax.broadcasted_iota(jnp.int32, (groups, BLOCK), 0) == lax.broadcasted_iota(
        jnp.int32, (groups, BLOCK), 1
    )

    def across(col):
        return jnp.sum(jnp.where(eye, col, 0.0), axis=0, keepdims=True)

    begins, lasts = [], []
    for b in range(2):
        piece_b = shift[:, b * BLOCK : (b + 1) * BLOCK]
        high, low = halves(piece_b)
        low2 = (piece_b - high.astype(f32) - low.astype(f32)).astype(bf)
        level = (
            jnp.dot(high, tri, preferred_element_type=f32)
            + jnp.dot(low, tri, preferred_element_type=f32)
            + jnp.dot(low2, tri, preferred_element_type=f32)
        )
        middle = level[:, centre : centre + 1]
        lifts[b] = jnp.exp(middle - level)
        grown = jnp.exp(level - middle)
        grows[b] = grown
        begins.append(across(jnp.exp(middle)))
        lasts.append(across(grown[:, BLOCK - 1 :]))
    rates, turns = columns_of

    def times(a, b):
        return a[0] * b[0] - a[1] * b[1], a[0] * b[1] + a[1] * b[0]

    def plus(a, b):
        return a[0] + b[0], a[1] + b[1]

    def scaled(row, a):
        return row * a[0], row * a[1]

    def spiral(count):
        fade = jnp.exp(-rates * count)
        return fade * jnp.cos(turns * count), fade * jnp.sin(turns * count)

    reach, end = spiral(centre + 1.0), spiral(BLOCK - 1.0 - centre)
    whole = times(reach, end)

    theirs = x_at(1 - par, other)
    remote(theirs, theirs, p_s.at[3], p_r.at[3], tp=other).wait_recv()
    normalize(1 - par)
    local[11].wait()
    for j in order:
        complete(0, j)
    u = jnp.dot(normed[...], w_ssm[...], preferred_element_type=f32)
    u_scr[...] = jnp.transpose(u.astype(bf).astype(f32))

    lane = lax.broadcasted_iota(jnp.int32, (state, BLOCK), 1)
    ends = [jnp.zeros((state, BLOCK), f32)] * 4
    for g in range(groups):
        u = u_scr[g * GROUP_CH : (g + 1) * GROUP_CH, :]
        drive = jnp.dot(inm[g], u.astype(bf), preferred_element_type=f32)
        up_re, up_im = tab[g, 0], tab[g, 1]
        lifted = []
        for b in range(2):
            span = slice(b * BLOCK, (b + 1) * BLOCK)
            row = lifts[b, g : g + 1, :]
            d_re, d_im = drive[:state, span] * row, drive[state:, span] * row
            lifted += [d_re * up_re - d_im * up_im, d_re * up_im + d_im * up_re]
        sums = split_dot(jnp.concatenate(lifted, axis=0), tri)
        prefix[g] = sums
        ends = [
            jnp.where(lane == g, sums[i * state : (i + 1) * state, BLOCK - 1 :], ends[i])
            for i in range(4)
        ]
        if g % 2 == 1:
            pump(2)
    pump(len(queue))
    queue += steps_of((3, 4))
    own = [scaled(lasts[b], times(end, (ends[2 * b], ends[2 * b + 1]))) for b in range(2)]
    decay = [scaled(lasts[b] * begins[b], whole) for b in range(2)]
    final = plus(own[1], times(decay[1], own[0]))
    carry_out[...] = jnp.transpose(jnp.concatenate(final, axis=0))[:groups]

    local[12].wait()
    for w in (1, 2):
        for j in order:
            complete(w, j)
    kv_scr[WINDOW:, :] = jnp.dot(normed[...], w_kv[...], preferred_element_type=f32).astype(bf)
    q_scr[...] = jnp.dot(normed[...], w_query[...], preferred_element_type=f32).astype(bf)
    ahead, behind = lax.rem(k + 2, n), lax.rem(k + 2, n)
    tail = kv_scr.at[pl.ds(2 * WINDOW, WINDOW)]
    head = kv_scr.at[pl.ds(0, WINDOW)]
    hand_kv = remote(tail, head, p_s.at[4], p_r.at[4], sp=ahead)
    hand_state = remote(carry_out, carry_in, p_s.at[5], p_r.at[5], sp=ahead)

    @pl.when(late == 0)
    def _():
        hand_kv.start()
        hand_state.start()
        kv_scr[:WINDOW, :] = jnp.zeros((WINDOW, kv_scr.shape[1]), bf)
        carry_in[...] = jnp.zeros(carry_in.shape, f32)

    gap_shape = (WINDOW, 2 * WINDOW)
    at = lax.broadcasted_iota(jnp.int32, gap_shape, 1)
    gap = lax.broadcasted_iota(jnp.int32, gap_shape, 0) + WINDOW - at
    inside = (gap >= 0) & (gap < WINDOW)
    inside_first = inside & (at >= WINDOW * (1 - late))
    sink_lane = lax.broadcasted_iota(jnp.int32, sinks.shape, 1)
    for b in (1, 0):
        if b == 0:

            @pl.when(late == 1)
            def _():
                hand_kv.wait_recv()
                hand_state.wait_recv()

        keys = kv_scr[b * WINDOW : (b + 2) * WINDOW, :HEAD_DIM]
        values = kv_scr[b * WINDOW : (b + 2) * WINDOW, HEAD_DIM:]
        valid = inside if b else inside_first
        outs = []
        for h in range(heads):
            q = q_scr[b * WINDOW : (b + 1) * WINDOW, h * HEAD_DIM : (h + 1) * HEAD_DIM]
            scores = lax.dot_general(q, keys, (((1,), (1,)), ((), ())), preferred_element_type=f32)
            scores = jnp.where(valid, scores * HEAD_DIM ** (-0.5), floor_score)
            sink = jnp.sum(jnp.where(sink_lane == par * heads + h, sinks[...], 0.0), axis=1, keepdims=True)
            peak = jnp.maximum(jnp.max(scores, axis=1, keepdims=True), sink)
            raised = jnp.where(valid, jnp.exp(scores - peak), 0.0)
            total = jnp.sum(raised, axis=1, keepdims=True) + jnp.exp(sink - peak)
            weights = (raised / total).astype(bf)
            outs.append(jnp.dot(weights, values, preferred_element_type=f32))
            if h % 2:
                pump(2)
        act_a[b * BLOCK : (b + 1) * BLOCK, :] = jnp.concatenate(outs, axis=1).astype(bf)

    back = jnp.transpose(carry_in[...])
    entry = (back[:state], back[state:])

    def bases(row, c):
        return scaled(row, times(c, reach))

    def grown_entry(c):
        return plus((own[0][0][:, :groups], own[0][1][:, :groups]),
                    times((decay[0][0][:, :groups], decay[0][1][:, :groups]), c))

    cut = (reach[0][:, :groups], reach[1][:, :groups])
    base = [
        scaled(begins[0][:, :groups], times(entry, cut)),
        scaled(begins[1][:, :groups], times(grown_entry(entry), cut)),
    ]
    for g in range(groups):
        u = u_scr[g * GROUP_CH : (g + 1) * GROUP_CH, :]
        down = (tab[g, 2], tab[g, 3])
        chosen = lax.broadcasted_iota(jnp.int32, skip.shape, 1) == first + g
        skips = jnp.sum(jnp.where(chosen, skip[...], 0.0), axis=1, keepdims=True)
        states = []
        for b in range(2):
            at_re = slice(2 * b * state, (2 * b + 1) * state)
            at_im = slice((2 * b + 1) * state, (2 * b + 2) * state)
            p = (prefix[g, at_re] + base[b][0][:, g : g + 1], prefix[g, at_im] + base[b][1][:, g : g + 1])
            states.append(jnp.concatenate(scaled(grows[b, g : g + 1, :], times(down, p)), axis=0))
        high, low = halves(jnp.concatenate(states, axis=1))
        y = jnp.dot(read[g], high, preferred_element_type=f32) + jnp.dot(
            read[g], low, preferred_element_type=f32
        )
        y_scr[g * GROUP_CH : (g + 1) * GROUP_CH, :] = y + skips * u
        if g % 2 == 1:
            pump(2)
    act_s[...] = jnp.transpose(jax.nn.gelu(y_scr[...])).astype(bf)
    pump(len(queue))

    for c in local[13:]:
        c.wait()

    def blocks_of(j):
        return pl.ds(pl.multiple_of(j * cols, 128), cols)

    def multiply(j):
        here = blocks_of(j)
        total = jnp.dot(act_s[...], wo_s[:, here], preferred_element_type=f32) + jnp.dot(
            act_a[...], wo_a[:, here], preferred_element_type=f32
        )
        size = tokens // 2
        for e in range(2):
            for side in range(2):
                block = total[e * tokens + side * size : e * tokens + (side + 1) * size]
                pf[j, e, side] = block
                pb[j, side, e] = block.astype(bf)
        launch(remote(pb.at[j, other], got.at[j], d_s.at[j], d_r.at[j], tp=other))

    def pass_on(j):
        remote(got.at[j], got.at[j], d_s.at[j], d_r.at[j], tp=other).wait_recv()
        fsend[j] = (pf[j, 1 - par, t] + got[j, 1 - par].astype(f32)).astype(bf)
        launch(remote(fsend.at[j], fgot.at[j], e_s.at[j], e_r.at[j], sp=pair))

    def settle(j):
        remote(fgot.at[j], fgot.at[j], e_s.at[j], e_r.at[j], sp=pair).wait_recv()
        total = pf[j, par, t] + got[j, par].astype(f32) + fgot[j].astype(f32)
        res[:, blocks_of(j)] = total.astype(bf)
        launch(pltpu.make_async_copy(res.at[:, blocks_of(j)], out.at[:, blocks_of(j)], o_s.at[j]))

    line = (k,) + order
    for i, j in enumerate(line):
        if i:
            complete(3, j)
            complete(4, j)
        multiply(j)
        if i:
            pass_on(line[i - 1])
    pass_on(line[-1])
    settle(pair)
    settle(k)
    for j in line[2:]:
        settle(j)

    for c in sent:
        if c.is_remote:
            c.wait_send()
        else:
            c.wait()

    @pl.when(late == 0)
    def _():
        hand_kv.wait_send()
        hand_state.wait_send()


def layer(x, gain, ssm, query, key, value, rate, turn, parts, reads, skip, shift, sinks, ows, owa):
    bf, f32 = jnp.bfloat16, jnp.float32
    tokens, half = x.shape
    rows, cols = ows.shape[0], ows.shape[1]
    depth = 4 * ssm.shape[0]
    wide = ssm.shape[1] // 2
    groups, state = rate.shape[0] // 2, rate.shape[1]
    length = 2 * tokens
    dma = pltpu.SemaphoreType.DMA
    vm = pltpu.VMEM
    return pl.pallas_call(
        layer_kernel,
        out_shape=jax.ShapeDtypeStruct((tokens // 2, 4 * cols), bf),
        in_specs=[ANY] * 15,
        out_specs=ANY,
        scratch_shapes=[
            vm((length, 2 * half), bf), vm((length, 2 * half), bf),
            vm((depth, wide), bf), vm((depth, wide), bf), vm((depth, 2 * HEAD_DIM), bf),
            vm((wide, 4 * cols), bf), vm((wide, 4 * cols), bf),
            vm(key.shape, bf), vm(value.shape, bf), vm((2, key.shape[0], 2 * HEAD_DIM), bf),
            vm(gain.shape, f32), vm(rate.shape, f32), vm(turn.shape, f32),
            vm(parts.shape, bf), vm(reads.shape, bf), vm(skip.shape, f32),
            vm((groups, length), f32), vm(sinks.shape, f32),
            vm((groups, 4, state, BLOCK), f32), vm((groups, 2 * state, GROUP_CH), bf),
            vm((groups, GROUP_CH, 2 * state), bf), vm((2, groups, BLOCK), f32), vm((2, groups, BLOCK), f32),
            vm((groups, 4 * state, BLOCK), f32), vm((wide, length), f32), vm((length, wide), bf),
            vm((length + WINDOW, 2 * HEAD_DIM), bf), vm((wide, length), f32),
            vm((length, wide), bf), vm((length, wide), bf),
            vm((groups, 2 * state), f32), vm((groups, 2 * state), f32),
            vm((4, 2, 2, tokens // 2, cols), f32), vm((4, 2, 2, tokens // 2, cols), bf),
            vm((4, 2, tokens // 2, cols), bf), vm((4, tokens // 2, cols), bf), vm((4, tokens // 2, cols), bf),
            vm((tokens // 2, 4 * cols), bf),
            dma((15,)), dma((5, 4)), dma((5, 4)), dma((6,)), dma((6,)),
            dma((5, 4, 2)), dma((5, 4, 2)), dma((5, 4, 2)), dma((5, 4, 2)),
            dma((5, 4)), dma((5, 4)), dma((5, 4)), dma((5, 4)),
            dma((4,)), dma((4,)), dma((4,)), dma((4,)), dma((4,)),
        ],
        compiler_params=pltpu.CompilerParams(collective_id=0, has_side_effects=True),
    )(x, gain, ssm, query, key, value, rate, turn, parts, reads, skip, shift, sinks, ows, owa)


def fast_body(
    inputs, norm_gain, in_ssm, in_query, in_key, in_value, decay_rate, rotation, input_parts,
    output_parts, skip_scale, decay_shift, sink_logit, out_state, out_attend,
):
    return layer(
        inputs, norm_gain[None], in_ssm, in_query, in_key, in_value, decay_rate, rotation,
        jnp.swapaxes(input_parts, 2, 3), output_parts, skip_scale.T, jnp.transpose(decay_shift),
        sink_logit[None], out_state, out_attend,
    )


def body(*args):
    n, n_fs, n_tp = lax.axis_size("sp"), lax.axis_size("fs"), lax.axis_size("tp")
    inputs, in_ssm, in_query, in_key, decay_rate = args[0], args[2], args[3], args[4], args[6]
    key_heads = in_key.shape[1] // HEAD_DIM
    query_heads = in_query.shape[1] // HEAD_DIM
    fits = (
        n_tp == 2
        and n == 4
        and n_fs == 4
        and key_heads == 2
        and query_heads % 4 == 0
        and query_heads * HEAD_DIM == in_ssm.shape[1]
        and in_ssm.shape[1] % 256 == 0
        and in_ssm.shape[1] == args[13].shape[0] == args[14].shape[0]
        and decay_rate.shape[0] % 32 == 0
        and decay_rate.shape[0] <= 2 * BLOCK
        and decay_rate.shape[1] * 2 == BLOCK
        and decay_rate.shape[0] * GROUP_CH == in_ssm.shape[1]
        and inputs.shape[0] == BLOCK == WINDOW
        and inputs.shape[1] % 128 == 0
        and in_ssm.shape[0] % 128 == 0
        and args[13].shape[1] % 128 == 0
    )
    return (fast_body if fits else general_body)(*args)


def solution(mesh):
    return jax.shard_map(
        body,
        mesh=mesh,
        in_specs=(
            P(("fs", "sp"), "tp"),
            P(),
            P("sp", "tp"),
            P("sp", "tp"),
            P("sp", "tp"),
            P("sp", "tp"),
            P("tp", None),
            P("tp", None),
            P(None, "tp", None, None),
            P(None, "tp", None, None),
            P("tp", None),
            P(("fs", "sp"), "tp"),
            P("tp"),
            P("tp", "sp"),
            P("tp", "sp"),
        ),
        out_specs=P(("fs", "sp", "tp"), None),
        check_vma=False,
    )
```

```python
import functools
import jax
import jax.numpy as jnp
from jax import lax
from jax.experimental import pallas as pl
from jax.experimental.pallas import tpu as pltpu
from jax.sharding import PartitionSpec as P

GROUP_CH = 16
HEAD_DIM = 64
WINDOW = 128
BLOCK = 128


epsilon = 1e-06
floor_score = -1e30


def prefix(x, axis, join, neutral):
    place = lax.axis_index(axis)
    gathered = jax.tree.map(
        lambda a, kind: lax.all_gather(a.astype(kind), axis),
        x,
        (jnp.bfloat16, jnp.bfloat16, jnp.bfloat16, jnp.bfloat16),
    )
    state = jax.tree.map(lambda a, e: jnp.zeros_like(a) + jnp.asarray(e, a.dtype), x, neutral)

    def one(hop, state):
        return join(
            state,
            jax.tree.map(
                lambda a, own: lax.dynamic_index_in_dim(a, hop, 0, False).astype(own.dtype),
                gathered,
                x,
            ),
        )

    return lax.fori_loop(0, place, one, state)


def from_behind(value, axis, steps):
    count = lax.axis_size(axis)
    initial, last = (max(0, -steps), min(count, count - steps))
    return lax.ppermute(value, axis, [(source, source + steps) for source in range(initial, last)])


def combine(earlier, later):
    first_re, first_im, state_re, state_im = earlier
    second_re, second_im, input_re, input_im = later
    return (
        second_re * first_re - second_im * first_im,
        second_re * first_im + second_im * first_re,
        second_re * state_re - second_im * state_im + input_re,
        second_re * state_im + second_im * state_re + input_im,
    )


def input_matrix(decay_rate, rotation, input_parts):
    damped = jnp.exp(-decay_rate)
    lift_re = damped * jnp.cos(rotation) - 1.0
    lift_im = damped * jnp.sin(rotation)
    modulus = decay_rate * decay_rate + rotation * rotation
    factor_re = (rotation * lift_im - decay_rate * lift_re) / modulus
    factor_im = -(rotation * lift_re + decay_rate * lift_im) / modulus
    part_re = input_parts[0].astype(jnp.float32)
    part_im = input_parts[1].astype(jnp.float32)
    joined_re = factor_re[:, :, None] * part_re - factor_im[:, :, None] * part_im
    joined_im = factor_re[:, :, None] * part_im + factor_im[:, :, None] * part_re
    return jnp.concatenate([joined_re, joined_im], axis=1).astype(jnp.bfloat16)


def window_attention(queries, keys_win, values_win, starts, sink_logit):
    window = queries.shape[1]
    scores = jnp.einsum("nqgrd,nkgd->ngrqk", queries, keys_win, preferred_element_type=jnp.float32)
    scores = scores * queries.shape[-1] ** (-0.5)
    places = (
        jnp.arange(window, dtype=jnp.int32)[:, None]
        + window
        - jnp.arange(2 * window, dtype=jnp.int32)[None, :]
    )
    inside = (places >= 0) & (places < window)
    reach = starts[:, None] - window + jnp.arange(2 * window, dtype=jnp.int32)[None, :] >= 0
    valid = (inside[None] & reach[:, None, :])[:, None, None]
    sinks = sink_logit.reshape(scores.shape[1], scores.shape[2])[None, :, :, None, None]
    scores = jnp.where(valid, scores, floor_score)
    row_peak = jnp.maximum(jnp.max(scores, axis=-1, keepdims=True), sinks)
    raised = jnp.where(valid, jnp.exp(scores - row_peak), 0.0)
    denominator = jnp.sum(raised, axis=-1, keepdims=True) + jnp.exp(sinks - row_peak)
    weights = (raised / denominator).astype(jnp.bfloat16)
    result = jnp.einsum(
        "ngrqk,nkgd->nqgrd", weights, values_win, preferred_element_type=jnp.float32
    )
    return result.astype(jnp.bfloat16)


def general_body(
    inputs,
    norm_gain,
    in_ssm,
    in_query,
    in_key,
    in_value,
    decay_rate,
    rotation,
    input_parts,
    output_parts,
    skip_scale,
    decay_shift,
    sink_logit,
    out_state,
    out_attend,
):
    gathered = lax.all_gather(inputs, "tp", axis=1, tiled=True)
    length = gathered.shape[0]
    widened = gathered.astype(jnp.float32)
    scale = lax.rsqrt(jnp.mean(widened * widened, axis=1, keepdims=True) + epsilon)
    normed = (widened * scale * norm_gain).astype(jnp.bfloat16)

    def add_rows(pieces):
        return tuple(
            (jnp.dot(normed, piece, preferred_element_type=jnp.float32) for piece in pieces)
        )

    projected = add_rows(
        (
            lax.all_gather(in_ssm, "sp", axis=0, tiled=True),
            lax.all_gather(in_query, "sp", axis=0, tiled=True),
            lax.all_gather(in_key, "sp", axis=0, tiled=True),
            lax.all_gather(in_value, "sp", axis=0, tiled=True),
        )
    )
    drive_in, queries, keys_local, values = [piece.astype(jnp.bfloat16) for piece in projected]
    groups = decay_rate.shape[0]
    state_dim = decay_rate.shape[1]
    channels = groups * GROUP_CH
    highest = lax.Precision.HIGHEST
    drive_cols = jnp.transpose(drive_in).reshape(groups, GROUP_CH, length)
    in_matrix = input_matrix(decay_rate, rotation, input_parts)
    drive = jnp.einsum("gqh,ght->gqt", in_matrix, drive_cols, preferred_element_type=jnp.float32)
    shift_cols = jnp.transpose(decay_shift)
    running = jnp.cumsum(shift_cols, axis=1)
    total_shift = running[:, -1]
    remain = length - 1.0 - jnp.arange(length, dtype=jnp.float32)
    to_end = (total_shift[:, None] - running)[:, None, :] - decay_rate[:, :, None] * remain[
        None, None, :
    ]
    fade = jnp.exp(to_end)
    turn = rotation[:, :, None] * remain[None, None, :]
    weight_re = fade * jnp.cos(turn)
    weight_im = fade * jnp.sin(turn)
    drive_re = drive[:, :state_dim]
    drive_im = drive[:, state_dim:]
    final_re = jnp.sum(weight_re * drive_re - weight_im * drive_im, axis=2)
    final_im = jnp.sum(weight_re * drive_im + weight_im * drive_re, axis=2)
    overall = jnp.exp(total_shift[:, None] - decay_rate * length)
    nothing = jnp.zeros_like(final_re)
    carried = prefix(
        (
            overall * jnp.cos(rotation * length),
            overall * jnp.sin(rotation * length),
            final_re,
            final_im,
        ),
        "sp",
        combine,
        (jnp.ones_like(final_re), nothing, nothing, nothing),
    )
    key_heads = keys_local.shape[1] // HEAD_DIM
    query_heads = queries.shape[1] // HEAD_DIM
    windows_dev = length // WINDOW
    previous = from_behind((keys_local, values), "sp", 1)

    def windows(flat, before):
        split = jnp.concatenate([before, flat], axis=0).reshape(
            windows_dev + 1, WINDOW, key_heads, HEAD_DIM
        )
        return jnp.concatenate([split[:-1], split[1:]], axis=1)

    offset = lax.axis_index("sp") * length
    starts = offset + jnp.arange(windows_dev, dtype=jnp.int32) * WINDOW
    queries_blk = queries.reshape(
        windows_dev, WINDOW, key_heads, query_heads // key_heads, HEAD_DIM
    )
    attended = window_attention(
        queries_blk,
        windows(keys_local, previous[0]),
        windows(values, previous[1]),
        starts,
        sink_logit,
    )
    attend_out = attended.reshape(length, query_heads * HEAD_DIM)
    blocks = length // BLOCK
    triangle = (
        jnp.arange(BLOCK, dtype=jnp.int32)[:, None] <= jnp.arange(BLOCK, dtype=jnp.int32)[None, :]
    ).astype(jnp.float32)
    offsets = jnp.arange(BLOCK, dtype=jnp.float32)
    centre = BLOCK // 2
    read_re = output_parts[0].astype(jnp.float32)
    read_im = output_parts[1].astype(jnp.float32)
    angle = rotation[:, :, None] * (offsets - centre)[None, None, :]
    cos_angle = jnp.cos(angle)
    sin_angle = jnp.sin(angle)
    phase = rotation[:, :, None] * (offsets + 1.0)[None, None, :]
    cos_phase = jnp.cos(phase)
    sin_phase = jnp.sin(phase)

    def advance(carry, pieces):
        carry_re, carry_im = carry
        part_re, part_im, shift_part, grouped_part = pieces
        level = jnp.dot(shift_part, triangle, precision=highest)
        log_from = level[:, None, :] - decay_rate[:, :, None] * (offsets + 1.0)[None, None, :]
        relative = log_from - log_from[:, :, centre : centre + 1]
        shrink = jnp.exp(-relative)
        lift_re = shrink * (part_re * cos_angle + part_im * sin_angle)
        lift_im = shrink * (part_im * cos_angle - part_re * sin_angle)
        prefix_re = jnp.dot(lift_re.reshape(groups * state_dim, BLOCK), triangle, precision=highest)
        prefix_im = jnp.dot(lift_im.reshape(groups * state_dim, BLOCK), triangle, precision=highest)
        prefix_re = prefix_re.reshape(groups, state_dim, BLOCK)
        prefix_im = prefix_im.reshape(groups, state_dim, BLOCK)
        grow = jnp.exp(relative)
        from_start = jnp.exp(log_from)
        keep_re = from_start * cos_phase
        keep_im = from_start * sin_phase
        state_re = grow * (prefix_re * cos_angle - prefix_im * sin_angle)
        state_im = grow * (prefix_im * cos_angle + prefix_re * sin_angle)
        state_re = state_re + keep_re * carry_re[:, :, None] - keep_im * carry_im[:, :, None]
        state_im = state_im + keep_re * carry_im[:, :, None] + keep_im * carry_re[:, :, None]
        result = jnp.einsum("ghp,gpt->ght", read_re, state_re, precision=highest)
        result = result - jnp.einsum("ghp,gpt->ght", read_im, state_im, precision=highest)
        result = result + skip_scale[:, :, None] * grouped_part.astype(jnp.float32)
        return ((state_re[:, :, -1], state_im[:, :, -1]), jax.nn.gelu(result).astype(jnp.bfloat16))

    drive_blocks = jnp.transpose(drive.reshape(groups, 2 * state_dim, blocks, BLOCK), (2, 0, 1, 3))
    shift_blocks = jnp.transpose(shift_cols.reshape(groups, blocks, BLOCK), (1, 0, 2))
    grouped_blocks = jnp.transpose(
        drive_cols.reshape(groups, GROUP_CH, blocks, BLOCK), (2, 0, 1, 3)
    )
    _, state_blocks = lax.scan(
        advance,
        (carried[2], carried[3]),
        (
            drive_blocks[:, :, :state_dim],
            drive_blocks[:, :, state_dim:],
            shift_blocks,
            grouped_blocks,
        ),
    )
    state_out = jnp.transpose(state_blocks, (0, 3, 1, 2)).reshape(length, channels)
    column_state, column_attend = (
        lax.all_gather(out_state, "sp", axis=1, tiled=True),
        lax.all_gather(out_attend, "sp", axis=1, tiled=True),
    )
    result = jnp.dot(state_out, column_state, preferred_element_type=jnp.float32)
    return lax.psum_scatter(
        (result + jnp.dot(attend_out, column_attend, preferred_element_type=jnp.float32)).astype(
            jnp.bfloat16
        ),
        "tp",
        scatter_dimension=0,
        tiled=True,
    )


MESH = pl.DeviceIdType.MESH
ANY = pl.BlockSpec(memory_space=pl.ANY)


def remote(src, dst, send, recv, **where):
    return pltpu.make_async_remote_copy(
        src_ref=src, dst_ref=dst, send_sem=send, recv_sem=recv, device_id=where, device_id_type=MESH
    )


def greet(peers):
    barrier = pltpu.get_barrier_semaphore()
    for peer in peers:
        pl.semaphore_signal(barrier, inc=1, device_id=peer, device_id_type=MESH)
    pl.semaphore_wait(barrier, len(peers))


def halves(x):
    high = x.astype(jnp.bfloat16)
    return high, (x - high.astype(jnp.float32)).astype(jnp.bfloat16)


def split_dot(x, exact):
    high, low = halves(x)
    return jnp.dot(high, exact, preferred_element_type=jnp.float32) + jnp.dot(
        low, exact, preferred_element_type=jnp.float32
    )


def column(row):
    size = row.shape[1]
    same = lax.broadcasted_iota(jnp.int32, (size, size), 0) == lax.broadcasted_iota(
        jnp.int32, (size, size), 1
    )
    return jnp.sum(jnp.where(same, row, 0.0), axis=1, keepdims=True)


def layer_kernel(x_in, gain_in, ssm, query, key_in, value_in, rate_in, turn_in, parts_in, reads_in,
                 skip_in, shift_in, sinks_in, ows, owa, out,
                 xf, xp, normed, w_ssm, w_query, w_key, w_value, wo_s, wo_a, gain, rate, turn,
                 parts, reads, skip, shift, sinks, tab, inm, read, lifts, grows, prefix, u_scr, q_scr,
                 kv_scr, y_scr, act_s, act_a, carry_out, carry_in, scale_out, scale_in, total_in,
                 give_u, give_q, give_kv, got_u, got_q, got_kv, pa, pf, pb, got, fsend, res,
                 loc, z_s, z_r, p_s, p_r, x_s, x_r, g_s, g_r, d_s, d_r, e_s, e_r, o_s):
    f32, bf = jnp.float32, jnp.bfloat16
    k, f, t = lax.axis_index("sp"), lax.axis_index("fs"), lax.axis_index("tp")
    n, n_fs = 4, 4
    tokens, half = x_in.shape
    rows, cols = ssm.shape[0], ows.shape[1]
    wide = w_ssm.shape[2] // 2
    groups, state = tab.shape[0], tab.shape[2]
    heads = wide // HEAD_DIM
    par, late = lax.rem(k, 2), lax.div(k, 2)
    pair = k + 1 - 2 * par
    other = 1 - t
    fx, fy, far = f + 1 - 2 * lax.rem(f, 2), lax.rem(f + 2, n_fs), n_fs - 1 - f
    across_z = lax.rem(k + 2, n)

    part = rows // n_fs
    into = (w_ssm, w_query, None, wo_s, wo_a)
    origin = (ssm, query, None, ows, owa)
    cuts = (4, 2, 2, 2, 2)

    def region(w, c, q, slot):
        if w == 2:
            return (w_key, w_value)[c].at[slot, pl.ds(pl.multiple_of(q * part, 16), part)]
        size = part // cuts[w]
        return into[w].at[slot, pl.ds(pl.multiple_of(q * part + c * size, 16), size)]

    def over_z(w, c):
        if w == 2:
            source = (key_in, value_in)[c].at[pl.ds(pl.multiple_of(f * part, 16), part)]
        else:
            size = part // cuts[w]
            source = origin[w].at[pl.ds(pl.multiple_of(f * part + c * size, 16), size)]
        return remote(source, region(w, c, f, late), z_s.at[w, c], z_r.at[w, c], sp=across_z)

    def spread_here(w, c):
        block = region(w, c, f, 1 - late)
        remote(block, block, z_s.at[w, c], z_r.at[w, c], sp=across_z).wait_recv()
        for i, who in enumerate((far, fx, fy)):
            launch(remote(block, block, x_s.at[w, c, i], x_r.at[w, c, i], fs=who))

    def spread_done(w):
        for c in range(cuts[w]):
            for i, who in enumerate((far, fx, fy)):
                block = region(w, c, who, 1 - late)
                remote(block, block, x_s.at[w, c, i], x_r.at[w, c, i], fs=who).wait_recv()

    sent = []

    def launch(c):
        c.start()
        sent.append(c)

    def shift_at(e):
        return shift.at[:, pl.ds(pl.multiple_of(e * tokens, 128), tokens)]

    def shift_rows(e):
        return shift_in.at[pl.ds(pl.multiple_of(e * groups, 8), groups)]

    queue = [(f"s{w}{c}", functools.partial(spread_here, w, c)) for w in (0, 2, 1, 4, 3) for c in range(cuts[w])]

    def pump(count):
        for _ in range(min(count, len(queue))):
            name, step = queue.pop(0)
            with jax.named_scope(name):
                step()

    local = [
        (rate_in, rate), (turn_in, turn), (parts_in, parts), (reads_in, reads), (skip_in, skip),
        (gain_in, gain), (sinks_in, sinks), (shift_rows(par), shift_at(par)),
        (x_in, xf.at[:, pl.ds(pl.multiple_of(t * half, 128), half)]),
        (ssm, w_ssm.at[late]), (query, w_query.at[late]), (key_in, w_key.at[late]),
        (value_in, w_value.at[late]), (ows, wo_s.at[late]), (owa, wo_a.at[late]),
    ]
    local = [pltpu.make_async_copy(a, b, loc.at[i]) for i, (a, b) in enumerate(local)]
    for c in local:
        c.start()
    first = par * groups

    def tables(g, columns_of):
        line, spin = rate[pl.ds(first + g, 1), :], turn[pl.ds(first + g, 1), :]
        rates, turns = column(line), column(spin)
        away = lax.broadcasted_iota(jnp.int32, (state, BLOCK), 1).astype(f32) - float(BLOCK // 2)
        angle = turns * away
        cos, sin = jnp.cos(angle), jnp.sin(angle)
        fade = jnp.exp(-rates * away)
        rise = jnp.exp(rates * away)
        tab[g, 0] = rise * cos
        tab[g, 1] = -(rise * sin)
        tab[g, 2] = fade * cos
        tab[g, 3] = fade * sin
        damped = jnp.exp(-line)
        lift_re = damped * jnp.cos(spin) - 1.0
        lift_im = damped * jnp.sin(spin)
        modulus = line * line + spin * spin
        factor_re = (spin * lift_im - line * lift_re) / modulus
        factor_im = -(spin * lift_re + line * lift_im) / modulus
        part_re = parts[0, first + g].astype(f32)
        part_im = parts[1, first + g].astype(f32)
        inm[g] = jnp.transpose(
            jnp.concatenate(
                [factor_re * part_re - factor_im * part_im, factor_re * part_im + factor_im * part_re],
                axis=1,
            )
        ).astype(bf)
        read[g] = jnp.concatenate(
            [reads[0, first + g].astype(f32), -reads[1, first + g].astype(f32)], axis=1
        ).astype(bf)
        spot = lax.broadcasted_iota(jnp.int32, (state, BLOCK), 1) == g
        return jnp.where(spot, rates, columns_of[0]), jnp.where(spot, turns, columns_of[1])

    columns_of = (jnp.zeros((state, BLOCK), f32), jnp.zeros((state, BLOCK), f32))
    early = (n - 1 - k) * (n - 1 - k)
    peers = [{"sp": pair}, {"sp": across_z}, {"fs": fx}, {"fs": fy}, {"fs": far}, {"tp": other}]
    barrier = pltpu.get_barrier_semaphore()
    for peer in peers:
        pl.semaphore_signal(barrier, inc=1, device_id=peer, device_id_type=MESH)

    def settle_params():
        for c in local[:8]:
            c.wait()

    pl.when(k < n - 1)(settle_params)
    with jax.named_scope("tables"):
        columns_of = lax.fori_loop(0, early, tables, columns_of)
    with jax.named_scope("greet"):
        pl.semaphore_wait(barrier, len(peers))
    at_end = k * (n - 1 - k) == 0
    sides = pl.ds(pl.multiple_of(t * half, 128), half)
    launch(remote(x_in, xf.at[:, sides], p_s.at[0], p_r.at[0], tp=other))
    launch(remote(x_in.at[:, pl.ds(pl.multiple_of((1 - par) * rows, 128), rows)], xp.at[t],
                  p_s.at[1], p_r.at[1], sp=pair))
    launch(remote(shift_rows(1 - par), shift_at(par), p_s.at[2], p_r.at[2], sp=pair))
    for c in range(cuts[0]):
        launch(over_z(0, c))
    pl.when(k == n - 1)(settle_params)
    with jax.named_scope("tables"):
        columns_of = lax.fori_loop(early, 10, tables, columns_of)

    local[8].wait()
    theirs = xf.at[:, pl.ds(pl.multiple_of(other * half, 128), half)]
    with jax.named_scope("own_x"):
        remote(theirs, theirs, p_s.at[0], p_r.at[0], tp=other).wait_recv()

    def gain_of(slot):
        return gain[:, pl.ds(pl.multiple_of((2 * slot + par) * rows, 128), rows)]

    own_rows = pl.ds(pl.multiple_of(par * tokens, 128), tokens)
    pair_rows = pl.ds(pl.multiple_of((1 - par) * tokens, 128), tokens)
    with jax.named_scope("norm"):
        full = xf[...].astype(f32)
        scale = lax.rsqrt(jnp.mean(full * full, axis=1, keepdims=True) + epsilon)
        same = lax.broadcasted_iota(jnp.int32, (tokens, tokens), 0) == lax.broadcasted_iota(
            jnp.int32, (tokens, tokens), 1
        )
        line = jnp.sum(jnp.where(same, scale, 0.0), axis=0, keepdims=True)
        scale_out[...] = jnp.broadcast_to(line, scale_out.shape)
    launch(remote(scale_out, scale_in, p_s.at[3], p_r.at[3], sp=pair))
    with jax.named_scope("norm"):
        for slot in range(2):
            block = xf[:, pl.ds(pl.multiple_of((2 * slot + par) * rows, 128), rows)].astype(f32)
            normed[slot, own_rows] = (block * scale * gain_of(slot)).astype(bf)
    with jax.named_scope("next_x"):
        remote(xp.at[t], xp.at[t], p_s.at[1], p_r.at[1], sp=pair).wait_recv()
    launch(remote(xp.at[t], xp.at[t], p_s.at[4], p_r.at[4], tp=other))
    pump(2)
    with jax.named_scope("tables"):
        columns_of = lax.fori_loop(10, 13, tables, columns_of)
    with jax.named_scope("partner_x"):
        remote(xp.at[other], xp.at[other], p_s.at[4], p_r.at[4], tp=other).wait_recv()
        remote(scale_in, scale_in, p_s.at[3], p_r.at[3], sp=pair).wait_recv()
    with jax.named_scope("norm"):
        scale = column(scale_in[0:1, :])
        for slot in range(2):
            normed[slot, pair_rows] = (xp[slot].astype(f32) * scale * gain_of(slot)).astype(bf)
    pump(2)
    fast = t == 1
    for c in range(2):
        launch(over_z(2, c))
    query_weights = [over_z(1, c) for c in range(2)]

    @pl.when(jnp.logical_not(fast))
    def _():
        for c in query_weights:
            c.start()

    with jax.named_scope("tables"):
        columns_of = lax.fori_loop(13, groups, tables, columns_of)
    for c in local[9:]:
        c.wait()
    with jax.named_scope("own_u"):
        total_in[...] = jnp.dot(normed[late], w_ssm[late], preferred_element_type=f32)

    def part_of(w, slot):
        return jnp.dot(normed[slot], w[slot], preferred_element_type=f32)

    def mine_at(e):
        return pl.ds(pl.multiple_of(e * wide, 128), wide)

    near_shift = shift_at(1 - par)
    remote(near_shift, near_shift, p_s.at[2], p_r.at[2], sp=pair).wait_recv()

    shape = (BLOCK, BLOCK)
    upto = lax.broadcasted_iota(jnp.int32, shape, 0) <= lax.broadcasted_iota(jnp.int32, shape, 1)
    tri = upto.astype(f32).astype(bf)
    centre = BLOCK // 2
    eye = lax.broadcasted_iota(jnp.int32, (groups, BLOCK), 0) == lax.broadcasted_iota(
        jnp.int32, (groups, BLOCK), 1
    )

    def across(col):
        return jnp.sum(jnp.where(eye, col, 0.0), axis=0, keepdims=True)

    begins, lasts = [], []
    for b in range(2):
        piece_b = shift[:, b * BLOCK : (b + 1) * BLOCK]
        high, low = halves(piece_b)
        low2 = (piece_b - high.astype(f32) - low.astype(f32)).astype(bf)
        level = (
            jnp.dot(high, tri, preferred_element_type=f32)
            + jnp.dot(low, tri, preferred_element_type=f32)
            + jnp.dot(low2, tri, preferred_element_type=f32)
        )
        middle = level[:, centre : centre + 1]
        lifts[b] = jnp.exp(middle - level)
        grown = jnp.exp(level - middle)
        grows[b] = grown
        begins.append(across(jnp.exp(middle)))
        lasts.append(across(grown[:, BLOCK - 1 :]))
    rates, turns = columns_of

    def times(a, b):
        return a[0] * b[0] - a[1] * b[1], a[0] * b[1] + a[1] * b[0]

    def plus(a, b):
        return a[0] + b[0], a[1] + b[1]

    def scaled(row, a):
        return row * a[0], row * a[1]

    def spiral(count):
        fade = jnp.exp(-rates * count)
        return fade * jnp.cos(turns * count), fade * jnp.sin(turns * count)

    reach, end = spiral(centre + 1.0), spiral(BLOCK - 1.0 - centre)
    whole = times(reach, end)

    pump(2)

    @pl.when(fast)
    def _():
        for c in query_weights:
            c.start()

    sent.extend(query_weights)
    with jax.named_scope("ssm_wait"):
        spread_done(0)
    with jax.named_scope("project_u"):
        total_in[...] += part_of(w_ssm, 1 - late)
        give_u[...] = total_in[:, mine_at(1 - par)].astype(bf)
    launch(remote(give_u, got_u, g_s.at[0], g_r.at[0], sp=pair))
    pump(2)
    for c in range(2):
        launch(over_z(4, c))
    def query_parts():
        with jax.named_scope("query_wait"):
            spread_done(1)
        with jax.named_scope("project_q"):
            total_in[...] = part_of(w_query, 0) + part_of(w_query, 1)
            give_q[...] = total_in[:, mine_at(1 - par)].astype(bf)
        launch(remote(give_q, got_q, g_s.at[1], g_r.at[1], sp=pair))

    def key_parts():
        with jax.named_scope("key_wait"):
            spread_done(2)
        with jax.named_scope("project_kv"):
            keys = part_of(w_key, 0) + part_of(w_key, 1)
            values = part_of(w_value, 0) + part_of(w_value, 1)
            both = [
                jnp.concatenate([a[:, e * HEAD_DIM : (e + 1) * HEAD_DIM] for a in (keys, values)], axis=1)
                for e in range(2)
            ]
            give_kv[...] = jnp.where(par == 0, both[1], both[0]).astype(bf)
        launch(remote(give_kv, got_kv, g_s.at[2], g_r.at[2], sp=pair))

        return jnp.where(par == 0, both[0], both[1])

    own_kv = key_parts()
    with jax.named_scope("got_u"):
        remote(got_u, got_u, g_s.at[0], g_r.at[0], sp=pair).wait_recv()
    with jax.named_scope("turn_u"):
        u = total_in[:, mine_at(par)] + got_u[...].astype(f32)
        u_scr[...] = jnp.transpose(u.astype(bf).astype(f32))

    tail = kv_scr.at[pl.ds(2 * WINDOW, WINDOW)]
    head = kv_scr.at[pl.ds(0, WINDOW)]
    hand_kv = remote(tail, head, p_s.at[5], p_r.at[5], sp=across_z)
    hand_state = remote(carry_out, carry_in, p_s.at[6], p_r.at[6], sp=across_z)

    def settle_kv():
        with jax.named_scope("kv_wait"):
            remote(got_kv, got_kv, g_s.at[2], g_r.at[2], sp=pair).wait_recv()
        kv_scr[WINDOW:, :] = (own_kv + got_kv[...].astype(f32)).astype(bf)

        @pl.when(late == 0)
        def _():
            hand_kv.start()
            kv_scr[:WINDOW, :] = jnp.zeros((WINDOW, kv_scr.shape[1]), bf)

    lane = lax.broadcasted_iota(jnp.int32, (state, BLOCK), 1)
    ends = [jnp.zeros((state, BLOCK), f32)] * 4
    for g in range(groups):
        with jax.named_scope("first"):
            u = u_scr[g * GROUP_CH : (g + 1) * GROUP_CH, :]
            drive = jnp.dot(inm[g], u.astype(bf), preferred_element_type=f32)
            up_re, up_im = tab[g, 0], tab[g, 1]
            lifted = []
            for b in range(2):
                span = slice(b * BLOCK, (b + 1) * BLOCK)
                row = lifts[b, g : g + 1, :]
                d_re, d_im = drive[:state, span] * row, drive[state:, span] * row
                lifted += [d_re * up_re - d_im * up_im, d_re * up_im + d_im * up_re]
            sums = split_dot(jnp.concatenate(lifted, axis=0), tri)
            prefix[g] = sums
            ends = [
                jnp.where(lane == g, sums[i * state : (i + 1) * state, BLOCK - 1 :], ends[i])
                for i in range(4)
            ]
        if g == 5:
            settle_kv()
        if g == 9:
            query_parts()
        if g in (11, 14):
            pump(1)
    with jax.named_scope("carry"):
        own = [scaled(lasts[b], times(end, (ends[2 * b], ends[2 * b + 1]))) for b in range(2)]
        decay = [scaled(lasts[b] * begins[b], whole) for b in range(2)]
        final = plus(own[1], times(decay[1], own[0]))
        carry_out[...] = jnp.transpose(jnp.concatenate(final, axis=0))[:groups]

    @pl.when(late == 0)
    def _():
        hand_state.start()
        carry_in[...] = jnp.zeros(carry_in.shape, f32)

    for c in range(2):
        launch(over_z(3, c))
    with jax.named_scope("q_wait"):
        remote(got_q, got_q, g_s.at[1], g_r.at[1], sp=pair).wait_recv()
    q_scr[...] = (total_in[:, mine_at(par)] + got_q[...].astype(f32)).astype(bf)
    gap_shape = (WINDOW, 2 * WINDOW)
    at = lax.broadcasted_iota(jnp.int32, gap_shape, 1)
    gap = lax.broadcasted_iota(jnp.int32, gap_shape, 0) + WINDOW - at
    inside = (gap >= 0) & (gap < WINDOW)
    inside_first = inside & (at >= WINDOW * (1 - late))
    sink_lane = lax.broadcasted_iota(jnp.int32, sinks.shape, 1)
    for b in (1, 0):
        if b == 0:

            @pl.when(late == 1)
            def _():
                with jax.named_scope("hand_wait"):
                    hand_kv.wait_recv()
                    hand_state.wait_recv()

        keys = kv_scr[b * WINDOW : (b + 2) * WINDOW, :HEAD_DIM]
        values = kv_scr[b * WINDOW : (b + 2) * WINDOW, HEAD_DIM:]
        valid = inside if b else inside_first
        outs = []
        for h in range(heads):
            with jax.named_scope("head"):
                q = q_scr[b * WINDOW : (b + 1) * WINDOW, h * HEAD_DIM : (h + 1) * HEAD_DIM]
                scores = lax.dot_general(q, keys, (((1,), (1,)), ((), ())), preferred_element_type=f32)
                scores = jnp.where(valid, scores * HEAD_DIM ** (-0.5), floor_score)
                sink = jnp.sum(jnp.where(sink_lane == par * heads + h, sinks[...], 0.0), axis=1, keepdims=True)
                peak = jnp.maximum(jnp.max(scores, axis=1, keepdims=True), sink)
                raised = jnp.where(valid, jnp.exp(scores - peak), 0.0)
                total = jnp.sum(raised, axis=1, keepdims=True) + jnp.exp(sink - peak)
                weights = (raised / total).astype(bf)
                outs.append(jnp.dot(weights, values, preferred_element_type=f32))
            if h == 2 and b == 0:
                pump(1)
        act_a[par, b * BLOCK : (b + 1) * BLOCK, :] = jnp.concatenate(outs, axis=1).astype(bf)

    mix_a = remote(act_a.at[par], act_a.at[par], e_s.at[4], e_r.at[4], sp=pair)
    launch(mix_a)
    back = jnp.transpose(carry_in[...])
    entry = (back[:state], back[state:])

    def bases(row, c):
        return scaled(row, times(c, reach))

    def grown_entry(c):
        return plus((own[0][0][:, :groups], own[0][1][:, :groups]),
                    times((decay[0][0][:, :groups], decay[0][1][:, :groups]), c))

    cut = (reach[0][:, :groups], reach[1][:, :groups])
    base = [
        scaled(begins[0][:, :groups], times(entry, cut)),
        scaled(begins[1][:, :groups], times(grown_entry(entry), cut)),
    ]
    for g in range(groups):
        with jax.named_scope("second"):
            u = u_scr[g * GROUP_CH : (g + 1) * GROUP_CH, :]
            down = (tab[g, 2], tab[g, 3])
            chosen = lax.broadcasted_iota(jnp.int32, skip.shape, 1) == first + g
            skips = jnp.sum(jnp.where(chosen, skip[...], 0.0), axis=1, keepdims=True)
            states = []
            for b in range(2):
                at_re = slice(2 * b * state, (2 * b + 1) * state)
                at_im = slice((2 * b + 1) * state, (2 * b + 2) * state)
                p = (prefix[g, at_re] + base[b][0][:, g : g + 1], prefix[g, at_im] + base[b][1][:, g : g + 1])
                states.append(jnp.concatenate(scaled(grows[b, g : g + 1, :], times(down, p)), axis=0))
            high, low = halves(jnp.concatenate(states, axis=1))
            y = jnp.dot(read[g], high, preferred_element_type=f32) + jnp.dot(
                read[g], low, preferred_element_type=f32
            )
            y_scr[g * GROUP_CH : (g + 1) * GROUP_CH, :] = y + skips * u
        if g == 7:
            pump(1)
        if (g + 1) % (groups // 2) == 0:
            side = (g + 1) // (groups // 2) - 1
            lanes = slice(side * BLOCK, (side + 1) * BLOCK)
            with jax.named_scope("gelu"):
                act_s[par, :, lanes] = jnp.transpose(jax.nn.gelu(y_scr[lanes, :])).astype(bf)
            half_s = act_s.at[par, :, pl.ds(side * BLOCK, BLOCK)]
            launch(remote(half_s, half_s, e_s.at[5 + side], e_r.at[5 + side], sp=pair))

    size, chunk = tokens // 2, cols // 2
    theirs = act_a.at[1 - par]
    with jax.named_scope("mix_a"):
        remote(theirs, theirs, e_s.at[4], e_r.at[4], sp=pair).wait_recv()
    pump(len(queue))

    def attend_part(slot):
        for side in range(2):
            lanes = slice(side * chunk, (side + 1) * chunk)
            rows_a = [jnp.dot(act_a[e], wo_a[slot, e * wide : (e + 1) * wide, lanes], preferred_element_type=f32)
                      for e in range(2)]
            pa[slot, :, lanes] = rows_a[0] + rows_a[1]

    with jax.named_scope("attend"):
        attend_part(late)
    with jax.named_scope("out_wait"):
        spread_done(4)
    with jax.named_scope("attend"):
        attend_part(1 - late)
    with jax.named_scope("mix_s"):
        for side in range(2):
            theirs = act_s.at[1 - par, :, pl.ds(side * BLOCK, BLOCK)]
            remote(theirs, theirs, e_s.at[5 + side], e_r.at[5 + side], sp=pair).wait_recv()

    def target(who, i):
        first_column = lax.rem(who + 2 * (i // 2), n) * cols + (i % 2) * chunk
        return out.at[:, pl.ds(pl.multiple_of(first_column, 128), chunk)]

    def multiply(i):
        slot, lanes = late if i < 2 else 1 - late, slice(i % 2 * chunk, (i % 2 + 1) * chunk)
        total = pa[slot, :, lanes]
        for e in range(2):
            total = total + jnp.dot(
                act_s[e], wo_s[slot, e * wide : (e + 1) * wide, lanes], preferred_element_type=f32
            )
        for e in range(2):
            for side in range(2):
                block = total[e * tokens + side * size : e * tokens + (side + 1) * size]
                pf[i, e, side] = block
                pb[i, side, e] = block.astype(bf)
        launch(remote(pb.at[i, other], got.at[i], d_s.at[i], d_r.at[i], tp=other))

    def pass_on(i):
        remote(got.at[i], got.at[i], d_s.at[i], d_r.at[i], tp=other).wait_recv()
        fsend[i] = (pf[i, 1 - par, t] + got[i, 1 - par].astype(f32)).astype(bf)
        launch(remote(fsend.at[i], target(k, i), e_s.at[i], e_r.at[i], sp=pair))
        res[i] = (pf[i, par, t] + got[i, par].astype(f32)).astype(bf)
        launch(pltpu.make_async_copy(res.at[i], target(k, i), o_s.at[i]))

    for i in range(4):
        if i == 2:
            with jax.named_scope("out_wait"):
                spread_done(3)
        with jax.named_scope("multiply"):
            multiply(i)
        if i:
            with jax.named_scope("pass"):
                pass_on(i - 1)
    with jax.named_scope("pass"):
        pass_on(3)
    with jax.named_scope("settle"):
        for i in range(4):
            theirs = target(pair, i)
            remote(theirs, theirs, e_s.at[i], e_r.at[i], sp=pair).wait_recv()

    with jax.named_scope("drain"):
        for c in sent:
            if c.is_remote:
                c.wait_send()
            else:
                c.wait()

    @pl.when(late == 0)
    def _():
        hand_kv.wait_send()
        hand_state.wait_send()


def layer(x, gain, ssm, query, key, value, rate, turn, parts, reads, skip, shift, sinks, ows, owa):
    bf, f32 = jnp.bfloat16, jnp.float32
    tokens, half = x.shape
    rows, cols = ows.shape[0], ows.shape[1]
    wide = ssm.shape[1] // 2
    groups, state = rate.shape[0] // 2, rate.shape[1]
    length = 2 * tokens
    dma = pltpu.SemaphoreType.DMA
    vm = pltpu.VMEM
    return pl.pallas_call(
        layer_kernel,
        out_shape=jax.ShapeDtypeStruct((tokens // 2, 4 * cols), bf),
        in_specs=[ANY] * 15,
        out_specs=ANY,
        scratch_shapes=[
            vm((tokens, 2 * half), bf), vm((2, tokens, rows), bf), vm((2, length, rows), bf),
            vm((2, rows, 2 * wide), bf), vm((2, rows, 2 * wide), bf), vm((2,) + key.shape, bf),
            vm((2,) + value.shape, bf), vm((2, rows, cols), bf), vm((2, rows, cols), bf),
            vm(gain.shape, f32), vm(rate.shape, f32), vm(turn.shape, f32),
            vm(parts.shape, bf), vm(reads.shape, bf), vm(skip.shape, f32),
            vm((groups, length), f32), vm(sinks.shape, f32),
            vm((groups, 4, state, BLOCK), f32), vm((groups, 2 * state, GROUP_CH), bf),
            vm((groups, GROUP_CH, 2 * state), bf), vm((2, groups, BLOCK), f32), vm((2, groups, BLOCK), f32),
            vm((groups, 4 * state, BLOCK), f32), vm((wide, length), f32), vm((length, wide), bf),
            vm((length + WINDOW, 2 * HEAD_DIM), bf), vm((wide, length), f32),
            vm((2, length, wide), bf), vm((2, length, wide), bf),
            vm((groups, 2 * state), f32), vm((groups, 2 * state), f32),
            vm((8, tokens), f32), vm((8, tokens), f32), vm((length, 2 * wide), f32),
            vm((length, wide), bf), vm((length, wide), bf), vm((length, 2 * HEAD_DIM), bf),
            vm((length, wide), bf), vm((length, wide), bf), vm((length, 2 * HEAD_DIM), bf),
            vm((2, length, cols), f32),
            vm((4, 2, 2, tokens // 2, cols // 2), f32), vm((4, 2, 2, tokens // 2, cols // 2), bf),
            vm((4, 2, tokens // 2, cols // 2), bf), vm((4, tokens // 2, cols // 2), bf),
            vm((4, tokens // 2, cols // 2), bf),
            dma((15,)), dma((5, 4)), dma((5, 4)), dma((7,)), dma((7,)), dma((5, 4, 3)), dma((5, 4, 3)),
            dma((3,)), dma((3,)), dma((4,)), dma((4,)), dma((7,)), dma((7,)), dma((4,)),
        ],
        compiler_params=pltpu.CompilerParams(collective_id=0, has_side_effects=True),
    )(x, gain, ssm, query, key, value, rate, turn, parts, reads, skip, shift, sinks, ows, owa)


def fast_body(
    inputs, norm_gain, in_ssm, in_query, in_key, in_value, decay_rate, rotation, input_parts,
    output_parts, skip_scale, decay_shift, sink_logit, out_state, out_attend,
):
    return layer(
        inputs, norm_gain[None], in_ssm, in_query, in_key, in_value, decay_rate, rotation,
        jnp.swapaxes(input_parts, 2, 3), output_parts, skip_scale.T, jnp.transpose(decay_shift),
        sink_logit[None], out_state, out_attend,
    )


def body(*args):
    n, n_fs, n_tp = lax.axis_size("sp"), lax.axis_size("fs"), lax.axis_size("tp")
    inputs, in_ssm, in_query, in_key, decay_rate = args[0], args[2], args[3], args[4], args[6]
    key_heads = in_key.shape[1] // HEAD_DIM
    query_heads = in_query.shape[1] // HEAD_DIM
    fits = (
        n_tp == 2
        and n == 4
        and n_fs == 4
        and key_heads == 2
        and query_heads % 4 == 0
        and query_heads * HEAD_DIM == in_ssm.shape[1]
        and in_ssm.shape[1] % 256 == 0
        and in_ssm.shape[1] == args[13].shape[0] == args[14].shape[0]
        and decay_rate.shape[0] % 32 == 0
        and decay_rate.shape[0] <= 2 * BLOCK
        and decay_rate.shape[1] * 2 == BLOCK
        and decay_rate.shape[0] * GROUP_CH == in_ssm.shape[1]
        and inputs.shape[0] == BLOCK == WINDOW
        and inputs.shape[1] % 128 == 0
        and in_ssm.shape[0] % 128 == 0
        and in_ssm.shape[0] == args[13].shape[0]
        and inputs.shape[1] == 2 * in_ssm.shape[0]
        and args[13].shape[1] % 128 == 0
    )
    return (fast_body if fits else general_body)(*args)


def solution(mesh):
    return jax.shard_map(
        body,
        mesh=mesh,
        in_specs=(
            P(("fs", "sp"), "tp"),
            P(),
            P("sp", "tp"),
            P("sp", "tp"),
            P("sp", "tp"),
            P("sp", "tp"),
            P("tp", None),
            P("tp", None),
            P(None, "tp", None, None),
            P(None, "tp", None, None),
            P("tp", None),
            P(("fs", "sp"), "tp"),
            P("tp"),
            P("tp", "sp"),
            P("tp", "sp"),
        ),
        out_specs=P(("fs", "sp", "tp"), None),
        check_vma=False,
    )
```

```python
import functools
import jax
import jax.numpy as jnp
from jax import lax
from jax.experimental import pallas as pl
from jax.experimental.pallas import tpu as pltpu
from jax.sharding import PartitionSpec as P

GROUP_CH = 16
HEAD_DIM = 64
WINDOW = 128
BLOCK = 128


epsilon = 1e-06
floor_score = -1e30


def prefix(x, axis, join, neutral):
    place = lax.axis_index(axis)
    gathered = jax.tree.map(
        lambda a, kind: lax.all_gather(a.astype(kind), axis),
        x,
        (jnp.bfloat16, jnp.bfloat16, jnp.bfloat16, jnp.bfloat16),
    )
    state = jax.tree.map(lambda a, e: jnp.zeros_like(a) + jnp.asarray(e, a.dtype), x, neutral)

    def one(hop, state):
        return join(
            state,
            jax.tree.map(
                lambda a, own: lax.dynamic_index_in_dim(a, hop, 0, False).astype(own.dtype),
                gathered,
                x,
            ),
        )

    return lax.fori_loop(0, place, one, state)


def from_behind(value, axis, steps):
    count = lax.axis_size(axis)
    initial, last = (max(0, -steps), min(count, count - steps))
    return lax.ppermute(value, axis, [(source, source + steps) for source in range(initial, last)])


def combine(earlier, later):
    first_re, first_im, state_re, state_im = earlier
    second_re, second_im, input_re, input_im = later
    return (
        second_re * first_re - second_im * first_im,
        second_re * first_im + second_im * first_re,
        second_re * state_re - second_im * state_im + input_re,
        second_re * state_im + second_im * state_re + input_im,
    )


def input_matrix(decay_rate, rotation, input_parts):
    damped = jnp.exp(-decay_rate)
    lift_re = damped * jnp.cos(rotation) - 1.0
    lift_im = damped * jnp.sin(rotation)
    modulus = decay_rate * decay_rate + rotation * rotation
    factor_re = (rotation * lift_im - decay_rate * lift_re) / modulus
    factor_im = -(rotation * lift_re + decay_rate * lift_im) / modulus
    part_re = input_parts[0].astype(jnp.float32)
    part_im = input_parts[1].astype(jnp.float32)
    joined_re = factor_re[:, :, None] * part_re - factor_im[:, :, None] * part_im
    joined_im = factor_re[:, :, None] * part_im + factor_im[:, :, None] * part_re
    return jnp.concatenate([joined_re, joined_im], axis=1).astype(jnp.bfloat16)


def window_attention(queries, keys_win, values_win, starts, sink_logit):
    window = queries.shape[1]
    scores = jnp.einsum("nqgrd,nkgd->ngrqk", queries, keys_win, preferred_element_type=jnp.float32)
    scores = scores * queries.shape[-1] ** (-0.5)
    places = (
        jnp.arange(window, dtype=jnp.int32)[:, None]
        + window
        - jnp.arange(2 * window, dtype=jnp.int32)[None, :]
    )
    inside = (places >= 0) & (places < window)
    reach = starts[:, None] - window + jnp.arange(2 * window, dtype=jnp.int32)[None, :] >= 0
    valid = (inside[None] & reach[:, None, :])[:, None, None]
    sinks = sink_logit.reshape(scores.shape[1], scores.shape[2])[None, :, :, None, None]
    scores = jnp.where(valid, scores, floor_score)
    row_peak = jnp.maximum(jnp.max(scores, axis=-1, keepdims=True), sinks)
    raised = jnp.where(valid, jnp.exp(scores - row_peak), 0.0)
    denominator = jnp.sum(raised, axis=-1, keepdims=True) + jnp.exp(sinks - row_peak)
    weights = (raised / denominator).astype(jnp.bfloat16)
    result = jnp.einsum(
        "ngrqk,nkgd->nqgrd", weights, values_win, preferred_element_type=jnp.float32
    )
    return result.astype(jnp.bfloat16)


def general_body(
    inputs,
    norm_gain,
    in_ssm,
    in_query,
    in_key,
    in_value,
    decay_rate,
    rotation,
    input_parts,
    output_parts,
    skip_scale,
    decay_shift,
    sink_logit,
    out_state,
    out_attend,
):
    gathered = lax.all_gather(inputs, "tp", axis=1, tiled=True)
    length = gathered.shape[0]
    widened = gathered.astype(jnp.float32)
    scale = lax.rsqrt(jnp.mean(widened * widened, axis=1, keepdims=True) + epsilon)
    normed = (widened * scale * norm_gain).astype(jnp.bfloat16)

    def add_rows(pieces):
        return tuple(
            (jnp.dot(normed, piece, preferred_element_type=jnp.float32) for piece in pieces)
        )

    projected = add_rows(
        (
            lax.all_gather(in_ssm, "sp", axis=0, tiled=True),
            lax.all_gather(in_query, "sp", axis=0, tiled=True),
            lax.all_gather(in_key, "sp", axis=0, tiled=True),
            lax.all_gather(in_value, "sp", axis=0, tiled=True),
        )
    )
    drive_in, queries, keys_local, values = [piece.astype(jnp.bfloat16) for piece in projected]
    groups = decay_rate.shape[0]
    state_dim = decay_rate.shape[1]
    channels = groups * GROUP_CH
    highest = lax.Precision.HIGHEST
    drive_cols = jnp.transpose(drive_in).reshape(groups, GROUP_CH, length)
    in_matrix = input_matrix(decay_rate, rotation, input_parts)
    drive = jnp.einsum("gqh,ght->gqt", in_matrix, drive_cols, preferred_element_type=jnp.float32)
    shift_cols = jnp.transpose(decay_shift)
    running = jnp.cumsum(shift_cols, axis=1)
    total_shift = running[:, -1]
    remain = length - 1.0 - jnp.arange(length, dtype=jnp.float32)
    to_end = (total_shift[:, None] - running)[:, None, :] - decay_rate[:, :, None] * remain[
        None, None, :
    ]
    fade = jnp.exp(to_end)
    turn = rotation[:, :, None] * remain[None, None, :]
    weight_re = fade * jnp.cos(turn)
    weight_im = fade * jnp.sin(turn)
    drive_re = drive[:, :state_dim]
    drive_im = drive[:, state_dim:]
    final_re = jnp.sum(weight_re * drive_re - weight_im * drive_im, axis=2)
    final_im = jnp.sum(weight_re * drive_im + weight_im * drive_re, axis=2)
    overall = jnp.exp(total_shift[:, None] - decay_rate * length)
    nothing = jnp.zeros_like(final_re)
    carried = prefix(
        (
            overall * jnp.cos(rotation * length),
            overall * jnp.sin(rotation * length),
            final_re,
            final_im,
        ),
        "sp",
        combine,
        (jnp.ones_like(final_re), nothing, nothing, nothing),
    )
    key_heads = keys_local.shape[1] // HEAD_DIM
    query_heads = queries.shape[1] // HEAD_DIM
    windows_dev = length // WINDOW
    previous = from_behind((keys_local, values), "sp", 1)

    def windows(flat, before):
        split = jnp.concatenate([before, flat], axis=0).reshape(
            windows_dev + 1, WINDOW, key_heads, HEAD_DIM
        )
        return jnp.concatenate([split[:-1], split[1:]], axis=1)

    offset = lax.axis_index("sp") * length
    starts = offset + jnp.arange(windows_dev, dtype=jnp.int32) * WINDOW
    queries_blk = queries.reshape(
        windows_dev, WINDOW, key_heads, query_heads // key_heads, HEAD_DIM
    )
    attended = window_attention(
        queries_blk,
        windows(keys_local, previous[0]),
        windows(values, previous[1]),
        starts,
        sink_logit,
    )
    attend_out = attended.reshape(length, query_heads * HEAD_DIM)
    blocks = length // BLOCK
    triangle = (
        jnp.arange(BLOCK, dtype=jnp.int32)[:, None] <= jnp.arange(BLOCK, dtype=jnp.int32)[None, :]
    ).astype(jnp.float32)
    offsets = jnp.arange(BLOCK, dtype=jnp.float32)
    centre = BLOCK // 2
    read_re = output_parts[0].astype(jnp.float32)
    read_im = output_parts[1].astype(jnp.float32)
    angle = rotation[:, :, None] * (offsets - centre)[None, None, :]
    cos_angle = jnp.cos(angle)
    sin_angle = jnp.sin(angle)
    phase = rotation[:, :, None] * (offsets + 1.0)[None, None, :]
    cos_phase = jnp.cos(phase)
    sin_phase = jnp.sin(phase)

    def advance(carry, pieces):
        carry_re, carry_im = carry
        part_re, part_im, shift_part, grouped_part = pieces
        level = jnp.dot(shift_part, triangle, precision=highest)
        log_from = level[:, None, :] - decay_rate[:, :, None] * (offsets + 1.0)[None, None, :]
        relative = log_from - log_from[:, :, centre : centre + 1]
        shrink = jnp.exp(-relative)
        lift_re = shrink * (part_re * cos_angle + part_im * sin_angle)
        lift_im = shrink * (part_im * cos_angle - part_re * sin_angle)
        prefix_re = jnp.dot(lift_re.reshape(groups * state_dim, BLOCK), triangle, precision=highest)
        prefix_im = jnp.dot(lift_im.reshape(groups * state_dim, BLOCK), triangle, precision=highest)
        prefix_re = prefix_re.reshape(groups, state_dim, BLOCK)
        prefix_im = prefix_im.reshape(groups, state_dim, BLOCK)
        grow = jnp.exp(relative)
        from_start = jnp.exp(log_from)
        keep_re = from_start * cos_phase
        keep_im = from_start * sin_phase
        state_re = grow * (prefix_re * cos_angle - prefix_im * sin_angle)
        state_im = grow * (prefix_im * cos_angle + prefix_re * sin_angle)
        state_re = state_re + keep_re * carry_re[:, :, None] - keep_im * carry_im[:, :, None]
        state_im = state_im + keep_re * carry_im[:, :, None] + keep_im * carry_re[:, :, None]
        result = jnp.einsum("ghp,gpt->ght", read_re, state_re, precision=highest)
        result = result - jnp.einsum("ghp,gpt->ght", read_im, state_im, precision=highest)
        result = result + skip_scale[:, :, None] * grouped_part.astype(jnp.float32)
        return ((state_re[:, :, -1], state_im[:, :, -1]), jax.nn.gelu(result).astype(jnp.bfloat16))

    drive_blocks = jnp.transpose(drive.reshape(groups, 2 * state_dim, blocks, BLOCK), (2, 0, 1, 3))
    shift_blocks = jnp.transpose(shift_cols.reshape(groups, blocks, BLOCK), (1, 0, 2))
    grouped_blocks = jnp.transpose(
        drive_cols.reshape(groups, GROUP_CH, blocks, BLOCK), (2, 0, 1, 3)
    )
    _, state_blocks = lax.scan(
        advance,
        (carried[2], carried[3]),
        (
            drive_blocks[:, :, :state_dim],
            drive_blocks[:, :, state_dim:],
            shift_blocks,
            grouped_blocks,
        ),
    )
    state_out = jnp.transpose(state_blocks, (0, 3, 1, 2)).reshape(length, channels)
    column_state, column_attend = (
        lax.all_gather(out_state, "sp", axis=1, tiled=True),
        lax.all_gather(out_attend, "sp", axis=1, tiled=True),
    )
    result = jnp.dot(state_out, column_state, preferred_element_type=jnp.float32)
    return lax.psum_scatter(
        (result + jnp.dot(attend_out, column_attend, preferred_element_type=jnp.float32)).astype(
            jnp.bfloat16
        ),
        "tp",
        scatter_dimension=0,
        tiled=True,
    )


MESH = pl.DeviceIdType.MESH
ANY = pl.BlockSpec(memory_space=pl.ANY)


def remote(src, dst, send, recv, **where):
    return pltpu.make_async_remote_copy(
        src_ref=src, dst_ref=dst, send_sem=send, recv_sem=recv, device_id=where, device_id_type=MESH
    )


def greet(peers):
    barrier = pltpu.get_barrier_semaphore()
    for peer in peers:
        pl.semaphore_signal(barrier, inc=1, device_id=peer, device_id_type=MESH)
    pl.semaphore_wait(barrier, len(peers))


def halves(x):
    high = x.astype(jnp.bfloat16)
    return high, (x - high.astype(jnp.float32)).astype(jnp.bfloat16)


def split_dot(x, exact):
    high, low = halves(x)
    return jnp.dot(high, exact, preferred_element_type=jnp.float32) + jnp.dot(
        low, exact, preferred_element_type=jnp.float32
    )


def column(row):
    size = row.shape[1]
    same = lax.broadcasted_iota(jnp.int32, (size, size), 0) == lax.broadcasted_iota(
        jnp.int32, (size, size), 1
    )
    return jnp.sum(jnp.where(same, row, 0.0), axis=1, keepdims=True)


def turned(angle):
    quarter = jnp.floor(angle * (2.0 / 3.141592653589793) + 0.5)
    r = ((angle - quarter * 1.5703125) - quarter * 4.837512969970703e-4) - quarter * 7.549789948768648e-8
    sq = r * r
    sin = r + r * sq * (-1.6666654611e-1 + sq * (8.3321608736e-3 + sq * -1.9515295891e-4))
    cos = 1.0 - 0.5 * sq + sq * sq * (4.166664568298827e-2 + sq * (-1.388731625493765e-3 + sq * 2.443315711809948e-5))
    which = quarter.astype(jnp.int32)
    swap = (which & 1) == 1
    flip_cos = ((which + 1) & 2) == 2
    flip_sin = (which & 2) == 2
    a, b = jnp.where(swap, sin, cos), jnp.where(swap, cos, sin)
    return jnp.where(flip_cos, -a, a), jnp.where(flip_sin, -b, b)


def layer_kernel(x_in, gain_in, ssm, query, key_in, value_in, rate_in, turn_in, parts_in, reads_in,
                 skip_in, shift_in, sinks_in, ows, owa, out,
                 xf, xp, normed, w_ssm, w_query, w_key, w_value, wo_s, wo_a, gain, rate, turn,
                 parts, reads, skip, shift, sinks, tab, inm, read, lifts, grows, prefix, u_scr, q_scr,
                 kv_scr, y_scr, act_s, act_a, carry_out, carry_in, scale_out, scale_in, total_in, total_q,
                 give_u, give_q, give_kv, got_u, got_q, got_kv, pa, pf, pb, got, fsend, res,
                 loc, z_s, z_r, p_s, p_r, x_s, x_r, g_s, g_r, d_s, d_r, e_s, e_r, o_s):
    f32, bf = jnp.float32, jnp.bfloat16
    k, f, t = lax.axis_index("sp"), lax.axis_index("fs"), lax.axis_index("tp")
    n, n_fs = 4, 4
    tokens, half = x_in.shape
    rows, cols = ssm.shape[0], ows.shape[1]
    wide = w_ssm.shape[2] // 2
    groups, state = tab.shape[0], tab.shape[2]
    heads = wide // HEAD_DIM
    par, late = lax.rem(k, 2), lax.div(k, 2)
    pair = k + 1 - 2 * par
    other = 1 - t
    fx, fy, far = f + 1 - 2 * lax.rem(f, 2), lax.rem(f + 2, n_fs), n_fs - 1 - f
    across_z = lax.rem(k + 2, n)

    part = rows // n_fs
    into = (w_ssm, w_query, None, wo_s, wo_a)
    origin = (ssm, query, None, ows, owa)
    cuts = (4, 4, 2, 2, 2)

    def stripe(c):
        return pl.ds(c % 2 * wide + c // 2 * (wide // 2), wide // 2)

    def region(w, c, q, slot):
        if w < 2:
            return into[w].at[slot, pl.ds(pl.multiple_of(q * part, 16), part), stripe(c)]
        if w == 2:
            return (w_key, w_value)[c].at[slot, pl.ds(pl.multiple_of(q * part, 16), part)]
        size = part // cuts[w]
        return into[w].at[slot, pl.ds(pl.multiple_of(q * part + c * size, 16), size)]

    def over_z(w, c):
        if w < 2:
            source = origin[w].at[pl.ds(pl.multiple_of(f * part, 16), part), stripe(c)]
        elif w == 2:
            source = (key_in, value_in)[c].at[pl.ds(pl.multiple_of(f * part, 16), part)]
        else:
            size = part // cuts[w]
            source = origin[w].at[pl.ds(pl.multiple_of(f * part + c * size, 16), size)]
        return remote(source, region(w, c, f, late), z_s.at[w, c], z_r.at[w, c], sp=across_z)

    def spread_here(w, c):
        block = region(w, c, f, 1 - late)
        remote(block, block, z_s.at[w, c], z_r.at[w, c], sp=across_z).wait_recv()
        for i, who in enumerate((far, fx, fy)):
            launch(remote(block, block, x_s.at[w, c, i], x_r.at[w, c, i], fs=who))

    def spread_done(w, pieces=None):
        for c in pieces or range(cuts[w]):
            for i, who in enumerate((far, fx, fy)):
                block = region(w, c, who, 1 - late)
                remote(block, block, x_s.at[w, c, i], x_r.at[w, c, i], fs=who).wait_recv()

    sent = []

    def launch(c):
        c.start()
        sent.append(c)

    def shift_at(e):
        return shift.at[:, pl.ds(pl.multiple_of(e * tokens, 128), tokens)]

    def shift_rows(e):
        return shift_in.at[pl.ds(pl.multiple_of(e * groups, 8), groups)]

    queue = [(f"s{w}{c}", functools.partial(spread_here, w, c)) for w in (0, 2, 1, 3, 4) for c in range(cuts[w])]

    def pump(count):
        for _ in range(min(count, len(queue))):
            name, step = queue.pop(0)
            with jax.named_scope(name):
                step()

    local = [
        (rate_in, rate), (turn_in, turn), (parts_in, parts), (reads_in, reads), (skip_in, skip),
        (gain_in, gain), (sinks_in, sinks), (shift_rows(par), shift_at(par)),
        (x_in, xf.at[:, pl.ds(pl.multiple_of(t * half, 128), half)]),
        (ssm, w_ssm.at[late]), (query, w_query.at[late]), (key_in, w_key.at[late]),
        (value_in, w_value.at[late]), (ows, wo_s.at[late]), (owa, wo_a.at[late]),
    ]
    local = [pltpu.make_async_copy(a, b, loc.at[i]) for i, (a, b) in enumerate(local)]
    for c in local:
        c.start()
    first = par * groups

    def tables(g, columns_of):
        line, spin = rate[pl.ds(first + g, 1), :], turn[pl.ds(first + g, 1), :]
        rates, turns = column(line), column(spin)
        away = lax.broadcasted_iota(jnp.int32, (state, BLOCK), 1).astype(f32) - float(BLOCK // 2)
        angle = turns * away
        cos, sin = turned(angle)
        fade = jnp.exp(-rates * away)
        rise = jnp.exp(rates * away)
        tab[g, 0] = rise * cos
        tab[g, 1] = -(rise * sin)
        tab[g, 2] = fade * cos
        tab[g, 3] = fade * sin
        damped = jnp.exp(-line)
        lift_re = damped * jnp.cos(spin) - 1.0
        lift_im = damped * jnp.sin(spin)
        modulus = line * line + spin * spin
        factor_re = (spin * lift_im - line * lift_re) / modulus
        factor_im = -(spin * lift_re + line * lift_im) / modulus
        part_re = parts[0, first + g].astype(f32)
        part_im = parts[1, first + g].astype(f32)
        inm[g] = jnp.transpose(
            jnp.concatenate(
                [factor_re * part_re - factor_im * part_im, factor_re * part_im + factor_im * part_re],
                axis=1,
            )
        ).astype(bf)
        read[g] = jnp.concatenate(
            [reads[0, first + g].astype(f32), -reads[1, first + g].astype(f32)], axis=1
        ).astype(bf)
        spot = lax.broadcasted_iota(jnp.int32, (state, BLOCK), 1) == g
        return jnp.where(spot, rates, columns_of[0]), jnp.where(spot, turns, columns_of[1])

    columns_of = (jnp.zeros((state, BLOCK), f32), jnp.zeros((state, BLOCK), f32))
    early = (n - 1 - k) * (n - 1 - k)
    peers = [{"sp": pair}, {"sp": across_z}, {"fs": fx}, {"fs": fy}, {"fs": far}, {"tp": other}]
    barrier = pltpu.get_barrier_semaphore()
    for peer in peers:
        pl.semaphore_signal(barrier, inc=1, device_id=peer, device_id_type=MESH)

    def settle_params():
        for c in local[:8]:
            c.wait()

    pl.when(k < n - 1)(settle_params)
    with jax.named_scope("tables"):
        columns_of = lax.fori_loop(0, early, tables, columns_of)
    with jax.named_scope("greet"):
        pl.semaphore_wait(barrier, len(peers))
    at_end = k * (n - 1 - k) == 0
    sides = pl.ds(pl.multiple_of(t * half, 128), half)
    launch(remote(x_in, xf.at[:, sides], p_s.at[0], p_r.at[0], tp=other))
    slow, fast = t == 0, t == 1

    def launch_if(choice, copies):
        @pl.when(choice)
        def _():
            for c in copies:
                c.start()

    state_weights = [over_z(0, c) for c in range(cuts[0])]
    early_keys = [over_z(2, c) for c in range(2)]
    query_weights = [over_z(1, c) for c in range(cuts[1])]
    out_weights = [over_z(3, c) for c in range(2)]
    attend_weights = [over_z(4, c) for c in range(2)]
    give_x = remote(x_in.at[:, pl.ds(pl.multiple_of((1 - par) * rows, 128), rows)], xp.at[t],
                    p_s.at[1], p_r.at[1], sp=pair)
    state_weights[0].start()
    launch_if(slow, state_weights[1:])
    launch(remote(shift_rows(1 - par), shift_at(par), p_s.at[2], p_r.at[2], sp=pair))
    launch_if(slow | jnp.logical_not(at_end), [give_x])
    launch_if(slow, early_keys)
    sent.extend(state_weights + early_keys + query_weights + out_weights + attend_weights + [give_x])
    pl.when(k == n - 1)(settle_params)
    with jax.named_scope("tables"):
        columns_of = lax.fori_loop(early, 10, tables, columns_of)

    local[8].wait()
    theirs = xf.at[:, pl.ds(pl.multiple_of(other * half, 128), half)]
    with jax.named_scope("own_x"):
        remote(theirs, theirs, p_s.at[0], p_r.at[0], tp=other).wait_recv()

    def gain_of(slot):
        return gain[:, pl.ds(pl.multiple_of((2 * slot + par) * rows, 128), rows)]

    own_rows = pl.ds(pl.multiple_of(par * tokens, 128), tokens)
    pair_rows = pl.ds(pl.multiple_of((1 - par) * tokens, 128), tokens)
    with jax.named_scope("norm"):
        full = xf[...].astype(f32)
        scale = lax.rsqrt(jnp.mean(full * full, axis=1, keepdims=True) + epsilon)
        same = lax.broadcasted_iota(jnp.int32, (tokens, tokens), 0) == lax.broadcasted_iota(
            jnp.int32, (tokens, tokens), 1
        )
        line = jnp.sum(jnp.where(same, scale, 0.0), axis=0, keepdims=True)
        scale_out[...] = jnp.broadcast_to(line, scale_out.shape)
    launch_if(fast, state_weights[1:])
    launch_if(fast & at_end, [give_x])
    launch(remote(scale_out, scale_in, p_s.at[3], p_r.at[3], sp=pair))
    with jax.named_scope("norm"):
        for slot in range(2):
            block = xf[:, pl.ds(pl.multiple_of((2 * slot + par) * rows, 128), rows)].astype(f32)
            normed[slot, own_rows] = (block * scale * gain_of(slot)).astype(bf)
    with jax.named_scope("tables"):
        columns_of = lax.fori_loop(10, groups, tables, columns_of)
    pump(2)
    launch_if(fast, early_keys)
    launch_if(slow, query_weights)
    pump(2)
    launch_if(fast, query_weights)
    with jax.named_scope("next_x"):
        remote(xp.at[t], xp.at[t], p_s.at[1], p_r.at[1], sp=pair).wait_recv()
    launch(remote(xp.at[t], xp.at[t], p_s.at[4], p_r.at[4], tp=other))
    with jax.named_scope("partner_x"):
        remote(xp.at[other], xp.at[other], p_s.at[4], p_r.at[4], tp=other).wait_recv()
        remote(scale_in, scale_in, p_s.at[3], p_r.at[3], sp=pair).wait_recv()
    with jax.named_scope("norm"):
        scale = column(scale_in[0:1, :])
        for slot in range(2):
            normed[slot, pair_rows] = (xp[slot].astype(f32) * scale * gain_of(slot)).astype(bf)
    for c in local[9:]:
        c.wait()
    with jax.named_scope("own_u"):
        total_in[...] = jnp.dot(normed[late], w_ssm[late], preferred_element_type=f32)

    def part_of(w, slot):
        return jnp.dot(normed[slot], w[slot], preferred_element_type=f32)

    def mine_at(e):
        return pl.ds(pl.multiple_of(e * wide, 128), wide)

    near_shift = shift_at(1 - par)
    remote(near_shift, near_shift, p_s.at[2], p_r.at[2], sp=pair).wait_recv()

    shape = (BLOCK, BLOCK)
    upto = lax.broadcasted_iota(jnp.int32, shape, 0) <= lax.broadcasted_iota(jnp.int32, shape, 1)
    tri = upto.astype(f32).astype(bf)
    both_shape = (2 * BLOCK, 2 * BLOCK)
    from_at, to_at = (lax.broadcasted_iota(jnp.int32, both_shape, i) for i in range(2))
    tri_both = ((from_at <= to_at) & ((from_at < BLOCK) == (to_at < BLOCK))).astype(f32).astype(bf)
    centre = BLOCK // 2
    eye = lax.broadcasted_iota(jnp.int32, (groups, BLOCK), 0) == lax.broadcasted_iota(
        jnp.int32, (groups, BLOCK), 1
    )

    def across(col):
        return jnp.sum(jnp.where(eye, col, 0.0), axis=0, keepdims=True)

    begins, lasts = [], []
    for b in range(2):
        piece_b = shift[:, b * BLOCK : (b + 1) * BLOCK]
        high, low = halves(piece_b)
        low2 = (piece_b - high.astype(f32) - low.astype(f32)).astype(bf)
        level = (
            jnp.dot(high, tri, preferred_element_type=f32)
            + jnp.dot(low, tri, preferred_element_type=f32)
            + jnp.dot(low2, tri, preferred_element_type=f32)
        )
        middle = level[:, centre : centre + 1]
        lifts[:, b * BLOCK : (b + 1) * BLOCK] = jnp.exp(middle - level)
        grown = jnp.exp(level - middle)
        grows[:, b * BLOCK : (b + 1) * BLOCK] = grown
        begins.append(across(jnp.exp(middle)))
        lasts.append(across(grown[:, BLOCK - 1 :]))
    rates, turns = columns_of

    def times(a, b):
        return a[0] * b[0] - a[1] * b[1], a[0] * b[1] + a[1] * b[0]

    def plus(a, b):
        return a[0] + b[0], a[1] + b[1]

    def scaled(row, a):
        return row * a[0], row * a[1]

    def spiral(count):
        fade = jnp.exp(-rates * count)
        return fade * jnp.cos(turns * count), fade * jnp.sin(turns * count)

    reach, end = spiral(centre + 1.0), spiral(BLOCK - 1.0 - centre)
    whole = times(reach, end)

    pump(2)
    narrow = wide // 2

    def state_inputs(h):
        with jax.named_scope("ssm_wait"):
            spread_done(0, (2 * h, 2 * h + 1))
        with jax.named_scope("project_u"):
            for e in range(2):
                lanes = slice(e * wide + h * narrow, e * wide + (h + 1) * narrow)
                total_in[:, lanes] += jnp.dot(
                    normed[1 - late], w_ssm[1 - late, :, lanes], preferred_element_type=f32
                )
            give_u[h] = total_in[:, half_at(1 - par, h)].astype(bf)
        launch(remote(give_u.at[h], got_u.at[h], g_s.at[3 * h], g_r.at[3 * h], sp=pair))

    def half_at(e, h):
        return pl.ds(pl.multiple_of(e * wide + h * narrow, 128), narrow)

    def turn_inputs(h):
        with jax.named_scope("got_u"):
            remote(got_u.at[h], got_u.at[h], g_s.at[3 * h], g_r.at[3 * h], sp=pair).wait_recv()
        with jax.named_scope("turn_u"):
            u = total_in[:, half_at(par, h)] + got_u[h].astype(f32)
            u_scr[h * narrow : (h + 1) * narrow, :] = jnp.transpose(u.astype(bf).astype(f32))

    state_inputs(0)
    state_inputs(1)
    launch_if(slow, out_weights)
    pump(2)
    turn_inputs(0)
    launch_if(fast, out_weights)
    launch_if(slow, attend_weights)

    def query_parts(h):
        with jax.named_scope("query_wait"):
            spread_done(1, (2 * h, 2 * h + 1))
        with jax.named_scope("project_q"):
            for e in range(2):
                lanes = slice(e * wide + h * narrow, e * wide + (h + 1) * narrow)
                total_q[:, lanes] = sum(
                    jnp.dot(normed[slot], w_query[slot, :, lanes], preferred_element_type=f32)
                    for slot in range(2)
                )
            give_q[h] = total_q[:, half_at(1 - par, h)].astype(bf)
        launch(remote(give_q.at[h], got_q.at[h], g_s.at[1 + 3 * h], g_r.at[1 + 3 * h], sp=pair))

    def key_parts():
        with jax.named_scope("key_wait"):
            spread_done(2)
        with jax.named_scope("project_kv"):
            keys = part_of(w_key, 0) + part_of(w_key, 1)
            values = part_of(w_value, 0) + part_of(w_value, 1)
            both = [
                jnp.concatenate([a[:, e * HEAD_DIM : (e + 1) * HEAD_DIM] for a in (keys, values)], axis=1)
                for e in range(2)
            ]
            give_kv[...] = jnp.where(par == 0, both[1], both[0]).astype(bf)
        launch(remote(give_kv, got_kv, g_s.at[2], g_r.at[2], sp=pair))

        return jnp.where(par == 0, both[0], both[1])

    tail = kv_scr.at[pl.ds(2 * WINDOW, WINDOW)]
    head = kv_scr.at[pl.ds(0, WINDOW)]
    hand_kv = remote(tail, head, p_s.at[5], p_r.at[5], sp=across_z)
    hand_state = remote(carry_out, carry_in, p_s.at[6], p_r.at[6], sp=across_z)

    def settle_kv():
        with jax.named_scope("kv_wait"):
            remote(got_kv, got_kv, g_s.at[2], g_r.at[2], sp=pair).wait_recv()
        kv_scr[WINDOW:, :] = (own_kv + got_kv[...].astype(f32)).astype(bf)

        @pl.when(late == 0)
        def _():
            hand_kv.start()
            kv_scr[:WINDOW, :] = jnp.zeros((WINDOW, kv_scr.shape[1]), bf)

    lane = lax.broadcasted_iota(jnp.int32, (state, BLOCK), 1)
    ends = [jnp.zeros((state, BLOCK), f32)] * 4
    for g in range(groups):
        if g == groups // 2:
            turn_inputs(1)
            launch_if(fast, attend_weights)
        with jax.named_scope("first"):
            u = u_scr[g * GROUP_CH : (g + 1) * GROUP_CH, :]
            drive = jnp.dot(inm[g], u.astype(bf), preferred_element_type=f32)
            up_re = jnp.concatenate([tab[g, 0]] * 2, axis=1)
            up_im = jnp.concatenate([tab[g, 1]] * 2, axis=1)
            row = lifts[g : g + 1, :]
            d_re, d_im = drive[:state] * row, drive[state:] * row
            lifted = jnp.concatenate([d_re * up_re - d_im * up_im, d_re * up_im + d_im * up_re], axis=0)
            sums = jnp.dot(lifted.astype(bf), tri_both, preferred_element_type=f32)
            prefix[g] = sums
            ends = [
                jnp.where(
                    lane == g,
                    sums[i % 2 * state : (i % 2 + 1) * state, (i // 2 + 1) * BLOCK - 1 : (i // 2 + 1) * BLOCK],
                    ends[i],
                )
                for i in range(4)
            ]
        if g == 5:
            own_kv = key_parts()
        if g in (1, 3, 9):
            pump(1)
        if g == 11:
            query_parts(0)
            if False:
                pump(1)
    with jax.named_scope("carry"):
        own = [scaled(lasts[b], times(end, (ends[2 * b], ends[2 * b + 1]))) for b in range(2)]
        decay = [scaled(lasts[b] * begins[b], whole) for b in range(2)]
        final = plus(own[1], times(decay[1], own[0]))
        carry_out[...] = jnp.transpose(jnp.concatenate(final, axis=0))[:groups]

    @pl.when(late == 0)
    def _():
        hand_state.start()
        carry_in[...] = jnp.zeros(carry_in.shape, f32)

    query_parts(1)
    settle_kv()
    pump(1)

    @pl.when(late == 1)
    def _():
        with jax.named_scope("hand_state"):
            hand_state.wait_recv()

    back = jnp.transpose(carry_in[...])
    entry = (back[:state], back[state:])

    def bases(row, c):
        return scaled(row, times(c, reach))

    def grown_entry(c):
        return plus((own[0][0][:, :groups], own[0][1][:, :groups]),
                    times((decay[0][0][:, :groups], decay[0][1][:, :groups]), c))

    cut = (reach[0][:, :groups], reach[1][:, :groups])
    base = [
        scaled(begins[0][:, :groups], times(entry, cut)),
        scaled(begins[1][:, :groups], times(grown_entry(entry), cut)),
    ]
    for g in range(groups):
        with jax.named_scope("second"):
            u = u_scr[g * GROUP_CH : (g + 1) * GROUP_CH, :]
            down = [jnp.concatenate([tab[g, i]] * 2, axis=1) for i in (2, 3)]
            chosen = lax.broadcasted_iota(jnp.int32, skip.shape, 1) == first + g
            skips = jnp.sum(jnp.where(chosen, skip[...], 0.0), axis=1, keepdims=True)
            p = [
                prefix[g, i * state : (i + 1) * state]
                + jnp.concatenate(
                    [jnp.broadcast_to(base[b][i][:, g : g + 1], (state, BLOCK)) for b in range(2)], axis=1
                )
                for i in range(2)
            ]
            states = jnp.concatenate(scaled(grows[g : g + 1, :], times(down, p)), axis=0).astype(bf)
            y = jnp.dot(read[g], states, preferred_element_type=f32)
            y_scr[g * GROUP_CH : (g + 1) * GROUP_CH, :] = y + skips * u
        if (g + 1) % (groups // 2) == 0:
            side = (g + 1) // (groups // 2) - 1
            lanes = slice(side * BLOCK, (side + 1) * BLOCK)
            with jax.named_scope("gelu"):
                act_s[par, :, lanes] = jnp.transpose(jax.nn.gelu(y_scr[lanes, :])).astype(bf)
            half_s = act_s.at[par, :, pl.ds(side * BLOCK, BLOCK)]
            launch(remote(half_s, half_s, e_s.at[6 + side], e_r.at[6 + side], sp=pair))

    gap_shape = (WINDOW, 2 * WINDOW)
    at = lax.broadcasted_iota(jnp.int32, gap_shape, 1)
    gap = lax.broadcasted_iota(jnp.int32, gap_shape, 0) + WINDOW - at
    inside = (gap >= 0) & (gap < WINDOW)
    inside_first = inside & (at >= WINDOW * (1 - late))
    sink_lane = lax.broadcasted_iota(jnp.int32, sinks.shape, 1)
    pump(1)
    for side in range(2):
        pump(1)
        with jax.named_scope("q_wait"):
            remote(got_q.at[side], got_q.at[side], g_s.at[1 + 3 * side], g_r.at[1 + 3 * side], sp=pair).wait_recv()
        q_scr[:, side * narrow : (side + 1) * narrow] = (
            (total_q[:, half_at(par, side)] + got_q[side].astype(f32)) * HEAD_DIM ** (-0.5)
        ).astype(bf)
        for b in (1, 0):
            if b == 0 and side == 0:

                @pl.when(late == 1)
                def _():
                    with jax.named_scope("hand_kv"):
                        hand_kv.wait_recv()

            keys = kv_scr[b * WINDOW : (b + 2) * WINDOW, :HEAD_DIM]
            values = kv_scr[b * WINDOW : (b + 2) * WINDOW, HEAD_DIM:]
            valid = inside if b else inside_first
            outs = []
            for h in range(side * heads // 2, (side + 1) * heads // 2):
                with jax.named_scope("head"):
                    q = q_scr[b * WINDOW : (b + 1) * WINDOW, h * HEAD_DIM : (h + 1) * HEAD_DIM]
                    scores = lax.dot_general(q, keys, (((1,), (1,)), ((), ())), preferred_element_type=f32)
                    scores = jnp.where(valid, scores, floor_score)
                    sink = jnp.sum(
                        jnp.where(sink_lane == par * heads + h, sinks[...], 0.0), axis=1, keepdims=True
                    )
                    peak = jnp.maximum(jnp.max(scores, axis=1, keepdims=True), sink)
                    raised = jnp.exp(scores - peak)
                    total = jnp.sum(raised, axis=1, keepdims=True) + jnp.exp(sink - peak)
                    weights = (raised * (1.0 / total)).astype(bf)
                    outs.append(jnp.dot(weights, values, preferred_element_type=f32))
            act_a[par, b * BLOCK : (b + 1) * BLOCK, side * narrow : (side + 1) * narrow] = jnp.concatenate(
                outs, axis=1
            ).astype(bf)
        half_a = act_a.at[par, :, pl.ds(side * narrow, narrow)]
        launch(remote(half_a, half_a, e_s.at[4 + side], e_r.at[4 + side], sp=pair))

    size, chunk = tokens // 2, cols // 2
    def state_part(slot):
        for side in range(2):
            lanes = slice(side * chunk, (side + 1) * chunk)
            both = [jnp.dot(act_s[e], wo_s[slot, e * wide : (e + 1) * wide, lanes], preferred_element_type=f32)
                    for e in range(2)]
            pa[slot, :, lanes] = both[0] + both[1]

    with jax.named_scope("mix_s"):
        for side in range(2):
            theirs = act_s.at[1 - par, :, pl.ds(side * BLOCK, BLOCK)]
            remote(theirs, theirs, e_s.at[6 + side], e_r.at[6 + side], sp=pair).wait_recv()
    with jax.named_scope("state"):
        state_part(late)
    pump(len(queue))
    with jax.named_scope("out_wait"):
        spread_done(3)
    with jax.named_scope("state"):
        state_part(1 - late)
    with jax.named_scope("mix_a"):
        for side in range(2):
            theirs = act_a.at[1 - par, :, pl.ds(side * narrow, narrow)]
            remote(theirs, theirs, e_s.at[4 + side], e_r.at[4 + side], sp=pair).wait_recv()

    def target(who, i):
        first_column = lax.rem(who + 2 * (i // 2), n) * cols + (i % 2) * chunk
        return out.at[:, pl.ds(pl.multiple_of(first_column, 128), chunk)]

    def multiply(i):
        slot, lanes = late if i < 2 else 1 - late, slice(i % 2 * chunk, (i % 2 + 1) * chunk)
        total = pa[slot, :, lanes]
        for e in range(2):
            total = total + jnp.dot(
                act_a[e], wo_a[slot, e * wide : (e + 1) * wide, lanes], preferred_element_type=f32
            )
        for e in range(2):
            for side in range(2):
                block = total[e * tokens + side * size : e * tokens + (side + 1) * size]
                pf[i, e, side] = block
                pb[i, side, e] = block.astype(bf)
        launch(remote(pb.at[i, other], got.at[i], d_s.at[i], d_r.at[i], tp=other))

    def pass_on(i):
        remote(got.at[i], got.at[i], d_s.at[i], d_r.at[i], tp=other).wait_recv()
        fsend[i] = (pf[i, 1 - par, t] + got[i, 1 - par].astype(f32)).astype(bf)
        launch(remote(fsend.at[i], target(k, i), e_s.at[i], e_r.at[i], sp=pair))
        res[i] = (pf[i, par, t] + got[i, par].astype(f32)).astype(bf)
        launch(pltpu.make_async_copy(res.at[i], target(k, i), o_s.at[i]))

    for i in range(4):
        if i == 2:
            with jax.named_scope("out_wait"):
                spread_done(4)
        with jax.named_scope("multiply"):
            multiply(i)
        if i:
            with jax.named_scope("pass"):
                pass_on(i - 1)
    with jax.named_scope("pass"):
        pass_on(3)
    with jax.named_scope("settle"):
        for i in range(4):
            theirs = target(pair, i)
            remote(theirs, theirs, e_s.at[i], e_r.at[i], sp=pair).wait_recv()

    with jax.named_scope("drain"):
        for c in sent:
            if c.is_remote:
                c.wait_send()
            else:
                c.wait()

    @pl.when(late == 0)
    def _():
        hand_kv.wait_send()
        hand_state.wait_send()


def layer(x, gain, ssm, query, key, value, rate, turn, parts, reads, skip, shift, sinks, ows, owa):
    bf, f32 = jnp.bfloat16, jnp.float32
    tokens, half = x.shape
    rows, cols = ows.shape[0], ows.shape[1]
    wide = ssm.shape[1] // 2
    groups, state = rate.shape[0] // 2, rate.shape[1]
    length = 2 * tokens
    dma = pltpu.SemaphoreType.DMA
    vm = pltpu.VMEM
    return pl.pallas_call(
        layer_kernel,
        out_shape=jax.ShapeDtypeStruct((tokens // 2, 4 * cols), bf),
        in_specs=[ANY] * 15,
        out_specs=ANY,
        scratch_shapes=[
            vm((tokens, 2 * half), bf), vm((2, tokens, rows), bf), vm((2, length, rows), bf),
            vm((2, rows, 2 * wide), bf), vm((2, rows, 2 * wide), bf), vm((2,) + key.shape, bf),
            vm((2,) + value.shape, bf), vm((2, rows, cols), bf), vm((2, rows, cols), bf),
            vm(gain.shape, f32), vm(rate.shape, f32), vm(turn.shape, f32),
            vm(parts.shape, bf), vm(reads.shape, bf), vm(skip.shape, f32),
            vm((groups, length), f32), vm(sinks.shape, f32),
            vm((groups, 4, state, BLOCK), f32), vm((groups, 2 * state, GROUP_CH), bf),
            vm((groups, GROUP_CH, 2 * state), bf), vm((groups, length), f32), vm((groups, length), f32),
            vm((groups, 2 * state, length), f32), vm((wide, length), f32), vm((length, wide), bf),
            vm((length + WINDOW, 2 * HEAD_DIM), bf), vm((wide, length), f32),
            vm((2, length, wide), bf), vm((2, length, wide), bf),
            vm((groups, 2 * state), f32), vm((groups, 2 * state), f32),
            vm((8, tokens), f32), vm((8, tokens), f32), vm((length, 2 * wide), f32), vm((length, 2 * wide), f32),
            vm((2, length, wide // 2), bf), vm((2, length, wide // 2), bf), vm((length, 2 * HEAD_DIM), bf),
            vm((2, length, wide // 2), bf), vm((2, length, wide // 2), bf), vm((length, 2 * HEAD_DIM), bf),
            vm((2, length, cols), f32),
            vm((4, 2, 2, tokens // 2, cols // 2), f32), vm((4, 2, 2, tokens // 2, cols // 2), bf),
            vm((4, 2, tokens // 2, cols // 2), bf), vm((4, tokens // 2, cols // 2), bf),
            vm((4, tokens // 2, cols // 2), bf),
            dma((15,)), dma((5, 4)), dma((5, 4)), dma((7,)), dma((7,)), dma((5, 4, 3)), dma((5, 4, 3)),
            dma((5,)), dma((5,)), dma((4,)), dma((4,)), dma((8,)), dma((8,)), dma((4,)),
        ],
        compiler_params=pltpu.CompilerParams(collective_id=0, has_side_effects=True),
    )(x, gain, ssm, query, key, value, rate, turn, parts, reads, skip, shift, sinks, ows, owa)


def fast_body(
    inputs, norm_gain, in_ssm, in_query, in_key, in_value, decay_rate, rotation, input_parts,
    output_parts, skip_scale, decay_shift, sink_logit, out_state, out_attend,
):
    return layer(
        inputs, norm_gain[None], in_ssm, in_query, in_key, in_value, decay_rate, rotation,
        jnp.swapaxes(input_parts, 2, 3), output_parts, skip_scale.T, jnp.transpose(decay_shift),
        sink_logit[None], out_state, out_attend,
    )


def body(*args):
    n, n_fs, n_tp = lax.axis_size("sp"), lax.axis_size("fs"), lax.axis_size("tp")
    inputs, in_ssm, in_query, in_key, decay_rate = args[0], args[2], args[3], args[4], args[6]
    key_heads = in_key.shape[1] // HEAD_DIM
    query_heads = in_query.shape[1] // HEAD_DIM
    fits = (
        n_tp == 2
        and n == 4
        and n_fs == 4
        and key_heads == 2
        and query_heads % 4 == 0
        and query_heads * HEAD_DIM == in_ssm.shape[1]
        and in_ssm.shape[1] % 256 == 0
        and in_ssm.shape[1] == args[13].shape[0] == args[14].shape[0]
        and decay_rate.shape[0] % 32 == 0
        and decay_rate.shape[0] <= 2 * BLOCK
        and decay_rate.shape[1] * 2 == BLOCK
        and decay_rate.shape[0] * GROUP_CH == in_ssm.shape[1]
        and inputs.shape[0] == BLOCK == WINDOW
        and inputs.shape[1] % 128 == 0
        and in_ssm.shape[0] % 128 == 0
        and in_ssm.shape[0] == args[13].shape[0]
        and inputs.shape[1] == 2 * in_ssm.shape[0]
        and args[13].shape[1] % 128 == 0
    )
    return (fast_body if fits else general_body)(*args)


def solution(mesh):
    return jax.shard_map(
        body,
        mesh=mesh,
        in_specs=(
            P(("fs", "sp"), "tp"),
            P(),
            P("sp", "tp"),
            P("sp", "tp"),
            P("sp", "tp"),
            P("sp", "tp"),
            P("tp", None),
            P("tp", None),
            P(None, "tp", None, None),
            P(None, "tp", None, None),
            P("tp", None),
            P(("fs", "sp"), "tp"),
            P("tp"),
            P("tp", "sp"),
            P("tp", "sp"),
        ),
        out_specs=P(("fs", "sp", "tp"), None),
        check_vma=False,
    )
```

```python
import functools
import jax
import jax.numpy as jnp
from jax import lax
from jax.experimental import pallas as pl
from jax.experimental.pallas import tpu as pltpu
from jax.sharding import PartitionSpec as P

GROUP_CH = 16
HEAD_DIM = 64
WINDOW = 128
BLOCK = 128


epsilon = 1e-06
floor_score = -1e30


def prefix(x, axis, join, neutral):
    place = lax.axis_index(axis)
    gathered = jax.tree.map(
        lambda a, kind: lax.all_gather(a.astype(kind), axis),
        x,
        (jnp.bfloat16, jnp.bfloat16, jnp.bfloat16, jnp.bfloat16),
    )
    state = jax.tree.map(lambda a, e: jnp.zeros_like(a) + jnp.asarray(e, a.dtype), x, neutral)

    def one(hop, state):
        return join(
            state,
            jax.tree.map(
                lambda a, own: lax.dynamic_index_in_dim(a, hop, 0, False).astype(own.dtype),
                gathered,
                x,
            ),
        )

    return lax.fori_loop(0, place, one, state)


def from_behind(value, axis, steps):
    count = lax.axis_size(axis)
    initial, last = (max(0, -steps), min(count, count - steps))
    return lax.ppermute(value, axis, [(source, source + steps) for source in range(initial, last)])


def combine(earlier, later):
    first_re, first_im, state_re, state_im = earlier
    second_re, second_im, input_re, input_im = later
    return (
        second_re * first_re - second_im * first_im,
        second_re * first_im + second_im * first_re,
        second_re * state_re - second_im * state_im + input_re,
        second_re * state_im + second_im * state_re + input_im,
    )


def input_matrix(decay_rate, rotation, input_parts):
    damped = jnp.exp(-decay_rate)
    lift_re = damped * jnp.cos(rotation) - 1.0
    lift_im = damped * jnp.sin(rotation)
    modulus = decay_rate * decay_rate + rotation * rotation
    factor_re = (rotation * lift_im - decay_rate * lift_re) / modulus
    factor_im = -(rotation * lift_re + decay_rate * lift_im) / modulus
    part_re = input_parts[0].astype(jnp.float32)
    part_im = input_parts[1].astype(jnp.float32)
    joined_re = factor_re[:, :, None] * part_re - factor_im[:, :, None] * part_im
    joined_im = factor_re[:, :, None] * part_im + factor_im[:, :, None] * part_re
    return jnp.concatenate([joined_re, joined_im], axis=1).astype(jnp.bfloat16)


def window_attention(queries, keys_win, values_win, starts, sink_logit):
    window = queries.shape[1]
    scores = jnp.einsum("nqgrd,nkgd->ngrqk", queries, keys_win, preferred_element_type=jnp.float32)
    scores = scores * queries.shape[-1] ** (-0.5)
    places = (
        jnp.arange(window, dtype=jnp.int32)[:, None]
        + window
        - jnp.arange(2 * window, dtype=jnp.int32)[None, :]
    )
    inside = (places >= 0) & (places < window)
    reach = starts[:, None] - window + jnp.arange(2 * window, dtype=jnp.int32)[None, :] >= 0
    valid = (inside[None] & reach[:, None, :])[:, None, None]
    sinks = sink_logit.reshape(scores.shape[1], scores.shape[2])[None, :, :, None, None]
    scores = jnp.where(valid, scores, floor_score)
    row_peak = jnp.maximum(jnp.max(scores, axis=-1, keepdims=True), sinks)
    raised = jnp.where(valid, jnp.exp(scores - row_peak), 0.0)
    denominator = jnp.sum(raised, axis=-1, keepdims=True) + jnp.exp(sinks - row_peak)
    weights = (raised / denominator).astype(jnp.bfloat16)
    result = jnp.einsum(
        "ngrqk,nkgd->nqgrd", weights, values_win, preferred_element_type=jnp.float32
    )
    return result.astype(jnp.bfloat16)


def general_body(
    inputs,
    norm_gain,
    in_ssm,
    in_query,
    in_key,
    in_value,
    decay_rate,
    rotation,
    input_parts,
    output_parts,
    skip_scale,
    decay_shift,
    sink_logit,
    out_state,
    out_attend,
):
    gathered = lax.all_gather(inputs, "tp", axis=1, tiled=True)
    length = gathered.shape[0]
    widened = gathered.astype(jnp.float32)
    scale = lax.rsqrt(jnp.mean(widened * widened, axis=1, keepdims=True) + epsilon)
    normed = (widened * scale * norm_gain).astype(jnp.bfloat16)

    def add_rows(pieces):
        return tuple(
            (jnp.dot(normed, piece, preferred_element_type=jnp.float32) for piece in pieces)
        )

    projected = add_rows(
        (
            lax.all_gather(in_ssm, "sp", axis=0, tiled=True),
            lax.all_gather(in_query, "sp", axis=0, tiled=True),
            lax.all_gather(in_key, "sp", axis=0, tiled=True),
            lax.all_gather(in_value, "sp", axis=0, tiled=True),
        )
    )
    drive_in, queries, keys_local, values = [piece.astype(jnp.bfloat16) for piece in projected]
    groups = decay_rate.shape[0]
    state_dim = decay_rate.shape[1]
    channels = groups * GROUP_CH
    highest = lax.Precision.HIGHEST
    drive_cols = jnp.transpose(drive_in).reshape(groups, GROUP_CH, length)
    in_matrix = input_matrix(decay_rate, rotation, input_parts)
    drive = jnp.einsum("gqh,ght->gqt", in_matrix, drive_cols, preferred_element_type=jnp.float32)
    shift_cols = jnp.transpose(decay_shift)
    running = jnp.cumsum(shift_cols, axis=1)
    total_shift = running[:, -1]
    remain = length - 1.0 - jnp.arange(length, dtype=jnp.float32)
    to_end = (total_shift[:, None] - running)[:, None, :] - decay_rate[:, :, None] * remain[
        None, None, :
    ]
    fade = jnp.exp(to_end)
    turn = rotation[:, :, None] * remain[None, None, :]
    weight_re = fade * jnp.cos(turn)
    weight_im = fade * jnp.sin(turn)
    drive_re = drive[:, :state_dim]
    drive_im = drive[:, state_dim:]
    final_re = jnp.sum(weight_re * drive_re - weight_im * drive_im, axis=2)
    final_im = jnp.sum(weight_re * drive_im + weight_im * drive_re, axis=2)
    overall = jnp.exp(total_shift[:, None] - decay_rate * length)
    nothing = jnp.zeros_like(final_re)
    carried = prefix(
        (
            overall * jnp.cos(rotation * length),
            overall * jnp.sin(rotation * length),
            final_re,
            final_im,
        ),
        "sp",
        combine,
        (jnp.ones_like(final_re), nothing, nothing, nothing),
    )
    key_heads = keys_local.shape[1] // HEAD_DIM
    query_heads = queries.shape[1] // HEAD_DIM
    windows_dev = length // WINDOW
    previous = from_behind((keys_local, values), "sp", 1)

    def windows(flat, before):
        split = jnp.concatenate([before, flat], axis=0).reshape(
            windows_dev + 1, WINDOW, key_heads, HEAD_DIM
        )
        return jnp.concatenate([split[:-1], split[1:]], axis=1)

    offset = lax.axis_index("sp") * length
    starts = offset + jnp.arange(windows_dev, dtype=jnp.int32) * WINDOW
    queries_blk = queries.reshape(
        windows_dev, WINDOW, key_heads, query_heads // key_heads, HEAD_DIM
    )
    attended = window_attention(
        queries_blk,
        windows(keys_local, previous[0]),
        windows(values, previous[1]),
        starts,
        sink_logit,
    )
    attend_out = attended.reshape(length, query_heads * HEAD_DIM)
    blocks = length // BLOCK
    triangle = (
        jnp.arange(BLOCK, dtype=jnp.int32)[:, None] <= jnp.arange(BLOCK, dtype=jnp.int32)[None, :]
    ).astype(jnp.float32)
    offsets = jnp.arange(BLOCK, dtype=jnp.float32)
    centre = BLOCK // 2
    read_re = output_parts[0].astype(jnp.float32)
    read_im = output_parts[1].astype(jnp.float32)
    angle = rotation[:, :, None] * (offsets - centre)[None, None, :]
    cos_angle = jnp.cos(angle)
    sin_angle = jnp.sin(angle)
    phase = rotation[:, :, None] * (offsets + 1.0)[None, None, :]
    cos_phase = jnp.cos(phase)
    sin_phase = jnp.sin(phase)

    def advance(carry, pieces):
        carry_re, carry_im = carry
        part_re, part_im, shift_part, grouped_part = pieces
        level = jnp.dot(shift_part, triangle, precision=highest)
        log_from = level[:, None, :] - decay_rate[:, :, None] * (offsets + 1.0)[None, None, :]
        relative = log_from - log_from[:, :, centre : centre + 1]
        shrink = jnp.exp(-relative)
        lift_re = shrink * (part_re * cos_angle + part_im * sin_angle)
        lift_im = shrink * (part_im * cos_angle - part_re * sin_angle)
        prefix_re = jnp.dot(lift_re.reshape(groups * state_dim, BLOCK), triangle, precision=highest)
        prefix_im = jnp.dot(lift_im.reshape(groups * state_dim, BLOCK), triangle, precision=highest)
        prefix_re = prefix_re.reshape(groups, state_dim, BLOCK)
        prefix_im = prefix_im.reshape(groups, state_dim, BLOCK)
        grow = jnp.exp(relative)
        from_start = jnp.exp(log_from)
        keep_re = from_start * cos_phase
        keep_im = from_start * sin_phase
        state_re = grow * (prefix_re * cos_angle - prefix_im * sin_angle)
        state_im = grow * (prefix_im * cos_angle + prefix_re * sin_angle)
        state_re = state_re + keep_re * carry_re[:, :, None] - keep_im * carry_im[:, :, None]
        state_im = state_im + keep_re * carry_im[:, :, None] + keep_im * carry_re[:, :, None]
        result = jnp.einsum("ghp,gpt->ght", read_re, state_re, precision=highest)
        result = result - jnp.einsum("ghp,gpt->ght", read_im, state_im, precision=highest)
        result = result + skip_scale[:, :, None] * grouped_part.astype(jnp.float32)
        return ((state_re[:, :, -1], state_im[:, :, -1]), jax.nn.gelu(result).astype(jnp.bfloat16))

    drive_blocks = jnp.transpose(drive.reshape(groups, 2 * state_dim, blocks, BLOCK), (2, 0, 1, 3))
    shift_blocks = jnp.transpose(shift_cols.reshape(groups, blocks, BLOCK), (1, 0, 2))
    grouped_blocks = jnp.transpose(
        drive_cols.reshape(groups, GROUP_CH, blocks, BLOCK), (2, 0, 1, 3)
    )
    _, state_blocks = lax.scan(
        advance,
        (carried[2], carried[3]),
        (
            drive_blocks[:, :, :state_dim],
            drive_blocks[:, :, state_dim:],
            shift_blocks,
            grouped_blocks,
        ),
    )
    state_out = jnp.transpose(state_blocks, (0, 3, 1, 2)).reshape(length, channels)
    column_state, column_attend = (
        lax.all_gather(out_state, "sp", axis=1, tiled=True),
        lax.all_gather(out_attend, "sp", axis=1, tiled=True),
    )
    result = jnp.dot(state_out, column_state, preferred_element_type=jnp.float32)
    return lax.psum_scatter(
        (result + jnp.dot(attend_out, column_attend, preferred_element_type=jnp.float32)).astype(
            jnp.bfloat16
        ),
        "tp",
        scatter_dimension=0,
        tiled=True,
    )


MESH = pl.DeviceIdType.MESH
ANY = pl.BlockSpec(memory_space=pl.ANY)


def remote(src, dst, send, recv, **where):
    return pltpu.make_async_remote_copy(
        src_ref=src, dst_ref=dst, send_sem=send, recv_sem=recv, device_id=where, device_id_type=MESH
    )


def greet(peers):
    barrier = pltpu.get_barrier_semaphore()
    for peer in peers:
        pl.semaphore_signal(barrier, inc=1, device_id=peer, device_id_type=MESH)
    pl.semaphore_wait(barrier, len(peers))


def halves(x):
    high = x.astype(jnp.bfloat16)
    return high, (x - high.astype(jnp.float32)).astype(jnp.bfloat16)


def split_dot(x, exact):
    high, low = halves(x)
    return jnp.dot(high, exact, preferred_element_type=jnp.float32) + jnp.dot(
        low, exact, preferred_element_type=jnp.float32
    )


def column(row):
    size = row.shape[1]
    same = lax.broadcasted_iota(jnp.int32, (size, size), 0) == lax.broadcasted_iota(
        jnp.int32, (size, size), 1
    )
    return jnp.sum(jnp.where(same, row, 0.0), axis=1, keepdims=True)


def turned(angle):
    quarter = jnp.floor(angle * (2.0 / 3.141592653589793) + 0.5)
    r = ((angle - quarter * 1.5703125) - quarter * 4.837512969970703e-4) - quarter * 7.549789948768648e-8
    sq = r * r
    sin = r + r * sq * (-1.6666654611e-1 + sq * (8.3321608736e-3 + sq * -1.9515295891e-4))
    cos = 1.0 - 0.5 * sq + sq * sq * (4.166664568298827e-2 + sq * (-1.388731625493765e-3 + sq * 2.443315711809948e-5))
    which = quarter.astype(jnp.int32)
    swap = (which & 1) == 1
    flip_cos = ((which + 1) & 2) == 2
    flip_sin = (which & 2) == 2
    a, b = jnp.where(swap, sin, cos), jnp.where(swap, cos, sin)
    return jnp.where(flip_cos, -a, a), jnp.where(flip_sin, -b, b)


def layer_kernel(x_in, gain_in, ssm, query, key_in, value_in, rate_in, turn_in, parts_in, reads_in,
                 skip_in, shift_in, sinks_in, ows, owa, out,
                 xf, xp, normed, w_ssm, w_query, w_key, w_value, wo_s, wo_a, gain, rate, turn,
                 parts, reads, skip, shift, sinks, tab, inm, read, lifts, grows, prefix, u_scr, q_scr,
                 kv_scr, y_scr, act_s, act_a, carry_out, carry_in, scale_out, scale_in, total_in, total_q,
                 give_u, give_q, give_kv, got_u, got_q, got_kv, pa, pf, pb, got, fsend, res,
                 loc, z_s, z_r, p_s, p_r, x_s, x_r, g_s, g_r, d_s, d_r, e_s, e_r, o_s):
    f32, bf = jnp.float32, jnp.bfloat16
    k, f, t = lax.axis_index("sp"), lax.axis_index("fs"), lax.axis_index("tp")
    n, n_fs = 4, 4
    tokens, half = x_in.shape
    rows, cols = ssm.shape[0], ows.shape[1]
    wide = w_ssm.shape[2] // 2
    groups, state = tab.shape[0], tab.shape[2]
    heads = wide // HEAD_DIM
    par, late = lax.rem(k, 2), lax.div(k, 2)
    pair = k + 1 - 2 * par
    other = 1 - t
    fx, fy, far = f + 1 - 2 * lax.rem(f, 2), lax.rem(f + 2, n_fs), n_fs - 1 - f
    across_z = lax.rem(k + 2, n)

    part = rows // n_fs
    into = (w_ssm, w_query, None, wo_s, wo_a)
    origin = (ssm, query, None, ows, owa)
    cuts = (4, 4, 2, 2, 4)

    def stripe(c):
        return pl.ds(c % 2 * wide + c // 2 * (wide // 2), wide // 2)

    def region(w, c, q, slot):
        if w < 2:
            return into[w].at[slot, pl.ds(pl.multiple_of(q * part, 16), part), stripe(c)]
        if w == 2:
            return (w_key, w_value)[c].at[slot, pl.ds(pl.multiple_of(q * part, 16), part)]
        size = part // cuts[w]
        return into[w].at[slot, pl.ds(pl.multiple_of(q * part + c * size, 16), size)]

    def over_z(w, c):
        if w < 2:
            source = origin[w].at[pl.ds(pl.multiple_of(f * part, 16), part), stripe(c)]
        elif w == 2:
            source = (key_in, value_in)[c].at[pl.ds(pl.multiple_of(f * part, 16), part)]
        else:
            size = part // cuts[w]
            source = origin[w].at[pl.ds(pl.multiple_of(f * part + c * size, 16), size)]
        return remote(source, region(w, c, f, late), z_s.at[w, c], z_r.at[w, c], sp=across_z)

    def spread_here(w, c):
        block = region(w, c, f, 1 - late)
        remote(block, block, z_s.at[w, c], z_r.at[w, c], sp=across_z).wait_recv()
        for i, who in enumerate((far, fx, fy)):
            launch(remote(block, block, x_s.at[w, c, i], x_r.at[w, c, i], fs=who))

    def spread_done(w, pieces=None):
        for c in pieces or range(cuts[w]):
            for i, who in enumerate((far, fx, fy)):
                block = region(w, c, who, 1 - late)
                remote(block, block, x_s.at[w, c, i], x_r.at[w, c, i], fs=who).wait_recv()

    sent = []

    def launch(c):
        c.start()
        sent.append(c)

    def shift_at(e):
        return shift.at[:, pl.ds(pl.multiple_of(e * tokens, 128), tokens)]

    def shift_rows(e):
        return shift_in.at[pl.ds(pl.multiple_of(e * groups, 8), groups)]

    queue = [(f"s{w}{c}", functools.partial(spread_here, w, c)) for w in (0, 2, 1, 3, 4) for c in range(cuts[w])]

    def pump(count):
        for _ in range(min(count, len(queue))):
            name, step = queue.pop(0)
            with jax.named_scope(name):
                step()

    local = [
        (rate_in, rate), (turn_in, turn), (parts_in, parts), (reads_in, reads), (skip_in, skip),
        (gain_in, gain), (sinks_in, sinks), (shift_rows(par), shift_at(par)),
        (x_in, xf.at[:, pl.ds(pl.multiple_of(t * half, 128), half)]),
        (ssm, w_ssm.at[late]), (query, w_query.at[late]), (key_in, w_key.at[late]),
        (value_in, w_value.at[late]), (ows, wo_s.at[late]), (owa, wo_a.at[late]),
    ]
    local = [pltpu.make_async_copy(a, b, loc.at[i]) for i, (a, b) in enumerate(local)]
    for c in local:
        c.start()
    first = par * groups

    def tables(g, columns_of):
        line, spin = rate[pl.ds(first + g, 1), :], turn[pl.ds(first + g, 1), :]
        rates, turns = column(line), column(spin)
        away = lax.broadcasted_iota(jnp.int32, (state, BLOCK), 1).astype(f32) - float(BLOCK // 2)
        angle = turns * away
        cos, sin = turned(angle)
        fade = jnp.exp(-rates * away)
        rise = jnp.exp(rates * away)
        tab[g, 0] = rise * cos
        tab[g, 1] = -(rise * sin)
        tab[g, 2] = fade * cos
        tab[g, 3] = fade * sin
        damped = jnp.exp(-line)
        lift_re = damped * jnp.cos(spin) - 1.0
        lift_im = damped * jnp.sin(spin)
        modulus = line * line + spin * spin
        factor_re = (spin * lift_im - line * lift_re) / modulus
        factor_im = -(spin * lift_re + line * lift_im) / modulus
        part_re = parts[0, first + g].astype(f32)
        part_im = parts[1, first + g].astype(f32)
        inm[g] = jnp.transpose(
            jnp.concatenate(
                [factor_re * part_re - factor_im * part_im, factor_re * part_im + factor_im * part_re],
                axis=1,
            )
        ).astype(bf)
        read[g] = jnp.concatenate(
            [reads[0, first + g].astype(f32), -reads[1, first + g].astype(f32)], axis=1
        ).astype(bf)
        spot = lax.broadcasted_iota(jnp.int32, (state, BLOCK), 1) == g
        return jnp.where(spot, rates, columns_of[0]), jnp.where(spot, turns, columns_of[1])

    columns_of = (jnp.zeros((state, BLOCK), f32), jnp.zeros((state, BLOCK), f32))
    early = (n - 1 - k) * (n - 1 - k)
    peers = [{"sp": pair}, {"sp": across_z}, {"fs": fx}, {"fs": fy}, {"fs": far}, {"tp": other}]
    barrier = pltpu.get_barrier_semaphore()
    for peer in peers:
        pl.semaphore_signal(barrier, inc=1, device_id=peer, device_id_type=MESH)

    def settle_params():
        for c in local[:8]:
            c.wait()

    pl.when(k < n - 1)(settle_params)
    with jax.named_scope("tables"):
        columns_of = lax.fori_loop(0, early, tables, columns_of)
    with jax.named_scope("greet"):
        pl.semaphore_wait(barrier, len(peers))
    at_end = k * (n - 1 - k) == 0
    sides = pl.ds(pl.multiple_of(t * half, 128), half)
    launch(remote(x_in, xf.at[:, sides], p_s.at[0], p_r.at[0], tp=other))
    slow, fast, at_mid = t == 0, t == 1, k * (n - 1 - k) > 0

    def launch_if(choice, copies):
        @pl.when(choice)
        def _():
            for c in copies:
                c.start()

    state_weights = [over_z(0, c) for c in range(cuts[0])]
    early_keys = [over_z(2, c) for c in range(2)]
    query_weights = [over_z(1, c) for c in range(cuts[1])]
    out_weights = [over_z(3, c) for c in range(2)]
    attend_weights = [over_z(4, c) for c in range(cuts[4])]
    give_x = remote(x_in.at[:, pl.ds(pl.multiple_of((1 - par) * rows, 128), rows)], xp.at[t],
                    p_s.at[1], p_r.at[1], sp=pair)
    launch(remote(shift_rows(1 - par), shift_at(par), p_s.at[2], p_r.at[2], sp=pair))
    state_weights[0].start()
    launch_if(slow, state_weights[1:])
    launch_if(slow | jnp.logical_not(at_end), [give_x])
    launch_if(slow, early_keys)
    sent.extend(state_weights + early_keys + query_weights + out_weights + attend_weights + [give_x])
    pl.when(k == n - 1)(settle_params)
    with jax.named_scope("tables"):
        columns_of = lax.fori_loop(early, 10, tables, columns_of)

    local[8].wait()
    theirs = xf.at[:, pl.ds(pl.multiple_of(other * half, 128), half)]
    with jax.named_scope("own_x"):
        remote(theirs, theirs, p_s.at[0], p_r.at[0], tp=other).wait_recv()

    def gain_of(slot):
        return gain[:, pl.ds(pl.multiple_of((2 * slot + par) * rows, 128), rows)]

    own_rows = pl.ds(pl.multiple_of(par * tokens, 128), tokens)
    pair_rows = pl.ds(pl.multiple_of((1 - par) * tokens, 128), tokens)
    with jax.named_scope("norm"):
        full = xf[...].astype(f32)
        scale = lax.rsqrt(jnp.mean(full * full, axis=1, keepdims=True) + epsilon)
        same = lax.broadcasted_iota(jnp.int32, (tokens, tokens), 0) == lax.broadcasted_iota(
            jnp.int32, (tokens, tokens), 1
        )
        line = jnp.sum(jnp.where(same, scale, 0.0), axis=0, keepdims=True)
        scale_out[...] = jnp.broadcast_to(line, scale_out.shape)
    launch_if(fast, state_weights[1:] + early_keys)
    launch_if(fast & at_end, [give_x])
    launch(remote(scale_out, scale_in, p_s.at[3], p_r.at[3], sp=pair))
    with jax.named_scope("norm"):
        for slot in range(2):
            block = xf[:, pl.ds(pl.multiple_of((2 * slot + par) * rows, 128), rows)].astype(f32)
            normed[slot, own_rows] = (block * scale * gain_of(slot)).astype(bf)
    with jax.named_scope("tables"):
        columns_of = lax.fori_loop(10, groups, tables, columns_of)
    hand_x = remote(xp.at[t], xp.at[t], p_s.at[4], p_r.at[4], tp=other)
    sent.append(hand_x)

    def take_x():
        with jax.named_scope("next_x"):
            remote(xp.at[t], xp.at[t], p_s.at[1], p_r.at[1], sp=pair).wait_recv()
        hand_x.start()

    pump(1)
    pl.when(at_end)(take_x)
    pump(1)
    pump(2)
    for c in query_weights:
        c.start()
    near_shift = shift_at(1 - par)
    remote(near_shift, near_shift, p_s.at[2], p_r.at[2], sp=pair).wait_recv()

    shape = (BLOCK, BLOCK)
    upto = lax.broadcasted_iota(jnp.int32, shape, 0) <= lax.broadcasted_iota(jnp.int32, shape, 1)
    tri = upto.astype(f32).astype(bf)
    both_shape = (2 * BLOCK, 2 * BLOCK)
    from_at, to_at = (lax.broadcasted_iota(jnp.int32, both_shape, i) for i in range(2))
    tri_both = ((from_at <= to_at) & ((from_at < BLOCK) == (to_at < BLOCK))).astype(f32).astype(bf)
    centre = BLOCK // 2
    eye = lax.broadcasted_iota(jnp.int32, (groups, BLOCK), 0) == lax.broadcasted_iota(
        jnp.int32, (groups, BLOCK), 1
    )

    def across(col):
        return jnp.sum(jnp.where(eye, col, 0.0), axis=0, keepdims=True)

    begins, lasts = [], []
    for b in range(2):
        piece_b = shift[:, b * BLOCK : (b + 1) * BLOCK]
        high, low = halves(piece_b)
        low2 = (piece_b - high.astype(f32) - low.astype(f32)).astype(bf)
        level = (
            jnp.dot(high, tri, preferred_element_type=f32)
            + jnp.dot(low, tri, preferred_element_type=f32)
            + jnp.dot(low2, tri, preferred_element_type=f32)
        )
        middle = level[:, centre : centre + 1]
        lifts[:, b * BLOCK : (b + 1) * BLOCK] = jnp.exp(middle - level)
        grown = jnp.exp(level - middle)
        grows[:, b * BLOCK : (b + 1) * BLOCK] = grown
        begins.append(across(jnp.exp(middle)))
        lasts.append(across(grown[:, BLOCK - 1 :]))
    rates, turns = columns_of

    def times(a, b):
        return a[0] * b[0] - a[1] * b[1], a[0] * b[1] + a[1] * b[0]

    def plus(a, b):
        return a[0] + b[0], a[1] + b[1]

    def scaled(row, a):
        return row * a[0], row * a[1]

    def spiral(count):
        fade = jnp.exp(-rates * count)
        return fade * jnp.cos(turns * count), fade * jnp.sin(turns * count)

    reach, end = spiral(centre + 1.0), spiral(BLOCK - 1.0 - centre)
    whole = times(reach, end)

    pl.when(at_mid)(take_x)
    with jax.named_scope("partner_x"):
        remote(xp.at[other], xp.at[other], p_s.at[4], p_r.at[4], tp=other).wait_recv()
        remote(scale_in, scale_in, p_s.at[3], p_r.at[3], sp=pair).wait_recv()
    with jax.named_scope("norm"):
        scale = column(scale_in[0:1, :])
        for slot in range(2):
            normed[slot, pair_rows] = (xp[slot].astype(f32) * scale * gain_of(slot)).astype(bf)
    for c in local[9:]:
        c.wait()
    with jax.named_scope("own_u"):
        total_in[...] = jnp.dot(normed[late], w_ssm[late], preferred_element_type=f32)

    def part_of(w, slot):
        return jnp.dot(normed[slot], w[slot], preferred_element_type=f32)

    def mine_at(e):
        return pl.ds(pl.multiple_of(e * wide, 128), wide)


    narrow = wide // 2

    def state_inputs(h):
        with jax.named_scope("ssm_wait"):
            spread_done(0, (2 * h, 2 * h + 1))
        with jax.named_scope("project_u"):
            for e in range(2):
                lanes = slice(e * wide + h * narrow, e * wide + (h + 1) * narrow)
                total_in[:, lanes] += jnp.dot(
                    normed[1 - late], w_ssm[1 - late, :, lanes], preferred_element_type=f32
                )
            give_u[h] = total_in[:, half_at(1 - par, h)].astype(bf)
        launch(remote(give_u.at[h], got_u.at[h], g_s.at[3 * h], g_r.at[3 * h], sp=pair))

    def half_at(e, h):
        return pl.ds(pl.multiple_of(e * wide + h * narrow, 128), narrow)

    def turn_inputs(h):
        with jax.named_scope("got_u"):
            remote(got_u.at[h], got_u.at[h], g_s.at[3 * h], g_r.at[3 * h], sp=pair).wait_recv()
        with jax.named_scope("turn_u"):
            u = total_in[:, half_at(par, h)] + got_u[h].astype(f32)
            u_scr[h * narrow : (h + 1) * narrow, :] = jnp.transpose(u.astype(bf).astype(f32))

    state_inputs(0)
    pump(1)
    state_inputs(1)
    pump(1)
    launch_if(slow, out_weights)
    pump(2)
    turn_inputs(0)
    launch_if(fast, out_weights)
    launch_if(slow, attend_weights)

    def query_parts(h):
        with jax.named_scope("query_wait"):
            spread_done(1, (2 * h, 2 * h + 1))
        with jax.named_scope("project_q"):
            for e in range(2):
                lanes = slice(e * wide + h * narrow, e * wide + (h + 1) * narrow)
                total_q[:, lanes] = sum(
                    jnp.dot(normed[slot], w_query[slot, :, lanes], preferred_element_type=f32)
                    for slot in range(2)
                )
            give_q[h] = total_q[:, half_at(1 - par, h)].astype(bf)
        launch(remote(give_q.at[h], got_q.at[h], g_s.at[1 + 3 * h], g_r.at[1 + 3 * h], sp=pair))

    def key_parts():
        with jax.named_scope("key_wait"):
            spread_done(2)
        with jax.named_scope("project_kv"):
            keys = part_of(w_key, 0) + part_of(w_key, 1)
            values = part_of(w_value, 0) + part_of(w_value, 1)
            both = [
                jnp.concatenate([a[:, e * HEAD_DIM : (e + 1) * HEAD_DIM] for a in (keys, values)], axis=1)
                for e in range(2)
            ]
            give_kv[...] = jnp.where(par == 0, both[1], both[0]).astype(bf)
        launch(remote(give_kv, got_kv, g_s.at[2], g_r.at[2], sp=pair))

        return jnp.where(par == 0, both[0], both[1])

    tail = kv_scr.at[pl.ds(2 * WINDOW, WINDOW)]
    head = kv_scr.at[pl.ds(0, WINDOW)]
    hand_kv = remote(tail, head, p_s.at[5], p_r.at[5], sp=across_z)
    hand_state = remote(carry_out, carry_in, p_s.at[6], p_r.at[6], sp=across_z)

    def settle_kv():
        with jax.named_scope("kv_wait"):
            remote(got_kv, got_kv, g_s.at[2], g_r.at[2], sp=pair).wait_recv()
        kv_scr[WINDOW:, :] = (own_kv + got_kv[...].astype(f32)).astype(bf)

        @pl.when(late == 0)
        def _():
            hand_kv.start()
            kv_scr[:WINDOW, :] = jnp.zeros((WINDOW, kv_scr.shape[1]), bf)

    lane = lax.broadcasted_iota(jnp.int32, (state, BLOCK), 1)
    ends = [jnp.zeros((state, BLOCK), f32)] * 4
    for g in range(groups):
        if g == groups // 2:
            turn_inputs(1)
            launch_if(fast, attend_weights)
        with jax.named_scope("first"):
            u = u_scr[g * GROUP_CH : (g + 1) * GROUP_CH, :]
            drive = jnp.dot(inm[g], u.astype(bf), preferred_element_type=f32)
            up_re = jnp.concatenate([tab[g, 0]] * 2, axis=1)
            up_im = jnp.concatenate([tab[g, 1]] * 2, axis=1)
            row = lifts[g : g + 1, :]
            d_re, d_im = drive[:state] * row, drive[state:] * row
            lifted = jnp.concatenate([d_re * up_re - d_im * up_im, d_re * up_im + d_im * up_re], axis=0)
            sums = jnp.dot(lifted.astype(bf), tri_both, preferred_element_type=f32)
            prefix[g] = sums
            ends = [
                jnp.where(
                    lane == g,
                    sums[i % 2 * state : (i % 2 + 1) * state, (i // 2 + 1) * BLOCK - 1 : (i // 2 + 1) * BLOCK],
                    ends[i],
                )
                for i in range(4)
            ]
        if g == 5:
            own_kv = key_parts()
        if g in (1, 3):
            pump(1)
        if g == 11:
            query_parts(0)
            pump(1)
            if False:
                pump(1)
    with jax.named_scope("carry"):
        own = [scaled(lasts[b], times(end, (ends[2 * b], ends[2 * b + 1]))) for b in range(2)]
        decay = [scaled(lasts[b] * begins[b], whole) for b in range(2)]
        final = plus(own[1], times(decay[1], own[0]))
        carry_out[...] = jnp.transpose(jnp.concatenate(final, axis=0))[:groups]

    @pl.when(late == 0)
    def _():
        hand_state.start()
        carry_in[...] = jnp.zeros(carry_in.shape, f32)

    query_parts(1)
    settle_kv()
    pump(1)

    @pl.when(late == 1)
    def _():
        with jax.named_scope("hand_state"):
            hand_state.wait_recv()

    back = jnp.transpose(carry_in[...])
    entry = (back[:state], back[state:])

    def bases(row, c):
        return scaled(row, times(c, reach))

    def grown_entry(c):
        return plus((own[0][0][:, :groups], own[0][1][:, :groups]),
                    times((decay[0][0][:, :groups], decay[0][1][:, :groups]), c))

    cut = (reach[0][:, :groups], reach[1][:, :groups])
    base = [
        scaled(begins[0][:, :groups], times(entry, cut)),
        scaled(begins[1][:, :groups], times(grown_entry(entry), cut)),
    ]
    for g in range(groups):
        with jax.named_scope("second"):
            u = u_scr[g * GROUP_CH : (g + 1) * GROUP_CH, :]
            down = [jnp.concatenate([tab[g, i]] * 2, axis=1) for i in (2, 3)]
            chosen = lax.broadcasted_iota(jnp.int32, skip.shape, 1) == first + g
            skips = jnp.sum(jnp.where(chosen, skip[...], 0.0), axis=1, keepdims=True)
            p = [
                prefix[g, i * state : (i + 1) * state]
                + jnp.concatenate(
                    [jnp.broadcast_to(base[b][i][:, g : g + 1], (state, BLOCK)) for b in range(2)], axis=1
                )
                for i in range(2)
            ]
            states = jnp.concatenate(scaled(grows[g : g + 1, :], times(down, p)), axis=0).astype(bf)
            y = jnp.dot(read[g], states, preferred_element_type=f32)
            y_scr[g * GROUP_CH : (g + 1) * GROUP_CH, :] = y + skips * u
        if (g + 1) % (groups // 2) == 0:
            side = (g + 1) // (groups // 2) - 1
            lanes = slice(side * BLOCK, (side + 1) * BLOCK)
            with jax.named_scope("gelu"):
                act_s[par, :, lanes] = jnp.transpose(jax.nn.gelu(y_scr[lanes, :])).astype(bf)
            half_s = act_s.at[par, :, pl.ds(side * BLOCK, BLOCK)]
            launch(remote(half_s, half_s, e_s.at[6 + side], e_r.at[6 + side], sp=pair))

    gap_shape = (WINDOW, 2 * WINDOW)
    at = lax.broadcasted_iota(jnp.int32, gap_shape, 1)
    gap = lax.broadcasted_iota(jnp.int32, gap_shape, 0) + WINDOW - at
    inside = (gap >= 0) & (gap < WINDOW)
    inside_first = inside & (at >= WINDOW * (1 - late))
    sink_lane = lax.broadcasted_iota(jnp.int32, sinks.shape, 1)
    pump(2)
    for side in range(2):
        pump(1)
        with jax.named_scope("q_wait"):
            remote(got_q.at[side], got_q.at[side], g_s.at[1 + 3 * side], g_r.at[1 + 3 * side], sp=pair).wait_recv()
        q_scr[:, side * narrow : (side + 1) * narrow] = (
            (total_q[:, half_at(par, side)] + got_q[side].astype(f32)) * HEAD_DIM ** (-0.5)
        ).astype(bf)
        for b in (1, 0):
            if b == 0 and side == 0:

                @pl.when(late == 1)
                def _():
                    with jax.named_scope("hand_kv"):
                        hand_kv.wait_recv()

            keys = kv_scr[b * WINDOW : (b + 2) * WINDOW, :HEAD_DIM]
            values = kv_scr[b * WINDOW : (b + 2) * WINDOW, HEAD_DIM:]
            valid = inside if b else inside_first
            outs = []
            for h in range(side * heads // 2, (side + 1) * heads // 2):
                with jax.named_scope("head"):
                    q = q_scr[b * WINDOW : (b + 1) * WINDOW, h * HEAD_DIM : (h + 1) * HEAD_DIM]
                    scores = lax.dot_general(q, keys, (((1,), (1,)), ((), ())), preferred_element_type=f32)
                    scores = jnp.where(valid, scores, floor_score)
                    sink = jnp.sum(
                        jnp.where(sink_lane == par * heads + h, sinks[...], 0.0), axis=1, keepdims=True
                    )
                    peak = jnp.maximum(jnp.max(scores, axis=1, keepdims=True), sink)
                    raised = jnp.exp(scores - peak)
                    total = jnp.sum(raised, axis=1, keepdims=True) + jnp.exp(sink - peak)
                    weights = (raised * (1.0 / total)).astype(bf)
                    outs.append(jnp.dot(weights, values, preferred_element_type=f32))
            act_a[par, b * BLOCK : (b + 1) * BLOCK, side * narrow : (side + 1) * narrow] = jnp.concatenate(
                outs, axis=1
            ).astype(bf)
        half_a = act_a.at[par, :, pl.ds(side * narrow, narrow)]
        launch(remote(half_a, half_a, e_s.at[4 + side], e_r.at[4 + side], sp=pair))

    size, chunk = tokens // 2, cols // 2
    def state_part(slot):
        for side in range(2):
            lanes = slice(side * chunk, (side + 1) * chunk)
            both = [jnp.dot(act_s[e], wo_s[slot, e * wide : (e + 1) * wide, lanes], preferred_element_type=f32)
                    for e in range(2)]
            pa[slot, :, lanes] = both[0] + both[1]

    with jax.named_scope("mix_s"):
        for side in range(2):
            theirs = act_s.at[1 - par, :, pl.ds(side * BLOCK, BLOCK)]
            remote(theirs, theirs, e_s.at[6 + side], e_r.at[6 + side], sp=pair).wait_recv()
    with jax.named_scope("state"):
        state_part(late)
    pump(len(queue))
    with jax.named_scope("out_wait"):
        spread_done(3)
    with jax.named_scope("state"):
        state_part(1 - late)
    with jax.named_scope("mix_a"):
        for side in range(2):
            theirs = act_a.at[1 - par, :, pl.ds(side * narrow, narrow)]
            remote(theirs, theirs, e_s.at[4 + side], e_r.at[4 + side], sp=pair).wait_recv()

    def target(who, i):
        first_column = lax.rem(who + 2 * (i // 2), n) * cols + (i % 2) * chunk
        return out.at[:, pl.ds(pl.multiple_of(first_column, 128), chunk)]

    def multiply(i):
        slot, lanes = late if i < 2 else 1 - late, slice(i % 2 * chunk, (i % 2 + 1) * chunk)
        total = pa[slot, :, lanes]
        for e in range(2):
            total = total + jnp.dot(
                act_a[e], wo_a[slot, e * wide : (e + 1) * wide, lanes], preferred_element_type=f32
            )
        for e in range(2):
            for side in range(2):
                block = total[e * tokens + side * size : e * tokens + (side + 1) * size]
                pf[i, e, side] = block
                pb[i, side, e] = block.astype(bf)
        launch(remote(pb.at[i, other], got.at[i], d_s.at[i], d_r.at[i], tp=other))

    def pass_on(i):
        remote(got.at[i], got.at[i], d_s.at[i], d_r.at[i], tp=other).wait_recv()
        fsend[i] = (pf[i, 1 - par, t] + got[i, 1 - par].astype(f32)).astype(bf)
        launch(remote(fsend.at[i], target(k, i), e_s.at[i], e_r.at[i], sp=pair))
        res[i] = (pf[i, par, t] + got[i, par].astype(f32)).astype(bf)
        launch(pltpu.make_async_copy(res.at[i], target(k, i), o_s.at[i]))

    for i in range(4):
        if i == 2:
            with jax.named_scope("out_wait"):
                spread_done(4)
        with jax.named_scope("multiply"):
            multiply(i)
        if i:
            with jax.named_scope("pass"):
                pass_on(i - 1)
    with jax.named_scope("pass"):
        pass_on(3)
    with jax.named_scope("settle"):
        for i in range(4):
            theirs = target(pair, i)
            remote(theirs, theirs, e_s.at[i], e_r.at[i], sp=pair).wait_recv()

    with jax.named_scope("drain"):
        for c in sent:
            if c.is_remote:
                c.wait_send()
            else:
                c.wait()

    @pl.when(late == 0)
    def _():
        hand_kv.wait_send()
        hand_state.wait_send()


def layer(x, gain, ssm, query, key, value, rate, turn, parts, reads, skip, shift, sinks, ows, owa):
    bf, f32 = jnp.bfloat16, jnp.float32
    tokens, half = x.shape
    rows, cols = ows.shape[0], ows.shape[1]
    wide = ssm.shape[1] // 2
    groups, state = rate.shape[0] // 2, rate.shape[1]
    length = 2 * tokens
    dma = pltpu.SemaphoreType.DMA
    vm = pltpu.VMEM
    return pl.pallas_call(
        layer_kernel,
        out_shape=jax.ShapeDtypeStruct((tokens // 2, 4 * cols), bf),
        in_specs=[ANY] * 15,
        out_specs=ANY,
        scratch_shapes=[
            vm((tokens, 2 * half), bf), vm((2, tokens, rows), bf), vm((2, length, rows), bf),
            vm((2, rows, 2 * wide), bf), vm((2, rows, 2 * wide), bf), vm((2,) + key.shape, bf),
            vm((2,) + value.shape, bf), vm((2, rows, cols), bf), vm((2, rows, cols), bf),
            vm(gain.shape, f32), vm(rate.shape, f32), vm(turn.shape, f32),
            vm(parts.shape, bf), vm(reads.shape, bf), vm(skip.shape, f32),
            vm((groups, length), f32), vm(sinks.shape, f32),
            vm((groups, 4, state, BLOCK), f32), vm((groups, 2 * state, GROUP_CH), bf),
            vm((groups, GROUP_CH, 2 * state), bf), vm((groups, length), f32), vm((groups, length), f32),
            vm((groups, 2 * state, length), f32), vm((wide, length), f32), vm((length, wide), bf),
            vm((length + WINDOW, 2 * HEAD_DIM), bf), vm((wide, length), f32),
            vm((2, length, wide), bf), vm((2, length, wide), bf),
            vm((groups, 2 * state), f32), vm((groups, 2 * state), f32),
            vm((8, tokens), f32), vm((8, tokens), f32), vm((length, 2 * wide), f32), vm((length, 2 * wide), f32),
            vm((2, length, wide // 2), bf), vm((2, length, wide // 2), bf), vm((length, 2 * HEAD_DIM), bf),
            vm((2, length, wide // 2), bf), vm((2, length, wide // 2), bf), vm((length, 2 * HEAD_DIM), bf),
            vm((2, length, cols), f32),
            vm((4, 2, 2, tokens // 2, cols // 2), f32), vm((4, 2, 2, tokens // 2, cols // 2), bf),
            vm((4, 2, tokens // 2, cols // 2), bf), vm((4, tokens // 2, cols // 2), bf),
            vm((4, tokens // 2, cols // 2), bf),
            dma((15,)), dma((5, 4)), dma((5, 4)), dma((7,)), dma((7,)), dma((5, 4, 3)), dma((5, 4, 3)),
            dma((5,)), dma((5,)), dma((4,)), dma((4,)), dma((8,)), dma((8,)), dma((4,)),
        ],
        compiler_params=pltpu.CompilerParams(collective_id=0, has_side_effects=True),
    )(x, gain, ssm, query, key, value, rate, turn, parts, reads, skip, shift, sinks, ows, owa)


def fast_body(
    inputs, norm_gain, in_ssm, in_query, in_key, in_value, decay_rate, rotation, input_parts,
    output_parts, skip_scale, decay_shift, sink_logit, out_state, out_attend,
):
    return layer(
        inputs, norm_gain[None], in_ssm, in_query, in_key, in_value, decay_rate, rotation,
        jnp.swapaxes(input_parts, 2, 3), output_parts, skip_scale.T, jnp.transpose(decay_shift),
        sink_logit[None], out_state, out_attend,
    )


def body(*args):
    n, n_fs, n_tp = lax.axis_size("sp"), lax.axis_size("fs"), lax.axis_size("tp")
    inputs, in_ssm, in_query, in_key, decay_rate = args[0], args[2], args[3], args[4], args[6]
    key_heads = in_key.shape[1] // HEAD_DIM
    query_heads = in_query.shape[1] // HEAD_DIM
    fits = (
        n_tp == 2
        and n == 4
        and n_fs == 4
        and key_heads == 2
        and query_heads % 4 == 0
        and query_heads * HEAD_DIM == in_ssm.shape[1]
        and in_ssm.shape[1] % 256 == 0
        and in_ssm.shape[1] == args[13].shape[0] == args[14].shape[0]
        and decay_rate.shape[0] % 32 == 0
        and decay_rate.shape[0] <= 2 * BLOCK
        and decay_rate.shape[1] * 2 == BLOCK
        and decay_rate.shape[0] * GROUP_CH == in_ssm.shape[1]
        and inputs.shape[0] == BLOCK == WINDOW
        and inputs.shape[1] % 128 == 0
        and in_ssm.shape[0] % 128 == 0
        and in_ssm.shape[0] == args[13].shape[0]
        and inputs.shape[1] == 2 * in_ssm.shape[0]
        and args[13].shape[1] % 128 == 0
    )
    return (fast_body if fits else general_body)(*args)


def solution(mesh):
    return jax.shard_map(
        body,
        mesh=mesh,
        in_specs=(
            P(("fs", "sp"), "tp"),
            P(),
            P("sp", "tp"),
            P("sp", "tp"),
            P("sp", "tp"),
            P("sp", "tp"),
            P("tp", None),
            P("tp", None),
            P(None, "tp", None, None),
            P(None, "tp", None, None),
            P("tp", None),
            P(("fs", "sp"), "tp"),
            P("tp"),
            P("tp", "sp"),
            P("tp", "sp"),
        ),
        out_specs=P(("fs", "sp", "tp"), None),
        check_vma=False,
    )
```

```python
import functools
import jax
import jax.numpy as jnp
from jax import lax
from jax.experimental import pallas as pl
from jax.experimental.pallas import tpu as pltpu
from jax.sharding import PartitionSpec as P

GROUP_CH = 16
HEAD_DIM = 64
WINDOW = 128
BLOCK = 128


epsilon = 1e-06
floor_score = -1e30


def prefix(x, axis, join, neutral):
    place = lax.axis_index(axis)
    gathered = jax.tree.map(
        lambda a, kind: lax.all_gather(a.astype(kind), axis),
        x,
        (jnp.bfloat16, jnp.bfloat16, jnp.bfloat16, jnp.bfloat16),
    )
    state = jax.tree.map(lambda a, e: jnp.zeros_like(a) + jnp.asarray(e, a.dtype), x, neutral)

    def one(hop, state):
        return join(
            state,
            jax.tree.map(
                lambda a, own: lax.dynamic_index_in_dim(a, hop, 0, False).astype(own.dtype),
                gathered,
                x,
            ),
        )

    return lax.fori_loop(0, place, one, state)


def from_behind(value, axis, steps):
    count = lax.axis_size(axis)
    initial, last = (max(0, -steps), min(count, count - steps))
    return lax.ppermute(value, axis, [(source, source + steps) for source in range(initial, last)])


def combine(earlier, later):
    first_re, first_im, state_re, state_im = earlier
    second_re, second_im, input_re, input_im = later
    return (
        second_re * first_re - second_im * first_im,
        second_re * first_im + second_im * first_re,
        second_re * state_re - second_im * state_im + input_re,
        second_re * state_im + second_im * state_re + input_im,
    )


def input_matrix(decay_rate, rotation, input_parts):
    damped = jnp.exp(-decay_rate)
    lift_re = damped * jnp.cos(rotation) - 1.0
    lift_im = damped * jnp.sin(rotation)
    modulus = decay_rate * decay_rate + rotation * rotation
    factor_re = (rotation * lift_im - decay_rate * lift_re) / modulus
    factor_im = -(rotation * lift_re + decay_rate * lift_im) / modulus
    part_re = input_parts[0].astype(jnp.float32)
    part_im = input_parts[1].astype(jnp.float32)
    joined_re = factor_re[:, :, None] * part_re - factor_im[:, :, None] * part_im
    joined_im = factor_re[:, :, None] * part_im + factor_im[:, :, None] * part_re
    return jnp.concatenate([joined_re, joined_im], axis=1).astype(jnp.bfloat16)


def window_attention(queries, keys_win, values_win, starts, sink_logit):
    window = queries.shape[1]
    scores = jnp.einsum("nqgrd,nkgd->ngrqk", queries, keys_win, preferred_element_type=jnp.float32)
    scores = scores * queries.shape[-1] ** (-0.5)
    places = (
        jnp.arange(window, dtype=jnp.int32)[:, None]
        + window
        - jnp.arange(2 * window, dtype=jnp.int32)[None, :]
    )
    inside = (places >= 0) & (places < window)
    reach = starts[:, None] - window + jnp.arange(2 * window, dtype=jnp.int32)[None, :] >= 0
    valid = (inside[None] & reach[:, None, :])[:, None, None]
    sinks = sink_logit.reshape(scores.shape[1], scores.shape[2])[None, :, :, None, None]
    scores = jnp.where(valid, scores, floor_score)
    row_peak = jnp.maximum(jnp.max(scores, axis=-1, keepdims=True), sinks)
    raised = jnp.where(valid, jnp.exp(scores - row_peak), 0.0)
    denominator = jnp.sum(raised, axis=-1, keepdims=True) + jnp.exp(sinks - row_peak)
    weights = (raised / denominator).astype(jnp.bfloat16)
    result = jnp.einsum(
        "ngrqk,nkgd->nqgrd", weights, values_win, preferred_element_type=jnp.float32
    )
    return result.astype(jnp.bfloat16)


def general_body(
    inputs,
    norm_gain,
    in_ssm,
    in_query,
    in_key,
    in_value,
    decay_rate,
    rotation,
    input_parts,
    output_parts,
    skip_scale,
    decay_shift,
    sink_logit,
    out_state,
    out_attend,
):
    gathered = lax.all_gather(inputs, "tp", axis=1, tiled=True)
    length = gathered.shape[0]
    widened = gathered.astype(jnp.float32)
    scale = lax.rsqrt(jnp.mean(widened * widened, axis=1, keepdims=True) + epsilon)
    normed = (widened * scale * norm_gain).astype(jnp.bfloat16)

    def add_rows(pieces):
        return tuple(
            (jnp.dot(normed, piece, preferred_element_type=jnp.float32) for piece in pieces)
        )

    projected = add_rows(
        (
            lax.all_gather(in_ssm, "sp", axis=0, tiled=True),
            lax.all_gather(in_query, "sp", axis=0, tiled=True),
            lax.all_gather(in_key, "sp", axis=0, tiled=True),
            lax.all_gather(in_value, "sp", axis=0, tiled=True),
        )
    )
    drive_in, queries, keys_local, values = [piece.astype(jnp.bfloat16) for piece in projected]
    groups = decay_rate.shape[0]
    state_dim = decay_rate.shape[1]
    channels = groups * GROUP_CH
    highest = lax.Precision.HIGHEST
    drive_cols = jnp.transpose(drive_in).reshape(groups, GROUP_CH, length)
    in_matrix = input_matrix(decay_rate, rotation, input_parts)
    drive = jnp.einsum("gqh,ght->gqt", in_matrix, drive_cols, preferred_element_type=jnp.float32)
    shift_cols = jnp.transpose(decay_shift)
    running = jnp.cumsum(shift_cols, axis=1)
    total_shift = running[:, -1]
    remain = length - 1.0 - jnp.arange(length, dtype=jnp.float32)
    to_end = (total_shift[:, None] - running)[:, None, :] - decay_rate[:, :, None] * remain[
        None, None, :
    ]
    fade = jnp.exp(to_end)
    turn = rotation[:, :, None] * remain[None, None, :]
    weight_re = fade * jnp.cos(turn)
    weight_im = fade * jnp.sin(turn)
    drive_re = drive[:, :state_dim]
    drive_im = drive[:, state_dim:]
    final_re = jnp.sum(weight_re * drive_re - weight_im * drive_im, axis=2)
    final_im = jnp.sum(weight_re * drive_im + weight_im * drive_re, axis=2)
    overall = jnp.exp(total_shift[:, None] - decay_rate * length)
    nothing = jnp.zeros_like(final_re)
    carried = prefix(
        (
            overall * jnp.cos(rotation * length),
            overall * jnp.sin(rotation * length),
            final_re,
            final_im,
        ),
        "sp",
        combine,
        (jnp.ones_like(final_re), nothing, nothing, nothing),
    )
    key_heads = keys_local.shape[1] // HEAD_DIM
    query_heads = queries.shape[1] // HEAD_DIM
    windows_dev = length // WINDOW
    previous = from_behind((keys_local, values), "sp", 1)

    def windows(flat, before):
        split = jnp.concatenate([before, flat], axis=0).reshape(
            windows_dev + 1, WINDOW, key_heads, HEAD_DIM
        )
        return jnp.concatenate([split[:-1], split[1:]], axis=1)

    offset = lax.axis_index("sp") * length
    starts = offset + jnp.arange(windows_dev, dtype=jnp.int32) * WINDOW
    queries_blk = queries.reshape(
        windows_dev, WINDOW, key_heads, query_heads // key_heads, HEAD_DIM
    )
    attended = window_attention(
        queries_blk,
        windows(keys_local, previous[0]),
        windows(values, previous[1]),
        starts,
        sink_logit,
    )
    attend_out = attended.reshape(length, query_heads * HEAD_DIM)
    blocks = length // BLOCK
    triangle = (
        jnp.arange(BLOCK, dtype=jnp.int32)[:, None] <= jnp.arange(BLOCK, dtype=jnp.int32)[None, :]
    ).astype(jnp.float32)
    offsets = jnp.arange(BLOCK, dtype=jnp.float32)
    centre = BLOCK // 2
    read_re = output_parts[0].astype(jnp.float32)
    read_im = output_parts[1].astype(jnp.float32)
    angle = rotation[:, :, None] * (offsets - centre)[None, None, :]
    cos_angle = jnp.cos(angle)
    sin_angle = jnp.sin(angle)
    phase = rotation[:, :, None] * (offsets + 1.0)[None, None, :]
    cos_phase = jnp.cos(phase)
    sin_phase = jnp.sin(phase)

    def advance(carry, pieces):
        carry_re, carry_im = carry
        part_re, part_im, shift_part, grouped_part = pieces
        level = jnp.dot(shift_part, triangle, precision=highest)
        log_from = level[:, None, :] - decay_rate[:, :, None] * (offsets + 1.0)[None, None, :]
        relative = log_from - log_from[:, :, centre : centre + 1]
        shrink = jnp.exp(-relative)
        lift_re = shrink * (part_re * cos_angle + part_im * sin_angle)
        lift_im = shrink * (part_im * cos_angle - part_re * sin_angle)
        prefix_re = jnp.dot(lift_re.reshape(groups * state_dim, BLOCK), triangle, precision=highest)
        prefix_im = jnp.dot(lift_im.reshape(groups * state_dim, BLOCK), triangle, precision=highest)
        prefix_re = prefix_re.reshape(groups, state_dim, BLOCK)
        prefix_im = prefix_im.reshape(groups, state_dim, BLOCK)
        grow = jnp.exp(relative)
        from_start = jnp.exp(log_from)
        keep_re = from_start * cos_phase
        keep_im = from_start * sin_phase
        state_re = grow * (prefix_re * cos_angle - prefix_im * sin_angle)
        state_im = grow * (prefix_im * cos_angle + prefix_re * sin_angle)
        state_re = state_re + keep_re * carry_re[:, :, None] - keep_im * carry_im[:, :, None]
        state_im = state_im + keep_re * carry_im[:, :, None] + keep_im * carry_re[:, :, None]
        result = jnp.einsum("ghp,gpt->ght", read_re, state_re, precision=highest)
        result = result - jnp.einsum("ghp,gpt->ght", read_im, state_im, precision=highest)
        result = result + skip_scale[:, :, None] * grouped_part.astype(jnp.float32)
        return ((state_re[:, :, -1], state_im[:, :, -1]), jax.nn.gelu(result).astype(jnp.bfloat16))

    drive_blocks = jnp.transpose(drive.reshape(groups, 2 * state_dim, blocks, BLOCK), (2, 0, 1, 3))
    shift_blocks = jnp.transpose(shift_cols.reshape(groups, blocks, BLOCK), (1, 0, 2))
    grouped_blocks = jnp.transpose(
        drive_cols.reshape(groups, GROUP_CH, blocks, BLOCK), (2, 0, 1, 3)
    )
    _, state_blocks = lax.scan(
        advance,
        (carried[2], carried[3]),
        (
            drive_blocks[:, :, :state_dim],
            drive_blocks[:, :, state_dim:],
            shift_blocks,
            grouped_blocks,
        ),
    )
    state_out = jnp.transpose(state_blocks, (0, 3, 1, 2)).reshape(length, channels)
    column_state, column_attend = (
        lax.all_gather(out_state, "sp", axis=1, tiled=True),
        lax.all_gather(out_attend, "sp", axis=1, tiled=True),
    )
    result = jnp.dot(state_out, column_state, preferred_element_type=jnp.float32)
    return lax.psum_scatter(
        (result + jnp.dot(attend_out, column_attend, preferred_element_type=jnp.float32)).astype(
            jnp.bfloat16
        ),
        "tp",
        scatter_dimension=0,
        tiled=True,
    )


MESH = pl.DeviceIdType.MESH
ANY = pl.BlockSpec(memory_space=pl.ANY)


def remote(src, dst, send, recv, **where):
    return pltpu.make_async_remote_copy(
        src_ref=src, dst_ref=dst, send_sem=send, recv_sem=recv, device_id=where, device_id_type=MESH
    )


def greet(peers):
    barrier = pltpu.get_barrier_semaphore()
    for peer in peers:
        pl.semaphore_signal(barrier, inc=1, device_id=peer, device_id_type=MESH)
    pl.semaphore_wait(barrier, len(peers))


def halves(x):
    high = x.astype(jnp.bfloat16)
    return high, (x - high.astype(jnp.float32)).astype(jnp.bfloat16)


def split_dot(x, exact):
    high, low = halves(x)
    return jnp.dot(high, exact, preferred_element_type=jnp.float32) + jnp.dot(
        low, exact, preferred_element_type=jnp.float32
    )


def column(row):
    size = row.shape[1]
    same = lax.broadcasted_iota(jnp.int32, (size, size), 0) == lax.broadcasted_iota(
        jnp.int32, (size, size), 1
    )
    return jnp.sum(jnp.where(same, row, 0.0), axis=1, keepdims=True)


def turned(angle):
    quarter = jnp.floor(angle * (2.0 / 3.141592653589793) + 0.5)
    r = ((angle - quarter * 1.5703125) - quarter * 4.837512969970703e-4) - quarter * 7.549789948768648e-8
    sq = r * r
    sin = r + r * sq * (-1.6666654611e-1 + sq * (8.3321608736e-3 + sq * -1.9515295891e-4))
    cos = 1.0 - 0.5 * sq + sq * sq * (4.166664568298827e-2 + sq * (-1.388731625493765e-3 + sq * 2.443315711809948e-5))
    which = quarter.astype(jnp.int32)
    swap = (which & 1) == 1
    flip_cos = ((which + 1) & 2) == 2
    flip_sin = (which & 2) == 2
    a, b = jnp.where(swap, sin, cos), jnp.where(swap, cos, sin)
    return jnp.where(flip_cos, -a, a), jnp.where(flip_sin, -b, b)


def layer_kernel(x_in, gain_in, ssm, query, key_in, value_in, rate_in, turn_in, parts_in, reads_in,
                 skip_in, shift_in, sinks_in, ows, owa, out,
                 xf, xp, normed, w_ssm, w_query, w_key, w_value, wo_s, wo_a, gain, rate, turn,
                 parts, reads, skip, shift, sinks, tab, inm, read, lifts, grows, prefix, u_scr, q_scr,
                 kv_scr, y_scr, act_s, act_a, carry_out, carry_in, scale_out, scale_in, total_in, total_q,
                 give_u, give_q, give_kv, got_u, got_q, got_kv, pa, pf, pb, got, fsend, res,
                 loc, z_s, z_r, p_s, p_r, x_s, x_r, g_r, d_s, d_r, e_r, o_s):
    f32, bf = jnp.float32, jnp.bfloat16
    k, f, t = lax.axis_index("sp"), lax.axis_index("fs"), lax.axis_index("tp")
    n, n_fs = 4, 4
    tokens, half = x_in.shape
    rows, cols = ssm.shape[0], ows.shape[1]
    wide = w_ssm.shape[2] // 2
    groups, state = tab.shape[0], tab.shape[2]
    heads = wide // HEAD_DIM
    par, late = lax.rem(k, 2), lax.div(k, 2)
    pair = k + 1 - 2 * par
    other = 1 - t
    fx, fy, far = f + 1 - 2 * lax.rem(f, 2), lax.rem(f + 2, n_fs), n_fs - 1 - f
    across_z = lax.rem(k + 2, n)

    part = rows // n_fs
    into = (w_ssm, w_query, None, wo_s, wo_a)
    origin = (ssm, query, None, ows, owa)
    cuts = (4, 4, 2, 2, 4)
    at_piece = [sum(cuts[:w]) for w in range(5)]

    def stripe(c):
        return pl.ds(c % 2 * wide + c // 2 * (wide // 2), wide // 2)

    def region(w, c, q, slot):
        if w < 2:
            return into[w].at[slot, pl.ds(pl.multiple_of(q * part, 16), part), stripe(c)]
        if w == 2:
            return (w_key, w_value)[c].at[slot, pl.ds(pl.multiple_of(q * part, 16), part)]
        size = part // cuts[w]
        return into[w].at[slot, pl.ds(pl.multiple_of(q * part + c * size, 16), size)]

    def over_z(w, c):
        if w < 2:
            source = origin[w].at[pl.ds(pl.multiple_of(f * part, 16), part), stripe(c)]
        elif w == 2:
            source = (key_in, value_in)[c].at[pl.ds(pl.multiple_of(f * part, 16), part)]
        else:
            size = part // cuts[w]
            source = origin[w].at[pl.ds(pl.multiple_of(f * part + c * size, 16), size)]
        return remote(source, region(w, c, f, late), z_s.at[at_piece[w] + c], z_r.at[at_piece[w] + c], sp=across_z)

    def spread_here(w, c):
        block = region(w, c, f, 1 - late)
        remote(block, block, z_s.at[at_piece[w] + c], z_r.at[at_piece[w] + c], sp=across_z).wait_recv()
        slot = len(spreads) % 4
        if len(spreads) >= 4:
            for copy in spreads[-4]:
                copy.wait_send()
        spreads.append([
            remote(block, block, x_s.at[slot, i], x_r.at[at_piece[w] + c, i], fs=who)
            for i, who in enumerate((far, fx, fy))
        ])
        for copy in spreads[-1]:
            copy.start()

    def spread_done(w, pieces=None):
        for c in pieces or range(cuts[w]):
            for i, who in enumerate((far, fx, fy)):
                block = region(w, c, who, 1 - late)
                remote(block, block, x_s.at[0, i], x_r.at[at_piece[w] + c, i], fs=who).wait_recv()

    sent, spreads = [], []
    g_s, e_s = [loc.at[i] for i in range(5)], [loc.at[5 + i] for i in range(8)]

    def launch(c):
        c.start()
        sent.append(c)

    def shift_at(e):
        return shift.at[:, pl.ds(pl.multiple_of(e * tokens, 128), tokens)]

    def shift_rows(e):
        return shift_in.at[pl.ds(pl.multiple_of(e * groups, 8), groups)]

    queue = [(f"s{w}{c}", functools.partial(spread_here, w, c)) for w in (0, 2, 1, 3, 4) for c in range(cuts[w])]

    def pump(count):
        for _ in range(min(count, len(queue))):
            name, step = queue.pop(0)
            with jax.named_scope(name):
                step()

    local = [
        (rate_in, rate), (turn_in, turn), (parts_in, parts), (reads_in, reads), (skip_in, skip),
        (gain_in, gain), (sinks_in, sinks), (shift_rows(par), shift_at(par)),
        (x_in, xf.at[:, pl.ds(pl.multiple_of(t * half, 128), half)]),
        (ssm, w_ssm.at[late]), (query, w_query.at[late]), (key_in, w_key.at[late]),
        (value_in, w_value.at[late]), (ows, wo_s.at[late]), (owa, wo_a.at[late]),
    ]
    local = [pltpu.make_async_copy(a, b, loc.at[i]) for i, (a, b) in enumerate(local)]
    for c in local:
        c.start()
    first = par * groups

    def tables(g, columns_of):
        line, spin = rate[pl.ds(first + g, 1), :], turn[pl.ds(first + g, 1), :]
        rates, turns = column(line), column(spin)
        away = lax.broadcasted_iota(jnp.int32, (state, BLOCK), 1).astype(f32) - float(BLOCK // 2)
        angle = turns * away
        cos, sin = turned(angle)
        fade = jnp.exp(-rates * away)
        rise = jnp.exp(rates * away)
        tab[g, 0] = rise * cos
        tab[g, 1] = -(rise * sin)
        tab[g, 2] = fade * cos
        tab[g, 3] = fade * sin
        damped = jnp.exp(-line)
        lift_re = damped * jnp.cos(spin) - 1.0
        lift_im = damped * jnp.sin(spin)
        modulus = line * line + spin * spin
        factor_re = (spin * lift_im - line * lift_re) / modulus
        factor_im = -(spin * lift_re + line * lift_im) / modulus
        part_re = parts[0, first + g].astype(f32)
        part_im = parts[1, first + g].astype(f32)
        inm[g] = jnp.transpose(
            jnp.concatenate(
                [factor_re * part_re - factor_im * part_im, factor_re * part_im + factor_im * part_re],
                axis=1,
            )
        ).astype(bf)
        read[g] = jnp.concatenate(
            [reads[0, first + g].astype(f32), -reads[1, first + g].astype(f32)], axis=1
        ).astype(bf)
        spot = lax.broadcasted_iota(jnp.int32, (state, BLOCK), 1) == g
        return jnp.where(spot, rates, columns_of[0]), jnp.where(spot, turns, columns_of[1])

    columns_of = (jnp.zeros((state, BLOCK), f32), jnp.zeros((state, BLOCK), f32))
    early = (n - 1 - k) * (n - 1 - k)
    peers = [{"sp": pair}, {"sp": across_z}, {"fs": fx}, {"fs": fy}, {"fs": far}, {"tp": other}]
    barrier = pltpu.get_barrier_semaphore()
    for peer in peers:
        pl.semaphore_signal(barrier, inc=1, device_id=peer, device_id_type=MESH)

    def settle_params():
        for c in local[:8]:
            c.wait()

    pl.when(k < n - 1)(settle_params)
    with jax.named_scope("tables"):
        columns_of = lax.fori_loop(0, early, tables, columns_of)
    with jax.named_scope("greet"):
        pl.semaphore_wait(barrier, len(peers))
    at_end = k * (n - 1 - k) == 0
    sides = pl.ds(pl.multiple_of(t * half, 128), half)
    launch(remote(x_in, xf.at[:, sides], p_s.at[0], p_r.at[0], tp=other))
    slow, fast, at_mid = t == 0, t == 1, k * (n - 1 - k) > 0

    def launch_if(choice, copies):
        @pl.when(choice)
        def _():
            for c in copies:
                c.start()

    state_weights = [over_z(0, c) for c in range(cuts[0])]
    early_keys = [over_z(2, c) for c in range(2)]
    query_weights = [over_z(1, c) for c in range(cuts[1])]
    out_weights = [over_z(3, c) for c in range(2)]
    attend_weights = [over_z(4, c) for c in range(cuts[4])]
    give_x = remote(x_in.at[:, pl.ds(pl.multiple_of((1 - par) * rows, 128), rows)], xp.at[t],
                    p_s.at[1], p_r.at[1], sp=pair)
    launch(remote(shift_rows(1 - par), shift_at(par), p_s.at[2], p_r.at[2], sp=pair))
    state_weights[0].start()
    launch_if(slow, state_weights[1:])
    launch_if(slow | jnp.logical_not(at_end), [give_x])
    launch_if(slow, early_keys)
    sent.extend(state_weights + early_keys + query_weights + out_weights + attend_weights + [give_x])
    pl.when(k == n - 1)(settle_params)
    with jax.named_scope("tables"):
        columns_of = lax.fori_loop(early, 10, tables, columns_of)

    local[8].wait()
    theirs = xf.at[:, pl.ds(pl.multiple_of(other * half, 128), half)]
    with jax.named_scope("own_x"):
        remote(theirs, theirs, p_s.at[0], p_r.at[0], tp=other).wait_recv()

    def gain_of(slot):
        return gain[:, pl.ds(pl.multiple_of((2 * slot + par) * rows, 128), rows)]

    own_rows = pl.ds(pl.multiple_of(par * tokens, 128), tokens)
    pair_rows = pl.ds(pl.multiple_of((1 - par) * tokens, 128), tokens)
    with jax.named_scope("norm"):
        full = xf[...].astype(f32)
        scale = lax.rsqrt(jnp.mean(full * full, axis=1, keepdims=True) + epsilon)
        same = lax.broadcasted_iota(jnp.int32, (tokens, tokens), 0) == lax.broadcasted_iota(
            jnp.int32, (tokens, tokens), 1
        )
        line = jnp.sum(jnp.where(same, scale, 0.0), axis=0, keepdims=True)
        scale_out[...] = jnp.broadcast_to(line, scale_out.shape)
    launch_if(fast, state_weights[1:] + early_keys)
    launch_if(fast & at_end, [give_x])
    launch(remote(scale_out, scale_in, p_s.at[3], p_r.at[3], sp=pair))
    with jax.named_scope("norm"):
        for slot in range(2):
            block = xf[:, pl.ds(pl.multiple_of((2 * slot + par) * rows, 128), rows)].astype(f32)
            normed[slot, own_rows] = (block * scale * gain_of(slot)).astype(bf)
    with jax.named_scope("tables"):
        columns_of = lax.fori_loop(10, groups, tables, columns_of)
    hand_x = remote(xp.at[t], xp.at[t], p_s.at[4], p_r.at[4], tp=other)
    sent.append(hand_x)

    def take_x():
        with jax.named_scope("next_x"):
            remote(xp.at[t], xp.at[t], p_s.at[1], p_r.at[1], sp=pair).wait_recv()
        hand_x.start()

    pump(1)
    pl.when(at_end)(take_x)
    pump(1)
    pump(2)
    for c in query_weights:
        c.start()
    near_shift = shift_at(1 - par)
    remote(near_shift, near_shift, p_s.at[2], p_r.at[2], sp=pair).wait_recv()

    shape = (BLOCK, BLOCK)
    upto = lax.broadcasted_iota(jnp.int32, shape, 0) <= lax.broadcasted_iota(jnp.int32, shape, 1)
    tri = upto.astype(f32).astype(bf)
    both_shape = (2 * BLOCK, 2 * BLOCK)
    from_at, to_at = (lax.broadcasted_iota(jnp.int32, both_shape, i) for i in range(2))
    tri_both = ((from_at <= to_at) & ((from_at < BLOCK) == (to_at < BLOCK))).astype(f32).astype(bf)
    centre = BLOCK // 2
    eye = lax.broadcasted_iota(jnp.int32, (groups, BLOCK), 0) == lax.broadcasted_iota(
        jnp.int32, (groups, BLOCK), 1
    )

    def across(col):
        return jnp.sum(jnp.where(eye, col, 0.0), axis=0, keepdims=True)

    begins, lasts = [], []
    for b in range(2):
        piece_b = shift[:, b * BLOCK : (b + 1) * BLOCK]
        high, low = halves(piece_b)
        low2 = (piece_b - high.astype(f32) - low.astype(f32)).astype(bf)
        level = (
            jnp.dot(high, tri, preferred_element_type=f32)
            + jnp.dot(low, tri, preferred_element_type=f32)
            + jnp.dot(low2, tri, preferred_element_type=f32)
        )
        middle = level[:, centre : centre + 1]
        lifts[:, b * BLOCK : (b + 1) * BLOCK] = jnp.exp(middle - level)
        grown = jnp.exp(level - middle)
        grows[:, b * BLOCK : (b + 1) * BLOCK] = grown
        begins.append(across(jnp.exp(middle)))
        lasts.append(across(grown[:, BLOCK - 1 :]))
    rates, turns = columns_of

    def times(a, b):
        return a[0] * b[0] - a[1] * b[1], a[0] * b[1] + a[1] * b[0]

    def plus(a, b):
        return a[0] + b[0], a[1] + b[1]

    def scaled(row, a):
        return row * a[0], row * a[1]

    def spiral(count):
        fade = jnp.exp(-rates * count)
        return fade * jnp.cos(turns * count), fade * jnp.sin(turns * count)

    reach, end = spiral(centre + 1.0), spiral(BLOCK - 1.0 - centre)
    whole = times(reach, end)

    pl.when(at_mid)(take_x)
    with jax.named_scope("partner_x"):
        remote(xp.at[other], xp.at[other], p_s.at[4], p_r.at[4], tp=other).wait_recv()
        remote(scale_in, scale_in, p_s.at[3], p_r.at[3], sp=pair).wait_recv()
    with jax.named_scope("norm"):
        scale = column(scale_in[0:1, :])
        for slot in range(2):
            normed[slot, pair_rows] = (xp[slot].astype(f32) * scale * gain_of(slot)).astype(bf)
    for c in local[9:]:
        c.wait()
    with jax.named_scope("own_u"):
        total_in[...] = jnp.dot(normed[late], w_ssm[late], preferred_element_type=f32)

    def part_of(w, slot):
        return jnp.dot(normed[slot], w[slot], preferred_element_type=f32)

    def mine_at(e):
        return pl.ds(pl.multiple_of(e * wide, 128), wide)


    narrow = wide // 2

    def state_inputs(h):
        with jax.named_scope("ssm_wait"):
            spread_done(0, (2 * h, 2 * h + 1))
        with jax.named_scope("project_u"):
            for e in range(2):
                lanes = slice(e * wide + h * narrow, e * wide + (h + 1) * narrow)
                total_in[:, lanes] += jnp.dot(
                    normed[1 - late], w_ssm[1 - late, :, lanes], preferred_element_type=f32
                )
            give_u[h] = total_in[:, half_at(1 - par, h)].astype(bf)
        launch(remote(give_u.at[h], got_u.at[h], g_s[3 * h], g_r.at[3 * h], sp=pair))

    def half_at(e, h):
        return pl.ds(pl.multiple_of(e * wide + h * narrow, 128), narrow)

    def turn_inputs(h):
        with jax.named_scope("got_u"):
            remote(got_u.at[h], got_u.at[h], g_s[3 * h], g_r.at[3 * h], sp=pair).wait_recv()
        with jax.named_scope("turn_u"):
            u = total_in[:, half_at(par, h)] + got_u[h].astype(f32)
            u_scr[h * narrow : (h + 1) * narrow, :] = jnp.transpose(u.astype(bf).astype(f32))

    state_inputs(0)
    pump(1)
    state_inputs(1)
    pump(1)
    launch_if(slow, out_weights)
    pump(2)
    turn_inputs(0)
    launch_if(fast, out_weights)
    launch_if(slow, attend_weights)

    def query_parts(h):
        with jax.named_scope("query_wait"):
            spread_done(1, (2 * h, 2 * h + 1))
        with jax.named_scope("project_q"):
            for e in range(2):
                lanes = slice(e * wide + h * narrow, e * wide + (h + 1) * narrow)
                total_q[:, lanes] = sum(
                    jnp.dot(normed[slot], w_query[slot, :, lanes], preferred_element_type=f32)
                    for slot in range(2)
                )
            give_q[h] = total_q[:, half_at(1 - par, h)].astype(bf)
        launch(remote(give_q.at[h], got_q.at[h], g_s[1 + 3 * h], g_r.at[1 + 3 * h], sp=pair))

    def key_parts():
        with jax.named_scope("key_wait"):
            spread_done(2)
        with jax.named_scope("project_kv"):
            keys = part_of(w_key, 0) + part_of(w_key, 1)
            values = part_of(w_value, 0) + part_of(w_value, 1)
            both = [
                jnp.concatenate([a[:, e * HEAD_DIM : (e + 1) * HEAD_DIM] for a in (keys, values)], axis=1)
                for e in range(2)
            ]
            give_kv[...] = jnp.where(par == 0, both[1], both[0]).astype(bf)
        launch(remote(give_kv, got_kv, g_s[2], g_r.at[2], sp=pair))

        return jnp.where(par == 0, both[0], both[1])

    tail = kv_scr.at[pl.ds(2 * WINDOW, WINDOW)]
    head = kv_scr.at[pl.ds(0, WINDOW)]
    hand_kv = remote(tail, head, p_s.at[5], p_r.at[5], sp=across_z)
    hand_state = remote(carry_out, carry_in, p_s.at[6], p_r.at[6], sp=across_z)

    def settle_kv():
        with jax.named_scope("kv_wait"):
            remote(got_kv, got_kv, g_s[2], g_r.at[2], sp=pair).wait_recv()
        kv_scr[WINDOW:, :] = (own_kv + got_kv[...].astype(f32)).astype(bf)

        @pl.when(late == 0)
        def _():
            hand_kv.start()
            kv_scr[:WINDOW, :] = jnp.zeros((WINDOW, kv_scr.shape[1]), bf)

    lane = lax.broadcasted_iota(jnp.int32, (state, BLOCK), 1)
    ends = [jnp.zeros((state, BLOCK), f32)] * 4
    for g in range(groups):
        if g == groups // 2:
            turn_inputs(1)
            launch_if(fast, attend_weights)
        with jax.named_scope("first"):
            u = u_scr[g * GROUP_CH : (g + 1) * GROUP_CH, :]
            drive = jnp.dot(inm[g], u.astype(bf), preferred_element_type=f32)
            up_re = jnp.concatenate([tab[g, 0]] * 2, axis=1)
            up_im = jnp.concatenate([tab[g, 1]] * 2, axis=1)
            row = lifts[g : g + 1, :]
            d_re, d_im = drive[:state] * row, drive[state:] * row
            lifted = jnp.concatenate([d_re * up_re - d_im * up_im, d_re * up_im + d_im * up_re], axis=0)
            sums = jnp.dot(lifted.astype(bf), tri_both, preferred_element_type=f32)
            prefix[g] = sums
            ends = [
                jnp.where(
                    lane == g,
                    sums[i % 2 * state : (i % 2 + 1) * state, (i // 2 + 1) * BLOCK - 1 : (i // 2 + 1) * BLOCK],
                    ends[i],
                )
                for i in range(4)
            ]
        if g == 5:
            own_kv = key_parts()
        if g in (1, 3):
            pump(1)
        if g == 11:
            query_parts(0)
            pump(1)
            if False:
                pump(1)
    with jax.named_scope("carry"):
        own = [scaled(lasts[b], times(end, (ends[2 * b], ends[2 * b + 1]))) for b in range(2)]
        decay = [scaled(lasts[b] * begins[b], whole) for b in range(2)]
        final = plus(own[1], times(decay[1], own[0]))
        carry_out[...] = jnp.transpose(jnp.concatenate(final, axis=0))[:groups]

    @pl.when(late == 0)
    def _():
        hand_state.start()
        carry_in[...] = jnp.zeros(carry_in.shape, f32)

    query_parts(1)
    settle_kv()
    pump(1)

    @pl.when(late == 1)
    def _():
        with jax.named_scope("hand_state"):
            hand_state.wait_recv()

    back = jnp.transpose(carry_in[...])
    entry = (back[:state], back[state:])

    def bases(row, c):
        return scaled(row, times(c, reach))

    def grown_entry(c):
        return plus((own[0][0][:, :groups], own[0][1][:, :groups]),
                    times((decay[0][0][:, :groups], decay[0][1][:, :groups]), c))

    cut = (reach[0][:, :groups], reach[1][:, :groups])
    base = [
        scaled(begins[0][:, :groups], times(entry, cut)),
        scaled(begins[1][:, :groups], times(grown_entry(entry), cut)),
    ]
    for g in range(groups):
        with jax.named_scope("second"):
            u = u_scr[g * GROUP_CH : (g + 1) * GROUP_CH, :]
            down = [jnp.concatenate([tab[g, i]] * 2, axis=1) for i in (2, 3)]
            chosen = lax.broadcasted_iota(jnp.int32, skip.shape, 1) == first + g
            skips = jnp.sum(jnp.where(chosen, skip[...], 0.0), axis=1, keepdims=True)
            p = [
                prefix[g, i * state : (i + 1) * state]
                + jnp.concatenate(
                    [jnp.broadcast_to(base[b][i][:, g : g + 1], (state, BLOCK)) for b in range(2)], axis=1
                )
                for i in range(2)
            ]
            states = jnp.concatenate(scaled(grows[g : g + 1, :], times(down, p)), axis=0).astype(bf)
            y = jnp.dot(read[g], states, preferred_element_type=f32)
            y_scr[g * GROUP_CH : (g + 1) * GROUP_CH, :] = y + skips * u
        if (g + 1) % (groups // 2) == 0:
            side = (g + 1) // (groups // 2) - 1
            lanes = slice(side * BLOCK, (side + 1) * BLOCK)
            with jax.named_scope("gelu"):
                act_s[par, :, lanes] = jnp.transpose(jax.nn.gelu(y_scr[lanes, :])).astype(bf)
            half_s = act_s.at[par, :, pl.ds(side * BLOCK, BLOCK)]
            launch(remote(half_s, half_s, e_s[6 + side], e_r.at[6 + side], sp=pair))

    gap_shape = (WINDOW, 2 * WINDOW)
    at = lax.broadcasted_iota(jnp.int32, gap_shape, 1)
    gap = lax.broadcasted_iota(jnp.int32, gap_shape, 0) + WINDOW - at
    inside = (gap >= 0) & (gap < WINDOW)
    inside_first = inside & (at >= WINDOW * (1 - late))
    sink_lane = lax.broadcasted_iota(jnp.int32, sinks.shape, 1)
    pump(2)
    for side in range(2):
        pump(1)
        with jax.named_scope("q_wait"):
            remote(got_q.at[side], got_q.at[side], g_s[1 + 3 * side], g_r.at[1 + 3 * side], sp=pair).wait_recv()
        q_scr[:, side * narrow : (side + 1) * narrow] = (
            (total_q[:, half_at(par, side)] + got_q[side].astype(f32)) * HEAD_DIM ** (-0.5)
        ).astype(bf)
        for b in (1, 0):
            if b == 0 and side == 0:

                @pl.when(late == 1)
                def _():
                    with jax.named_scope("hand_kv"):
                        hand_kv.wait_recv()

            keys = kv_scr[b * WINDOW : (b + 2) * WINDOW, :HEAD_DIM]
            values = kv_scr[b * WINDOW : (b + 2) * WINDOW, HEAD_DIM:]
            valid = inside if b else inside_first
            outs = []
            for h in range(side * heads // 2, (side + 1) * heads // 2):
                with jax.named_scope("head"):
                    q = q_scr[b * WINDOW : (b + 1) * WINDOW, h * HEAD_DIM : (h + 1) * HEAD_DIM]
                    scores = lax.dot_general(q, keys, (((1,), (1,)), ((), ())), preferred_element_type=f32)
                    scores = jnp.where(valid, scores, floor_score)
                    sink = jnp.sum(
                        jnp.where(sink_lane == par * heads + h, sinks[...], 0.0), axis=1, keepdims=True
                    )
                    peak = jnp.maximum(jnp.max(scores, axis=1, keepdims=True), sink)
                    raised = jnp.exp(scores - peak)
                    total = jnp.sum(raised, axis=1, keepdims=True) + jnp.exp(sink - peak)
                    weights = (raised * (1.0 / total)).astype(bf)
                    outs.append(jnp.dot(weights, values, preferred_element_type=f32))
            act_a[par, b * BLOCK : (b + 1) * BLOCK, side * narrow : (side + 1) * narrow] = jnp.concatenate(
                outs, axis=1
            ).astype(bf)
        half_a = act_a.at[par, :, pl.ds(side * narrow, narrow)]
        launch(remote(half_a, half_a, e_s[4 + side], e_r.at[4 + side], sp=pair))

    size, chunk = tokens // 2, cols // 2
    def state_part(slot):
        for side in range(2):
            lanes = slice(side * chunk, (side + 1) * chunk)
            both = [jnp.dot(act_s[e], wo_s[slot, e * wide : (e + 1) * wide, lanes], preferred_element_type=f32)
                    for e in range(2)]
            pa[slot, :, lanes] = both[0] + both[1]

    with jax.named_scope("mix_s"):
        for side in range(2):
            theirs = act_s.at[1 - par, :, pl.ds(side * BLOCK, BLOCK)]
            remote(theirs, theirs, e_s[6 + side], e_r.at[6 + side], sp=pair).wait_recv()
    with jax.named_scope("state"):
        state_part(late)
    pump(len(queue))
    with jax.named_scope("out_wait"):
        spread_done(3)
    with jax.named_scope("state"):
        state_part(1 - late)
    with jax.named_scope("mix_a"):
        for side in range(2):
            theirs = act_a.at[1 - par, :, pl.ds(side * narrow, narrow)]
            remote(theirs, theirs, e_s[4 + side], e_r.at[4 + side], sp=pair).wait_recv()

    def target(who, i):
        first_column = lax.rem(who + 2 * (i // 2), n) * cols + (i % 2) * chunk
        return out.at[:, pl.ds(pl.multiple_of(first_column, 128), chunk)]

    def multiply(i):
        slot, lanes = late if i < 2 else 1 - late, slice(i % 2 * chunk, (i % 2 + 1) * chunk)
        total = pa[slot, :, lanes]
        for e in range(2):
            total = total + jnp.dot(
                act_a[e], wo_a[slot, e * wide : (e + 1) * wide, lanes], preferred_element_type=f32
            )
        for e in range(2):
            for side in range(2):
                block = total[e * tokens + side * size : e * tokens + (side + 1) * size]
                pf[i, e, side] = block
                pb[i, side, e] = block.astype(bf)
        launch(remote(pb.at[i, other], got.at[i], d_s.at[i], d_r.at[i], tp=other))

    def pass_on(i):
        remote(got.at[i], got.at[i], d_s.at[i], d_r.at[i], tp=other).wait_recv()
        fsend[i] = (pf[i, 1 - par, t] + got[i, 1 - par].astype(f32)).astype(bf)
        launch(remote(fsend.at[i], target(k, i), e_s[i], e_r.at[i], sp=pair))
        res[i] = (pf[i, par, t] + got[i, par].astype(f32)).astype(bf)
        launch(pltpu.make_async_copy(res.at[i], target(k, i), o_s.at[i]))

    for i in range(4):
        if i == 2:
            with jax.named_scope("out_wait"):
                spread_done(4)
        with jax.named_scope("multiply"):
            multiply(i)
        if i:
            with jax.named_scope("pass"):
                pass_on(i - 1)
    with jax.named_scope("pass"):
        pass_on(3)
    with jax.named_scope("settle"):
        for i in range(4):
            theirs = target(pair, i)
            remote(theirs, theirs, e_s[i], e_r.at[i], sp=pair).wait_recv()

    with jax.named_scope("drain"):
        for copies in spreads[-4:]:
            sent.extend(copies)
        for c in sent:
            if c.is_remote:
                c.wait_send()
            else:
                c.wait()

    @pl.when(late == 0)
    def _():
        hand_kv.wait_send()
        hand_state.wait_send()


def layer(x, gain, ssm, query, key, value, rate, turn, parts, reads, skip, shift, sinks, ows, owa):
    bf, f32 = jnp.bfloat16, jnp.float32
    tokens, half = x.shape
    rows, cols = ows.shape[0], ows.shape[1]
    wide = ssm.shape[1] // 2
    groups, state = rate.shape[0] // 2, rate.shape[1]
    length = 2 * tokens
    dma = pltpu.SemaphoreType.DMA
    vm = pltpu.VMEM
    return pl.pallas_call(
        layer_kernel,
        out_shape=jax.ShapeDtypeStruct((tokens // 2, 4 * cols), bf),
        in_specs=[ANY] * 15,
        out_specs=ANY,
        scratch_shapes=[
            vm((tokens, 2 * half), bf), vm((2, tokens, rows), bf), vm((2, length, rows), bf),
            vm((2, rows, 2 * wide), bf), vm((2, rows, 2 * wide), bf), vm((2,) + key.shape, bf),
            vm((2,) + value.shape, bf), vm((2, rows, cols), bf), vm((2, rows, cols), bf),
            vm(gain.shape, f32), vm(rate.shape, f32), vm(turn.shape, f32),
            vm(parts.shape, bf), vm(reads.shape, bf), vm(skip.shape, f32),
            vm((groups, length), f32), vm(sinks.shape, f32),
            vm((groups, 4, state, BLOCK), f32), vm((groups, 2 * state, GROUP_CH), bf),
            vm((groups, GROUP_CH, 2 * state), bf), vm((groups, length), f32), vm((groups, length), f32),
            vm((groups, 2 * state, length), f32), vm((wide, length), f32), vm((length, wide), bf),
            vm((length + WINDOW, 2 * HEAD_DIM), bf), vm((wide, length), f32),
            vm((2, length, wide), bf), vm((2, length, wide), bf),
            vm((groups, 2 * state), f32), vm((groups, 2 * state), f32),
            vm((8, tokens), f32), vm((8, tokens), f32), vm((length, 2 * wide), f32), vm((length, 2 * wide), f32),
            vm((2, length, wide // 2), bf), vm((2, length, wide // 2), bf), vm((length, 2 * HEAD_DIM), bf),
            vm((2, length, wide // 2), bf), vm((2, length, wide // 2), bf), vm((length, 2 * HEAD_DIM), bf),
            vm((2, length, cols), f32),
            vm((4, 2, 2, tokens // 2, cols // 2), f32), vm((4, 2, 2, tokens // 2, cols // 2), bf),
            vm((4, 2, tokens // 2, cols // 2), bf), vm((4, tokens // 2, cols // 2), bf),
            vm((4, tokens // 2, cols // 2), bf),
            dma((15,)), dma((16,)), dma((16,)), dma((7,)), dma((7,)), dma((4, 3)), dma((16, 3)),
            dma((5,)), dma((4,)), dma((4,)), dma((8,)), dma((4,)),
        ],
        compiler_params=pltpu.CompilerParams(collective_id=0, has_side_effects=True),
    )(x, gain, ssm, query, key, value, rate, turn, parts, reads, skip, shift, sinks, ows, owa)


def fast_body(
    inputs, norm_gain, in_ssm, in_query, in_key, in_value, decay_rate, rotation, input_parts,
    output_parts, skip_scale, decay_shift, sink_logit, out_state, out_attend,
):
    return layer(
        inputs, norm_gain[None], in_ssm, in_query, in_key, in_value, decay_rate, rotation,
        jnp.swapaxes(input_parts, 2, 3), output_parts, skip_scale.T, jnp.transpose(decay_shift),
        sink_logit[None], out_state, out_attend,
    )


def body(*args):
    n, n_fs, n_tp = lax.axis_size("sp"), lax.axis_size("fs"), lax.axis_size("tp")
    inputs, in_ssm, in_query, in_key, decay_rate = args[0], args[2], args[3], args[4], args[6]
    key_heads = in_key.shape[1] // HEAD_DIM
    query_heads = in_query.shape[1] // HEAD_DIM
    fits = (
        n_tp == 2
        and n == 4
        and n_fs == 4
        and key_heads == 2
        and query_heads % 4 == 0
        and query_heads * HEAD_DIM == in_ssm.shape[1]
        and in_ssm.shape[1] % 256 == 0
        and in_ssm.shape[1] == args[13].shape[0] == args[14].shape[0]
        and decay_rate.shape[0] % 32 == 0
        and decay_rate.shape[0] <= 2 * BLOCK
        and decay_rate.shape[1] * 2 == BLOCK
        and decay_rate.shape[0] * GROUP_CH == in_ssm.shape[1]
        and inputs.shape[0] == BLOCK == WINDOW
        and inputs.shape[1] % 128 == 0
        and in_ssm.shape[0] % 128 == 0
        and in_ssm.shape[0] == args[13].shape[0]
        and inputs.shape[1] == 2 * in_ssm.shape[0]
        and args[13].shape[1] % 128 == 0
    )
    return (fast_body if fits else general_body)(*args)


def solution(mesh):
    return jax.shard_map(
        body,
        mesh=mesh,
        in_specs=(
            P(("fs", "sp"), "tp"),
            P(),
            P("sp", "tp"),
            P("sp", "tp"),
            P("sp", "tp"),
            P("sp", "tp"),
            P("tp", None),
            P("tp", None),
            P(None, "tp", None, None),
            P(None, "tp", None, None),
            P("tp", None),
            P(("fs", "sp"), "tp"),
            P("tp"),
            P("tp", "sp"),
            P("tp", "sp"),
        ),
        out_specs=P(("fs", "sp", "tp"), None),
        check_vma=False,
    )
```

```python
import functools
import jax
import jax.numpy as jnp
from jax import lax
from jax.experimental import pallas as pl
from jax.experimental.pallas import tpu as pltpu
from jax.sharding import PartitionSpec as P

GROUP_CH = 16
HEAD_DIM = 64
WINDOW = 128
BLOCK = 128


epsilon = 1e-06
floor_score = -1e30


def prefix(x, axis, join, neutral):
    place = lax.axis_index(axis)
    gathered = jax.tree.map(
        lambda a, kind: lax.all_gather(a.astype(kind), axis),
        x,
        (jnp.bfloat16, jnp.bfloat16, jnp.bfloat16, jnp.bfloat16),
    )
    state = jax.tree.map(lambda a, e: jnp.zeros_like(a) + jnp.asarray(e, a.dtype), x, neutral)

    def one(hop, state):
        return join(
            state,
            jax.tree.map(
                lambda a, own: lax.dynamic_index_in_dim(a, hop, 0, False).astype(own.dtype),
                gathered,
                x,
            ),
        )

    return lax.fori_loop(0, place, one, state)


def from_behind(value, axis, steps):
    count = lax.axis_size(axis)
    initial, last = (max(0, -steps), min(count, count - steps))
    return lax.ppermute(value, axis, [(source, source + steps) for source in range(initial, last)])


def combine(earlier, later):
    first_re, first_im, state_re, state_im = earlier
    second_re, second_im, input_re, input_im = later
    return (
        second_re * first_re - second_im * first_im,
        second_re * first_im + second_im * first_re,
        second_re * state_re - second_im * state_im + input_re,
        second_re * state_im + second_im * state_re + input_im,
    )


def input_matrix(decay_rate, rotation, input_parts):
    damped = jnp.exp(-decay_rate)
    lift_re = damped * jnp.cos(rotation) - 1.0
    lift_im = damped * jnp.sin(rotation)
    modulus = decay_rate * decay_rate + rotation * rotation
    factor_re = (rotation * lift_im - decay_rate * lift_re) / modulus
    factor_im = -(rotation * lift_re + decay_rate * lift_im) / modulus
    part_re = input_parts[0].astype(jnp.float32)
    part_im = input_parts[1].astype(jnp.float32)
    joined_re = factor_re[:, :, None] * part_re - factor_im[:, :, None] * part_im
    joined_im = factor_re[:, :, None] * part_im + factor_im[:, :, None] * part_re
    return jnp.concatenate([joined_re, joined_im], axis=1).astype(jnp.bfloat16)


def window_attention(queries, keys_win, values_win, starts, sink_logit):
    window = queries.shape[1]
    scores = jnp.einsum("nqgrd,nkgd->ngrqk", queries, keys_win, preferred_element_type=jnp.float32)
    scores = scores * queries.shape[-1] ** (-0.5)
    places = (
        jnp.arange(window, dtype=jnp.int32)[:, None]
        + window
        - jnp.arange(2 * window, dtype=jnp.int32)[None, :]
    )
    inside = (places >= 0) & (places < window)
    reach = starts[:, None] - window + jnp.arange(2 * window, dtype=jnp.int32)[None, :] >= 0
    valid = (inside[None] & reach[:, None, :])[:, None, None]
    sinks = sink_logit.reshape(scores.shape[1], scores.shape[2])[None, :, :, None, None]
    scores = jnp.where(valid, scores, floor_score)
    row_peak = jnp.maximum(jnp.max(scores, axis=-1, keepdims=True), sinks)
    raised = jnp.where(valid, jnp.exp(scores - row_peak), 0.0)
    denominator = jnp.sum(raised, axis=-1, keepdims=True) + jnp.exp(sinks - row_peak)
    weights = (raised / denominator).astype(jnp.bfloat16)
    result = jnp.einsum(
        "ngrqk,nkgd->nqgrd", weights, values_win, preferred_element_type=jnp.float32
    )
    return result.astype(jnp.bfloat16)


def general_body(
    inputs,
    norm_gain,
    in_ssm,
    in_query,
    in_key,
    in_value,
    decay_rate,
    rotation,
    input_parts,
    output_parts,
    skip_scale,
    decay_shift,
    sink_logit,
    out_state,
    out_attend,
):
    gathered = lax.all_gather(inputs, "tp", axis=1, tiled=True)
    length = gathered.shape[0]
    widened = gathered.astype(jnp.float32)
    scale = lax.rsqrt(jnp.mean(widened * widened, axis=1, keepdims=True) + epsilon)
    normed = (widened * scale * norm_gain).astype(jnp.bfloat16)

    def add_rows(pieces):
        return tuple(
            (jnp.dot(normed, piece, preferred_element_type=jnp.float32) for piece in pieces)
        )

    projected = add_rows(
        (
            lax.all_gather(in_ssm, "sp", axis=0, tiled=True),
            lax.all_gather(in_query, "sp", axis=0, tiled=True),
            lax.all_gather(in_key, "sp", axis=0, tiled=True),
            lax.all_gather(in_value, "sp", axis=0, tiled=True),
        )
    )
    drive_in, queries, keys_local, values = [piece.astype(jnp.bfloat16) for piece in projected]
    groups = decay_rate.shape[0]
    state_dim = decay_rate.shape[1]
    channels = groups * GROUP_CH
    highest = lax.Precision.HIGHEST
    drive_cols = jnp.transpose(drive_in).reshape(groups, GROUP_CH, length)
    in_matrix = input_matrix(decay_rate, rotation, input_parts)
    drive = jnp.einsum("gqh,ght->gqt", in_matrix, drive_cols, preferred_element_type=jnp.float32)
    shift_cols = jnp.transpose(decay_shift)
    running = jnp.cumsum(shift_cols, axis=1)
    total_shift = running[:, -1]
    remain = length - 1.0 - jnp.arange(length, dtype=jnp.float32)
    to_end = (total_shift[:, None] - running)[:, None, :] - decay_rate[:, :, None] * remain[
        None, None, :
    ]
    fade = jnp.exp(to_end)
    turn = rotation[:, :, None] * remain[None, None, :]
    weight_re = fade * jnp.cos(turn)
    weight_im = fade * jnp.sin(turn)
    drive_re = drive[:, :state_dim]
    drive_im = drive[:, state_dim:]
    final_re = jnp.sum(weight_re * drive_re - weight_im * drive_im, axis=2)
    final_im = jnp.sum(weight_re * drive_im + weight_im * drive_re, axis=2)
    overall = jnp.exp(total_shift[:, None] - decay_rate * length)
    nothing = jnp.zeros_like(final_re)
    carried = prefix(
        (
            overall * jnp.cos(rotation * length),
            overall * jnp.sin(rotation * length),
            final_re,
            final_im,
        ),
        "sp",
        combine,
        (jnp.ones_like(final_re), nothing, nothing, nothing),
    )
    key_heads = keys_local.shape[1] // HEAD_DIM
    query_heads = queries.shape[1] // HEAD_DIM
    windows_dev = length // WINDOW
    previous = from_behind((keys_local, values), "sp", 1)

    def windows(flat, before):
        split = jnp.concatenate([before, flat], axis=0).reshape(
            windows_dev + 1, WINDOW, key_heads, HEAD_DIM
        )
        return jnp.concatenate([split[:-1], split[1:]], axis=1)

    offset = lax.axis_index("sp") * length
    starts = offset + jnp.arange(windows_dev, dtype=jnp.int32) * WINDOW
    queries_blk = queries.reshape(
        windows_dev, WINDOW, key_heads, query_heads // key_heads, HEAD_DIM
    )
    attended = window_attention(
        queries_blk,
        windows(keys_local, previous[0]),
        windows(values, previous[1]),
        starts,
        sink_logit,
    )
    attend_out = attended.reshape(length, query_heads * HEAD_DIM)
    blocks = length // BLOCK
    triangle = (
        jnp.arange(BLOCK, dtype=jnp.int32)[:, None] <= jnp.arange(BLOCK, dtype=jnp.int32)[None, :]
    ).astype(jnp.float32)
    offsets = jnp.arange(BLOCK, dtype=jnp.float32)
    centre = BLOCK // 2
    read_re = output_parts[0].astype(jnp.float32)
    read_im = output_parts[1].astype(jnp.float32)
    angle = rotation[:, :, None] * (offsets - centre)[None, None, :]
    cos_angle = jnp.cos(angle)
    sin_angle = jnp.sin(angle)
    phase = rotation[:, :, None] * (offsets + 1.0)[None, None, :]
    cos_phase = jnp.cos(phase)
    sin_phase = jnp.sin(phase)

    def advance(carry, pieces):
        carry_re, carry_im = carry
        part_re, part_im, shift_part, grouped_part = pieces
        level = jnp.dot(shift_part, triangle, precision=highest)
        log_from = level[:, None, :] - decay_rate[:, :, None] * (offsets + 1.0)[None, None, :]
        relative = log_from - log_from[:, :, centre : centre + 1]
        shrink = jnp.exp(-relative)
        lift_re = shrink * (part_re * cos_angle + part_im * sin_angle)
        lift_im = shrink * (part_im * cos_angle - part_re * sin_angle)
        prefix_re = jnp.dot(lift_re.reshape(groups * state_dim, BLOCK), triangle, precision=highest)
        prefix_im = jnp.dot(lift_im.reshape(groups * state_dim, BLOCK), triangle, precision=highest)
        prefix_re = prefix_re.reshape(groups, state_dim, BLOCK)
        prefix_im = prefix_im.reshape(groups, state_dim, BLOCK)
        grow = jnp.exp(relative)
        from_start = jnp.exp(log_from)
        keep_re = from_start * cos_phase
        keep_im = from_start * sin_phase
        state_re = grow * (prefix_re * cos_angle - prefix_im * sin_angle)
        state_im = grow * (prefix_im * cos_angle + prefix_re * sin_angle)
        state_re = state_re + keep_re * carry_re[:, :, None] - keep_im * carry_im[:, :, None]
        state_im = state_im + keep_re * carry_im[:, :, None] + keep_im * carry_re[:, :, None]
        result = jnp.einsum("ghp,gpt->ght", read_re, state_re, precision=highest)
        result = result - jnp.einsum("ghp,gpt->ght", read_im, state_im, precision=highest)
        result = result + skip_scale[:, :, None] * grouped_part.astype(jnp.float32)
        return ((state_re[:, :, -1], state_im[:, :, -1]), jax.nn.gelu(result).astype(jnp.bfloat16))

    drive_blocks = jnp.transpose(drive.reshape(groups, 2 * state_dim, blocks, BLOCK), (2, 0, 1, 3))
    shift_blocks = jnp.transpose(shift_cols.reshape(groups, blocks, BLOCK), (1, 0, 2))
    grouped_blocks = jnp.transpose(
        drive_cols.reshape(groups, GROUP_CH, blocks, BLOCK), (2, 0, 1, 3)
    )
    _, state_blocks = lax.scan(
        advance,
        (carried[2], carried[3]),
        (
            drive_blocks[:, :, :state_dim],
            drive_blocks[:, :, state_dim:],
            shift_blocks,
            grouped_blocks,
        ),
    )
    state_out = jnp.transpose(state_blocks, (0, 3, 1, 2)).reshape(length, channels)
    column_state, column_attend = (
        lax.all_gather(out_state, "sp", axis=1, tiled=True),
        lax.all_gather(out_attend, "sp", axis=1, tiled=True),
    )
    result = jnp.dot(state_out, column_state, preferred_element_type=jnp.float32)
    return lax.psum_scatter(
        (result + jnp.dot(attend_out, column_attend, preferred_element_type=jnp.float32)).astype(
            jnp.bfloat16
        ),
        "tp",
        scatter_dimension=0,
        tiled=True,
    )


MESH = pl.DeviceIdType.MESH
ANY = pl.BlockSpec(memory_space=pl.ANY)


def remote(src, dst, send, recv, **where):
    return pltpu.make_async_remote_copy(
        src_ref=src, dst_ref=dst, send_sem=send, recv_sem=recv, device_id=where, device_id_type=MESH
    )


def greet(peers):
    barrier = pltpu.get_barrier_semaphore()
    for peer in peers:
        pl.semaphore_signal(barrier, inc=1, device_id=peer, device_id_type=MESH)
    pl.semaphore_wait(barrier, len(peers))


def halves(x):
    high = x.astype(jnp.bfloat16)
    return high, (x - high.astype(jnp.float32)).astype(jnp.bfloat16)


def split_dot(x, exact):
    high, low = halves(x)
    return jnp.dot(high, exact, preferred_element_type=jnp.float32) + jnp.dot(
        low, exact, preferred_element_type=jnp.float32
    )


def column(row):
    size = row.shape[1]
    same = lax.broadcasted_iota(jnp.int32, (size, size), 0) == lax.broadcasted_iota(
        jnp.int32, (size, size), 1
    )
    return jnp.sum(jnp.where(same, row, 0.0), axis=1, keepdims=True)


def turned(angle):
    quarter = jnp.floor(angle * (2.0 / 3.141592653589793) + 0.5)
    r = ((angle - quarter * 1.5703125) - quarter * 4.837512969970703e-4) - quarter * 7.549789948768648e-8
    sq = r * r
    sin = r + r * sq * (-1.6666654611e-1 + sq * (8.3321608736e-3 + sq * -1.9515295891e-4))
    cos = 1.0 - 0.5 * sq + sq * sq * (4.166664568298827e-2 + sq * (-1.388731625493765e-3 + sq * 2.443315711809948e-5))
    which = quarter.astype(jnp.int32)
    swap = (which & 1) == 1
    flip_cos = ((which + 1) & 2) == 2
    flip_sin = (which & 2) == 2
    a, b = jnp.where(swap, sin, cos), jnp.where(swap, cos, sin)
    return jnp.where(flip_cos, -a, a), jnp.where(flip_sin, -b, b)


def layer_kernel(x_in, gain_in, ssm, query, key_in, value_in, rate_in, turn_in, parts_in, reads_in,
                 skip_in, shift_in, sinks_in, ows, owa, out,
                 xf, xp, normed, w_ssm, w_query, w_key, w_value, wo_s, wo_a, gain, rate, turn,
                 parts, reads, skip, shift, sinks, tab, inm, read, lifts, grows, prefix, u_scr, q_scr,
                 kv_scr, y_scr, act_s, act_a, carry_out, carry_in, scale_out, scale_in, total_in, total_q,
                 give_u, give_q, give_kv, got_u, got_q, got_kv, pa, pf, pb, got, fsend, res,
                 loc, z_s, z_r, p_s, p_r, x_s, x_r, g_r, d_r, e_r):
    f32, bf = jnp.float32, jnp.bfloat16
    k, f, t = lax.axis_index("sp"), lax.axis_index("fs"), lax.axis_index("tp")
    n, n_fs = 4, 4
    tokens, half = x_in.shape
    rows, cols = ssm.shape[0], ows.shape[1]
    wide = w_ssm.shape[2] // 2
    groups, state = tab.shape[0], tab.shape[2]
    heads = wide // HEAD_DIM
    par, late = lax.rem(k, 2), lax.div(k, 2)
    pair = k + 1 - 2 * par
    other = 1 - t
    fx, fy, far = f + 1 - 2 * lax.rem(f, 2), lax.rem(f + 2, n_fs), n_fs - 1 - f
    across_z = lax.rem(k + 2, n)

    part = rows // n_fs
    into = (w_ssm, w_query, None, wo_s, wo_a)
    origin = (ssm, query, None, ows, owa)
    cuts = (4, 4, 2, 2, 4)
    at_piece = [sum(cuts[:w]) for w in range(5)]

    def stripe(c):
        return pl.ds(c % 2 * wide + c // 2 * (wide // 2), wide // 2)

    def region(w, c, q, slot):
        if w < 2:
            return into[w].at[slot, pl.ds(pl.multiple_of(q * part, 16), part), stripe(c)]
        if w == 2:
            return (w_key, w_value)[c].at[slot, pl.ds(pl.multiple_of(q * part, 16), part)]
        size = part // cuts[w]
        return into[w].at[slot, pl.ds(pl.multiple_of(q * part + c * size, 16), size)]

    def over_z(w, c):
        if w < 2:
            source = origin[w].at[pl.ds(pl.multiple_of(f * part, 16), part), stripe(c)]
        elif w == 2:
            source = (key_in, value_in)[c].at[pl.ds(pl.multiple_of(f * part, 16), part)]
        else:
            size = part // cuts[w]
            source = origin[w].at[pl.ds(pl.multiple_of(f * part + c * size, 16), size)]
        return remote(source, region(w, c, f, late), z_s.at[at_piece[w] + c], z_r.at[at_piece[w] + c], sp=across_z)

    def spread_here(w, c):
        block = region(w, c, f, 1 - late)
        remote(block, block, z_s.at[at_piece[w] + c], z_r.at[at_piece[w] + c], sp=across_z).wait_recv()
        slot = len(spreads) % 4
        if len(spreads) >= 4:
            for copy in spreads[-4]:
                copy.wait_send()
        spreads.append([
            remote(block, block, x_s.at[slot, i], x_r.at[at_piece[w] + c, i], fs=who)
            for i, who in enumerate((far, fx, fy))
        ])
        for copy in spreads[-1]:
            copy.start()

    def spread_done(w, pieces=None):
        for c in pieces or range(cuts[w]):
            for i, who in enumerate((far, fx, fy)):
                block = region(w, c, who, 1 - late)
                remote(block, block, x_s.at[0, i], x_r.at[at_piece[w] + c, i], fs=who).wait_recv()

    sent, spreads = [], []
    g_s, e_s = [loc.at[i] for i in range(5)], [loc.at[5 + i] for i in range(8)]

    def launch(c):
        c.start()
        sent.append(c)

    def shift_at(e):
        return shift.at[:, pl.ds(pl.multiple_of(e * tokens, 128), tokens)]

    def shift_rows(e):
        return shift_in.at[pl.ds(pl.multiple_of(e * groups, 8), groups)]

    queue = [(f"s{w}{c}", functools.partial(spread_here, w, c)) for w in (0, 2, 1, 3, 4) for c in range(cuts[w])]

    def pump(count):
        for _ in range(min(count, len(queue))):
            name, step = queue.pop(0)
            with jax.named_scope(name):
                step()

    local = [
        (rate_in, rate), (turn_in, turn), (parts_in, parts), (reads_in, reads), (skip_in, skip),
        (gain_in, gain), (sinks_in, sinks), (shift_rows(par), shift_at(par)),
        (x_in, xf.at[:, pl.ds(pl.multiple_of(t * half, 128), half)]),
        (ssm, w_ssm.at[late]), (query, w_query.at[late]), (key_in, w_key.at[late]),
        (value_in, w_value.at[late]), (ows, wo_s.at[late]), (owa, wo_a.at[late]),
    ]
    local = [pltpu.make_async_copy(a, b, loc.at[i]) for i, (a, b) in enumerate(local)]
    for c in local:
        c.start()
    first = par * groups

    def tables(g, columns_of):
        line, spin = rate[pl.ds(first + g, 1), :], turn[pl.ds(first + g, 1), :]
        rates, turns = column(line), column(spin)
        away = lax.broadcasted_iota(jnp.int32, (state, BLOCK), 1).astype(f32) - float(BLOCK // 2)
        angle = turns * away
        cos, sin = turned(angle)
        fade = jnp.exp(-rates * away)
        rise = jnp.exp(rates * away)
        tab[g, 0] = rise * cos
        tab[g, 1] = -(rise * sin)
        tab[g, 2] = fade * cos
        tab[g, 3] = fade * sin
        damped = jnp.exp(-line)
        lift_re = damped * jnp.cos(spin) - 1.0
        lift_im = damped * jnp.sin(spin)
        modulus = line * line + spin * spin
        factor_re = (spin * lift_im - line * lift_re) / modulus
        factor_im = -(spin * lift_re + line * lift_im) / modulus
        part_re = parts[0, first + g].astype(f32)
        part_im = parts[1, first + g].astype(f32)
        inm[g] = jnp.transpose(
            jnp.concatenate(
                [factor_re * part_re - factor_im * part_im, factor_re * part_im + factor_im * part_re],
                axis=1,
            )
        ).astype(bf)
        read[g] = jnp.concatenate(
            [reads[0, first + g].astype(f32), -reads[1, first + g].astype(f32)], axis=1
        ).astype(bf)
        spot = lax.broadcasted_iota(jnp.int32, (state, BLOCK), 1) == g
        return jnp.where(spot, rates, columns_of[0]), jnp.where(spot, turns, columns_of[1])

    columns_of = (jnp.zeros((state, BLOCK), f32), jnp.zeros((state, BLOCK), f32))
    early = (n - 1 - k) * (n - 1 - k)
    peers = [{"sp": pair}, {"sp": across_z}, {"fs": fx}, {"fs": fy}, {"fs": far}, {"tp": other}]
    barrier = pltpu.get_barrier_semaphore()
    for peer in peers:
        pl.semaphore_signal(barrier, inc=1, device_id=peer, device_id_type=MESH)

    def settle_params():
        for c in local[:8]:
            c.wait()

    pl.when(k < n - 1)(settle_params)
    with jax.named_scope("tables"):
        columns_of = lax.fori_loop(0, early, tables, columns_of)
    with jax.named_scope("greet"):
        pl.semaphore_wait(barrier, len(peers))
    at_end = k * (n - 1 - k) == 0
    sides = pl.ds(pl.multiple_of(t * half, 128), half)
    launch(remote(x_in, xf.at[:, sides], p_s.at[0], p_r.at[0], tp=other))
    slow, fast, at_mid = t == 0, t == 1, k * (n - 1 - k) > 0

    def launch_if(choice, copies):
        @pl.when(choice)
        def _():
            for c in copies:
                c.start()

    state_weights = [over_z(0, c) for c in range(cuts[0])]
    early_keys = [over_z(2, c) for c in range(2)]
    query_weights = [over_z(1, c) for c in range(cuts[1])]
    out_weights = [over_z(3, c) for c in range(2)]
    attend_weights = [over_z(4, c) for c in range(cuts[4])]
    give_x = remote(x_in.at[:, pl.ds(pl.multiple_of((1 - par) * rows, 128), rows)], xp.at[t],
                    p_s.at[1], p_r.at[1], sp=pair)
    launch(remote(shift_rows(1 - par), shift_at(par), p_s.at[2], p_r.at[2], sp=pair))
    state_weights[0].start()
    launch_if(slow, state_weights[1:])
    launch_if(slow | jnp.logical_not(at_end), [give_x])
    launch_if(slow, early_keys)
    sent.append(give_x)
    pl.when(k == n - 1)(settle_params)
    with jax.named_scope("tables"):
        columns_of = lax.fori_loop(early, 10, tables, columns_of)

    local[8].wait()
    theirs = xf.at[:, pl.ds(pl.multiple_of(other * half, 128), half)]
    with jax.named_scope("own_x"):
        remote(theirs, theirs, p_s.at[0], p_r.at[0], tp=other).wait_recv()

    def gain_of(slot):
        return gain[:, pl.ds(pl.multiple_of((2 * slot + par) * rows, 128), rows)]

    own_rows = pl.ds(pl.multiple_of(par * tokens, 128), tokens)
    pair_rows = pl.ds(pl.multiple_of((1 - par) * tokens, 128), tokens)
    with jax.named_scope("norm"):
        full = xf[...].astype(f32)
        scale = lax.rsqrt(jnp.mean(full * full, axis=1, keepdims=True) + epsilon)
        same = lax.broadcasted_iota(jnp.int32, (tokens, tokens), 0) == lax.broadcasted_iota(
            jnp.int32, (tokens, tokens), 1
        )
        line = jnp.sum(jnp.where(same, scale, 0.0), axis=0, keepdims=True)
        scale_out[...] = jnp.broadcast_to(line, scale_out.shape)
    launch_if(fast, state_weights[1:] + early_keys)
    launch_if(fast & at_end, [give_x])
    launch(remote(scale_out, scale_in, p_s.at[3], p_r.at[3], sp=pair))
    with jax.named_scope("norm"):
        for slot in range(2):
            block = xf[:, pl.ds(pl.multiple_of((2 * slot + par) * rows, 128), rows)].astype(f32)
            normed[slot, own_rows] = (block * scale * gain_of(slot)).astype(bf)
    with jax.named_scope("tables"):
        columns_of = lax.fori_loop(10, groups, tables, columns_of)
    hand_x = remote(xp.at[t], xp.at[t], p_s.at[4], p_r.at[4], tp=other)
    sent.append(hand_x)

    def take_x():
        with jax.named_scope("next_x"):
            remote(xp.at[t], xp.at[t], p_s.at[1], p_r.at[1], sp=pair).wait_recv()
        hand_x.start()

    pump(1)
    pl.when(at_end)(take_x)
    pump(1)
    pump(2)
    for c in query_weights:
        c.start()
    near_shift = shift_at(1 - par)
    remote(near_shift, near_shift, p_s.at[2], p_r.at[2], sp=pair).wait_recv()

    shape = (BLOCK, BLOCK)
    upto = lax.broadcasted_iota(jnp.int32, shape, 0) <= lax.broadcasted_iota(jnp.int32, shape, 1)
    tri = upto.astype(f32).astype(bf)
    both_shape = (2 * BLOCK, 2 * BLOCK)
    from_at, to_at = (lax.broadcasted_iota(jnp.int32, both_shape, i) for i in range(2))
    tri_both = ((from_at <= to_at) & ((from_at < BLOCK) == (to_at < BLOCK))).astype(f32).astype(bf)
    centre = BLOCK // 2
    eye = lax.broadcasted_iota(jnp.int32, (groups, BLOCK), 0) == lax.broadcasted_iota(
        jnp.int32, (groups, BLOCK), 1
    )

    def across(col):
        return jnp.sum(jnp.where(eye, col, 0.0), axis=0, keepdims=True)

    begins, lasts = [], []
    for b in range(2):
        piece_b = shift[:, b * BLOCK : (b + 1) * BLOCK]
        high, low = halves(piece_b)
        low2 = (piece_b - high.astype(f32) - low.astype(f32)).astype(bf)
        level = (
            jnp.dot(high, tri, preferred_element_type=f32)
            + jnp.dot(low, tri, preferred_element_type=f32)
            + jnp.dot(low2, tri, preferred_element_type=f32)
        )
        middle = level[:, centre : centre + 1]
        lifts[:, b * BLOCK : (b + 1) * BLOCK] = jnp.exp(middle - level)
        grown = jnp.exp(level - middle)
        grows[:, b * BLOCK : (b + 1) * BLOCK] = grown
        begins.append(across(jnp.exp(middle)))
        lasts.append(across(grown[:, BLOCK - 1 :]))
    rates, turns = columns_of

    def times(a, b):
        return a[0] * b[0] - a[1] * b[1], a[0] * b[1] + a[1] * b[0]

    def plus(a, b):
        return a[0] + b[0], a[1] + b[1]

    def scaled(row, a):
        return row * a[0], row * a[1]

    def spiral(count):
        fade = jnp.exp(-rates * count)
        return fade * jnp.cos(turns * count), fade * jnp.sin(turns * count)

    reach, end = spiral(centre + 1.0), spiral(BLOCK - 1.0 - centre)
    whole = times(reach, end)

    pl.when(at_mid)(take_x)
    with jax.named_scope("partner_x"):
        remote(xp.at[other], xp.at[other], p_s.at[4], p_r.at[4], tp=other).wait_recv()
        remote(scale_in, scale_in, p_s.at[3], p_r.at[3], sp=pair).wait_recv()
    with jax.named_scope("norm"):
        scale = column(scale_in[0:1, :])
        for slot in range(2):
            normed[slot, pair_rows] = (xp[slot].astype(f32) * scale * gain_of(slot)).astype(bf)
    for c in local[9:]:
        c.wait()
    with jax.named_scope("own_u"):
        total_in[...] = jnp.dot(normed[late], w_ssm[late], preferred_element_type=f32)

    def part_of(w, slot):
        return jnp.dot(normed[slot], w[slot], preferred_element_type=f32)

    def mine_at(e):
        return pl.ds(pl.multiple_of(e * wide, 128), wide)


    narrow = wide // 2

    def state_inputs(h):
        with jax.named_scope("ssm_wait"):
            spread_done(0, (2 * h, 2 * h + 1))
        with jax.named_scope("project_u"):
            for e in range(2):
                lanes = slice(e * wide + h * narrow, e * wide + (h + 1) * narrow)
                total_in[:, lanes] += jnp.dot(
                    normed[1 - late], w_ssm[1 - late, :, lanes], preferred_element_type=f32
                )
            give_u[h] = total_in[:, half_at(1 - par, h)].astype(bf)
        launch(remote(give_u.at[h], got_u.at[h], g_s[3 * h], g_r.at[3 * h], sp=pair))

    def half_at(e, h):
        return pl.ds(pl.multiple_of(e * wide + h * narrow, 128), narrow)

    def turn_inputs(h):
        with jax.named_scope("got_u"):
            remote(got_u.at[h], got_u.at[h], g_s[3 * h], g_r.at[3 * h], sp=pair).wait_recv()
        with jax.named_scope("turn_u"):
            u = total_in[:, half_at(par, h)] + got_u[h].astype(f32)
            u_scr[h * narrow : (h + 1) * narrow, :] = jnp.transpose(u.astype(bf).astype(f32))

    state_inputs(0)
    pump(1)
    state_inputs(1)
    pump(1)
    launch_if(slow, out_weights)
    pump(2)
    turn_inputs(0)
    launch_if(fast, out_weights)
    launch_if(slow, attend_weights)

    def query_parts(h):
        with jax.named_scope("query_wait"):
            spread_done(1, (2 * h, 2 * h + 1))
        with jax.named_scope("project_q"):
            for e in range(2):
                lanes = slice(e * wide + h * narrow, e * wide + (h + 1) * narrow)
                total_q[:, lanes] = sum(
                    jnp.dot(normed[slot], w_query[slot, :, lanes], preferred_element_type=f32)
                    for slot in range(2)
                )
            give_q[h] = total_q[:, half_at(1 - par, h)].astype(bf)
        launch(remote(give_q.at[h], got_q.at[h], g_s[1 + 3 * h], g_r.at[1 + 3 * h], sp=pair))

    def key_parts():
        with jax.named_scope("key_wait"):
            spread_done(2)
        with jax.named_scope("project_kv"):
            keys = part_of(w_key, 0) + part_of(w_key, 1)
            values = part_of(w_value, 0) + part_of(w_value, 1)
            both = [
                jnp.concatenate([a[:, e * HEAD_DIM : (e + 1) * HEAD_DIM] for a in (keys, values)], axis=1)
                for e in range(2)
            ]
            give_kv[...] = jnp.where(par == 0, both[1], both[0]).astype(bf)
        launch(remote(give_kv, got_kv, g_s[2], g_r.at[2], sp=pair))

        return jnp.where(par == 0, both[0], both[1])

    tail = kv_scr.at[pl.ds(2 * WINDOW, WINDOW)]
    head = kv_scr.at[pl.ds(0, WINDOW)]
    hand_kv = remote(tail, head, p_s.at[5], p_r.at[5], sp=across_z)
    hand_state = remote(carry_out, carry_in, p_s.at[6], p_r.at[6], sp=across_z)

    def settle_kv():
        with jax.named_scope("kv_wait"):
            remote(got_kv, got_kv, g_s[2], g_r.at[2], sp=pair).wait_recv()
        kv_scr[WINDOW:, :] = (own_kv + got_kv[...].astype(f32)).astype(bf)

        @pl.when(late == 0)
        def _():
            hand_kv.start()
            kv_scr[:WINDOW, :] = jnp.zeros((WINDOW, kv_scr.shape[1]), bf)

    lane = lax.broadcasted_iota(jnp.int32, (state, BLOCK), 1)
    ends = [jnp.zeros((state, BLOCK), f32)] * 4
    for g in range(groups):
        if g == groups // 2:
            turn_inputs(1)
            launch_if(fast, attend_weights)
        with jax.named_scope("first"):
            u = u_scr[g * GROUP_CH : (g + 1) * GROUP_CH, :]
            drive = jnp.dot(inm[g], u.astype(bf), preferred_element_type=f32)
            up_re = jnp.concatenate([tab[g, 0]] * 2, axis=1)
            up_im = jnp.concatenate([tab[g, 1]] * 2, axis=1)
            row = lifts[g : g + 1, :]
            d_re, d_im = drive[:state] * row, drive[state:] * row
            lifted = jnp.concatenate([d_re * up_re - d_im * up_im, d_re * up_im + d_im * up_re], axis=0)
            sums = jnp.dot(lifted.astype(bf), tri_both, preferred_element_type=f32)
            prefix[g] = sums
            ends = [
                jnp.where(
                    lane == g,
                    sums[i % 2 * state : (i % 2 + 1) * state, (i // 2 + 1) * BLOCK - 1 : (i // 2 + 1) * BLOCK],
                    ends[i],
                )
                for i in range(4)
            ]
        if g == 5:
            own_kv = key_parts()
        if g in (1, 3):
            pump(1)
        if g == 11:
            query_parts(0)
            pump(1)
            if False:
                pump(1)
    with jax.named_scope("carry"):
        own = [scaled(lasts[b], times(end, (ends[2 * b], ends[2 * b + 1]))) for b in range(2)]
        decay = [scaled(lasts[b] * begins[b], whole) for b in range(2)]
        final = plus(own[1], times(decay[1], own[0]))
        carry_out[...] = jnp.transpose(jnp.concatenate(final, axis=0))[:groups]

    @pl.when(late == 0)
    def _():
        hand_state.start()
        carry_in[...] = jnp.zeros(carry_in.shape, f32)

    query_parts(1)
    settle_kv()
    pump(1)

    @pl.when(late == 1)
    def _():
        with jax.named_scope("hand_state"):
            hand_state.wait_recv()

    back = jnp.transpose(carry_in[...])
    entry = (back[:state], back[state:])

    def bases(row, c):
        return scaled(row, times(c, reach))

    def grown_entry(c):
        return plus((own[0][0][:, :groups], own[0][1][:, :groups]),
                    times((decay[0][0][:, :groups], decay[0][1][:, :groups]), c))

    cut = (reach[0][:, :groups], reach[1][:, :groups])
    base = [
        scaled(begins[0][:, :groups], times(entry, cut)),
        scaled(begins[1][:, :groups], times(grown_entry(entry), cut)),
    ]
    for g in range(groups):
        with jax.named_scope("second"):
            u = u_scr[g * GROUP_CH : (g + 1) * GROUP_CH, :]
            down = [jnp.concatenate([tab[g, i]] * 2, axis=1) for i in (2, 3)]
            chosen = lax.broadcasted_iota(jnp.int32, skip.shape, 1) == first + g
            skips = jnp.sum(jnp.where(chosen, skip[...], 0.0), axis=1, keepdims=True)
            p = [
                prefix[g, i * state : (i + 1) * state]
                + jnp.concatenate(
                    [jnp.broadcast_to(base[b][i][:, g : g + 1], (state, BLOCK)) for b in range(2)], axis=1
                )
                for i in range(2)
            ]
            states = jnp.concatenate(scaled(grows[g : g + 1, :], times(down, p)), axis=0).astype(bf)
            y = jnp.dot(read[g], states, preferred_element_type=f32)
            y_scr[g * GROUP_CH : (g + 1) * GROUP_CH, :] = y + skips * u
        if (g + 1) % (groups // 2) == 0:
            side = (g + 1) // (groups // 2) - 1
            lanes = slice(side * BLOCK, (side + 1) * BLOCK)
            with jax.named_scope("gelu"):
                act_s[par, :, lanes] = jnp.transpose(jax.nn.gelu(y_scr[lanes, :])).astype(bf)
            half_s = act_s.at[par, :, pl.ds(side * BLOCK, BLOCK)]
            launch(remote(half_s, half_s, e_s[6 + side], e_r.at[6 + side], sp=pair))

    gap_shape = (WINDOW, 2 * WINDOW)
    at = lax.broadcasted_iota(jnp.int32, gap_shape, 1)
    gap = lax.broadcasted_iota(jnp.int32, gap_shape, 0) + WINDOW - at
    inside = (gap >= 0) & (gap < WINDOW)
    inside_first = inside & (at >= WINDOW * (1 - late))
    sink_lane = lax.broadcasted_iota(jnp.int32, sinks.shape, 1)
    pump(2)
    for side in range(2):
        pump(1)
        with jax.named_scope("q_wait"):
            remote(got_q.at[side], got_q.at[side], g_s[1 + 3 * side], g_r.at[1 + 3 * side], sp=pair).wait_recv()
        q_scr[:, side * narrow : (side + 1) * narrow] = (
            (total_q[:, half_at(par, side)] + got_q[side].astype(f32)) * HEAD_DIM ** (-0.5)
        ).astype(bf)
        for b in (1, 0):
            if b == 0 and side == 0:

                @pl.when(late == 1)
                def _():
                    with jax.named_scope("hand_kv"):
                        hand_kv.wait_recv()

            keys = kv_scr[b * WINDOW : (b + 2) * WINDOW, :HEAD_DIM]
            values = kv_scr[b * WINDOW : (b + 2) * WINDOW, HEAD_DIM:]
            valid = inside if b else inside_first
            outs = []
            for h in range(side * heads // 2, (side + 1) * heads // 2):
                with jax.named_scope("head"):
                    q = q_scr[b * WINDOW : (b + 1) * WINDOW, h * HEAD_DIM : (h + 1) * HEAD_DIM]
                    scores = lax.dot_general(q, keys, (((1,), (1,)), ((), ())), preferred_element_type=f32)
                    scores = jnp.where(valid, scores, floor_score)
                    sink = jnp.sum(
                        jnp.where(sink_lane == par * heads + h, sinks[...], 0.0), axis=1, keepdims=True
                    )
                    peak = jnp.maximum(jnp.max(scores, axis=1, keepdims=True), sink)
                    raised = jnp.exp(scores - peak)
                    total = jnp.sum(raised, axis=1, keepdims=True) + jnp.exp(sink - peak)
                    weights = (raised * (1.0 / total)).astype(bf)
                    outs.append(jnp.dot(weights, values, preferred_element_type=f32))
            act_a[par, b * BLOCK : (b + 1) * BLOCK, side * narrow : (side + 1) * narrow] = jnp.concatenate(
                outs, axis=1
            ).astype(bf)
        half_a = act_a.at[par, :, pl.ds(side * narrow, narrow)]
        launch(remote(half_a, half_a, e_s[4 + side], e_r.at[4 + side], sp=pair))

    size, chunk = tokens // 2, cols // 2
    def state_part(slot):
        for side in range(2):
            lanes = slice(side * chunk, (side + 1) * chunk)
            both = [jnp.dot(act_s[e], wo_s[slot, e * wide : (e + 1) * wide, lanes], preferred_element_type=f32)
                    for e in range(2)]
            pa[slot, :, lanes] = both[0] + both[1]

    with jax.named_scope("mix_s"):
        for side in range(2):
            theirs = act_s.at[1 - par, :, pl.ds(side * BLOCK, BLOCK)]
            remote(theirs, theirs, e_s[6 + side], e_r.at[6 + side], sp=pair).wait_recv()
    with jax.named_scope("state"):
        state_part(late)
    pump(len(queue))
    with jax.named_scope("out_wait"):
        spread_done(3)
    with jax.named_scope("state"):
        state_part(1 - late)
    with jax.named_scope("mix_a"):
        for side in range(2):
            theirs = act_a.at[1 - par, :, pl.ds(side * narrow, narrow)]
            remote(theirs, theirs, e_s[4 + side], e_r.at[4 + side], sp=pair).wait_recv()

    for c in state_weights + early_keys + query_weights + out_weights + attend_weights:
        c.wait_send()

    def target(who, i):
        first_column = lax.rem(who + 2 * (i // 2), n) * cols + (i % 2) * chunk
        return out.at[:, pl.ds(pl.multiple_of(first_column, 128), chunk)]

    def multiply(i):
        slot, lanes = late if i < 2 else 1 - late, slice(i % 2 * chunk, (i % 2 + 1) * chunk)
        total = pa[slot, :, lanes]
        for e in range(2):
            total = total + jnp.dot(
                act_a[e], wo_a[slot, e * wide : (e + 1) * wide, lanes], preferred_element_type=f32
            )
        for e in range(2):
            for side in range(2):
                block = total[e * tokens + side * size : e * tokens + (side + 1) * size]
                pf[i, e, side] = block
                pb[i, side, e] = block.astype(bf)
        launch(remote(pb.at[i, other], got.at[i], z_s.at[i], d_r.at[i], tp=other))

    def pass_on(i):
        remote(got.at[i], got.at[i], z_s.at[i], d_r.at[i], tp=other).wait_recv()
        fsend[i] = (pf[i, 1 - par, t] + got[i, 1 - par].astype(f32)).astype(bf)
        launch(remote(fsend.at[i], target(k, i), e_s[i], e_r.at[i], sp=pair))
        res[i] = (pf[i, par, t] + got[i, par].astype(f32)).astype(bf)
        launch(pltpu.make_async_copy(res.at[i], target(k, i), z_s.at[4 + i]))

    for i in range(4):
        if i == 2:
            with jax.named_scope("out_wait"):
                spread_done(4)
        with jax.named_scope("multiply"):
            multiply(i)
        if i:
            with jax.named_scope("pass"):
                pass_on(i - 1)
    with jax.named_scope("pass"):
        pass_on(3)
    with jax.named_scope("settle"):
        for i in range(4):
            theirs = target(pair, i)
            remote(theirs, theirs, e_s[i], e_r.at[i], sp=pair).wait_recv()

    with jax.named_scope("drain"):
        for copies in spreads[-4:]:
            sent.extend(copies)
        for c in sent:
            if c.is_remote:
                c.wait_send()
            else:
                c.wait()

    @pl.when(late == 0)
    def _():
        hand_kv.wait_send()
        hand_state.wait_send()


def layer(x, gain, ssm, query, key, value, rate, turn, parts, reads, skip, shift, sinks, ows, owa):
    bf, f32 = jnp.bfloat16, jnp.float32
    tokens, half = x.shape
    rows, cols = ows.shape[0], ows.shape[1]
    wide = ssm.shape[1] // 2
    groups, state = rate.shape[0] // 2, rate.shape[1]
    length = 2 * tokens
    dma = pltpu.SemaphoreType.DMA
    vm = pltpu.VMEM
    return pl.pallas_call(
        layer_kernel,
        out_shape=jax.ShapeDtypeStruct((tokens // 2, 4 * cols), bf),
        in_specs=[ANY] * 15,
        out_specs=ANY,
        scratch_shapes=[
            vm((tokens, 2 * half), bf), vm((2, tokens, rows), bf), vm((2, length, rows), bf),
            vm((2, rows, 2 * wide), bf), vm((2, rows, 2 * wide), bf), vm((2,) + key.shape, bf),
            vm((2,) + value.shape, bf), vm((2, rows, cols), bf), vm((2, rows, cols), bf),
            vm(gain.shape, f32), vm(rate.shape, f32), vm(turn.shape, f32),
            vm(parts.shape, bf), vm(reads.shape, bf), vm(skip.shape, f32),
            vm((groups, length), f32), vm(sinks.shape, f32),
            vm((groups, 4, state, BLOCK), f32), vm((groups, 2 * state, GROUP_CH), bf),
            vm((groups, GROUP_CH, 2 * state), bf), vm((groups, length), f32), vm((groups, length), f32),
            vm((groups, 2 * state, length), f32), vm((wide, length), f32), vm((length, wide), bf),
            vm((length + WINDOW, 2 * HEAD_DIM), bf), vm((wide, length), f32),
            vm((2, length, wide), bf), vm((2, length, wide), bf),
            vm((groups, 2 * state), f32), vm((groups, 2 * state), f32),
            vm((8, tokens), f32), vm((8, tokens), f32), vm((length, 2 * wide), f32), vm((length, 2 * wide), f32),
            vm((2, length, wide // 2), bf), vm((2, length, wide // 2), bf), vm((length, 2 * HEAD_DIM), bf),
            vm((2, length, wide // 2), bf), vm((2, length, wide // 2), bf), vm((length, 2 * HEAD_DIM), bf),
            vm((2, length, cols), f32),
            vm((4, 2, 2, tokens // 2, cols // 2), f32), vm((4, 2, 2, tokens // 2, cols // 2), bf),
            vm((4, 2, tokens // 2, cols // 2), bf), vm((4, tokens // 2, cols // 2), bf),
            vm((4, tokens // 2, cols // 2), bf),
            dma((15,)), dma((16,)), dma((16,)), dma((7,)), dma((7,)), dma((4, 3)), dma((16, 3)),
            dma((5,)), dma((4,)), dma((8,)),
        ],
        compiler_params=pltpu.CompilerParams(collective_id=0, has_side_effects=True),
    )(x, gain, ssm, query, key, value, rate, turn, parts, reads, skip, shift, sinks, ows, owa)


def fast_body(
    inputs, norm_gain, in_ssm, in_query, in_key, in_value, decay_rate, rotation, input_parts,
    output_parts, skip_scale, decay_shift, sink_logit, out_state, out_attend,
):
    return layer(
        inputs, norm_gain[None], in_ssm, in_query, in_key, in_value, decay_rate, rotation,
        jnp.swapaxes(input_parts, 2, 3), output_parts, skip_scale.T, jnp.transpose(decay_shift),
        sink_logit[None], out_state, out_attend,
    )


def body(*args):
    n, n_fs, n_tp = lax.axis_size("sp"), lax.axis_size("fs"), lax.axis_size("tp")
    inputs, in_ssm, in_query, in_key, decay_rate = args[0], args[2], args[3], args[4], args[6]
    key_heads = in_key.shape[1] // HEAD_DIM
    query_heads = in_query.shape[1] // HEAD_DIM
    fits = (
        n_tp == 2
        and n == 4
        and n_fs == 4
        and key_heads == 2
        and query_heads % 4 == 0
        and query_heads * HEAD_DIM == in_ssm.shape[1]
        and in_ssm.shape[1] % 256 == 0
        and in_ssm.shape[1] == args[13].shape[0] == args[14].shape[0]
        and decay_rate.shape[0] % 32 == 0
        and decay_rate.shape[0] <= 2 * BLOCK
        and decay_rate.shape[1] * 2 == BLOCK
        and decay_rate.shape[0] * GROUP_CH == in_ssm.shape[1]
        and inputs.shape[0] == BLOCK == WINDOW
        and inputs.shape[1] % 128 == 0
        and in_ssm.shape[0] % 128 == 0
        and in_ssm.shape[0] == args[13].shape[0]
        and inputs.shape[1] == 2 * in_ssm.shape[0]
        and args[13].shape[1] % 128 == 0
    )
    return (fast_body if fits else general_body)(*args)


def solution(mesh):
    return jax.shard_map(
        body,
        mesh=mesh,
        in_specs=(
            P(("fs", "sp"), "tp"),
            P(),
            P("sp", "tp"),
            P("sp", "tp"),
            P("sp", "tp"),
            P("sp", "tp"),
            P("tp", None),
            P("tp", None),
            P(None, "tp", None, None),
            P(None, "tp", None, None),
            P("tp", None),
            P(("fs", "sp"), "tp"),
            P("tp"),
            P("tp", "sp"),
            P("tp", "sp"),
        ),
        out_specs=P(("fs", "sp", "tp"), None),
        check_vma=False,
    )
```
